32 devices in a mesh: grp: 2 (over y), sp: 4 (over z), tp: 4 (over x, core).
Axes of the slice: x: 2, y: 2, z: 4, core: 2. Of those that a mesh axis runs over, the one named last changes fastest.
Arguments:
- latent: bfloat16 [12288, 2048], P(('grp', 'sp')), parts along dimension 0, may hold values from -6 to 6
- condition: bfloat16 [4096], P('grp'), parts along dimension 0, may hold values from -6 to 6
- context_tokens: bfloat16 [512, 2048], P(('grp', 'sp')), parts along dimension 0, may hold values from -6 to 6
- context_condition: bfloat16 [2048], replicated, may hold values from -6 to 6
- shift_weight: bfloat16 [2048, 2048], P('sp', 'tp'), may hold values from -0.25 to 0.25
- scale_weight: bfloat16 [2048, 2048], P('sp', 'tp'), may hold values from -0.25 to 0.25
- gate_weight: bfloat16 [2048, 2048], P('sp', 'tp'), may hold values from -0.25 to 0.25
- norm_gain: bfloat16 [2048], replicated, may hold values from 0.099609375 to 1.8984375
- query_weight: bfloat16 [2048, 1024], P(None, 'tp'), may hold values from -0.125 to 0.125
- key_weight: bfloat16 [2048, 1024], P(None, 'tp'), may hold values from -0.125 to 0.125
- value_weight: bfloat16 [2048, 1024], P(None, 'tp'), may hold values from -0.125 to 0.125
- out_weight: bfloat16 [1024, 2048], replicated, may hold values from -0.1875 to 0.1875
- offset_bias: float32 [16, 15, 31], P('tp'), may hold values from 0.5 to 260
Outputs:
- mixed_latent: bfloat16 [12288, 2048], P(('grp', 'sp', 'tp')), parts along dimension 0
The draws below stay inside these ranges and needn't reach their ends.
There are 2 independent parts, one for each index of `grp`. The reference program is written for one: setup_inputs(seed, part) draws one part's arguments, and reference() takes and returns one part's arrays. A program takes and returns all parts, laid end to end along the dimension named above; an argument that names none is the same for every part. Nothing has to cross between parts.
All inputs are finite; a program needn't handle non-finite values.
Results may differ from the reference program's by a relative error of at most 0.011.
Values may be sent and summed in bfloat16 or wider, within the bound.
No kernel may reach another device: no remote copies, remote signals or barrier semaphores. Data moves between devices by JAX's collectives and lax.ppermute only.
A program may use at most 192 MiB of HBM per device.

```python
import jax
import jax.numpy as jnp
import numpy as np
from jax import lax

D = 2048
HEADS = 16
HEAD_DIM = 64
ATT = 1024
GRID_W = 64
WIN_ROWS = 8
WIN_COLS = 16
COL_BLOCK = 16
CTX = 256
TOKENS = 6144


def draw_offset_bias(key, part):
    keys_all = jax.random.split(key, 1)
    table_shape = (HEADS, 2 * WIN_ROWS - 1, 2 * WIN_COLS - 1)
    bias_table = jax.random.uniform(keys_all[0], table_shape, jnp.float32, 0.5, 2.5)
    return bias_table


def shard_levels(key, dims, cuts, least, top_value):
    level, own = 1.0, jax.random.fold_in(key, 6)
    for dim, blocks in cuts:
        steps = jnp.exp(jax.random.uniform(jax.random.fold_in(own, dim), (blocks,), jnp.float32, least / len(cuts), top_value / len(cuts)))
        level = level * jnp.repeat(steps, dims[dim] // blocks).reshape([-1 if axis == dim else 1 for axis in range(len(dims))])
    return level


def centred(stream_key, shape, width, limit, cuts=(), kind=jnp.bfloat16):
    loudness = shard_levels(stream_key, shape, cuts, -0.22, 0.18) if cuts else 1.0
    array = jax.random.normal(stream_key, shape, jnp.float32) * width * loudness
    return jnp.minimum(jnp.maximum(array, -limit), limit).astype(kind)


def setup_inputs(seed: int = 0, part: int = 0) -> dict:
    key_of = jax.random.split(jax.random.key(seed), 14)
    part_keys = jax.random.split(jax.random.fold_in(key_of[13], part), 14)
    return {
        "latent": centred(part_keys[0], (TOKENS, D), 1.0, 6.0, ((0, 4),)),
        "condition": centred(part_keys[1], (D,), 1.0, 6.0),
        "context_tokens": centred(part_keys[2], (CTX, D), 1.0, 6.0, ((0, 4),)),
        "context_condition": centred(key_of[3], (D,), 1.0, 6.0),
        "shift_weight": centred(key_of[4], (D, D), (D // 4) ** -0.5, 0.25, ((0, 4), (1, 4))),
        "scale_weight": centred(key_of[5], (D, D), (D // 4) ** -0.5, 0.25, ((0, 4), (1, 4))),
        "gate_weight": centred(key_of[6], (D, D), (D // 4) ** -0.5, 0.25, ((0, 4), (1, 4))),
        "norm_gain": jnp.clip(1.0 + 0.18 * jax.random.normal(key_of[7], (D,), jnp.float32), 0.099609375, 1.8984375).astype(jnp.bfloat16),
        "query_weight": centred(key_of[8], (D, ATT), D ** -0.5, 0.125, ((1, 4),)),
        "key_weight": centred(key_of[9], (D, ATT), D ** -0.5, 0.125, ((1, 4),)),
        "value_weight": centred(key_of[10], (D, ATT), D ** -0.5, 0.125, ((1, 4),)),
        "out_weight": centred(key_of[11], (ATT, D), ATT ** -0.5, 0.1875),
        "offset_bias": draw_offset_bias(jax.random.fold_in(key_of[13], 71), part),
    }


epsilon = 1e-06
masked_score = -1e+30

def column_tables():
    block_count = GRID_W // COL_BLOCK
    strip_width = COL_BLOCK + WIN_COLS
    query_column = np.arange(GRID_W).reshape(block_count, COL_BLOCK)
    strip_start = np.clip(np.arange(block_count) * COL_BLOCK - WIN_COLS // 2, 0, GRID_W - strip_width)
    key_column = strip_start[:, None] + np.arange(strip_width)
    window_start = np.clip(query_column - WIN_COLS // 2, 0, GRID_W - WIN_COLS)
    inside = (key_column[:, None, :] >= window_start[..., None]) & (key_column[:, None, :] < window_start[..., None] + WIN_COLS)
    column_offset = np.clip(key_column[:, None, :] - query_column[..., None] + WIN_COLS - 1, 0, 2 * WIN_COLS - 2)
    return (strip_start, inside, column_offset)

def modulate_rows(tokens, norm_gain, shift_vector, scale_vector):
    values = tokens.astype(jnp.float32)
    normed = values * lax.rsqrt(lax.optimization_barrier(jnp.mean(values * values, axis=-1, keepdims=True)) + epsilon)
    return (normed * norm_gain.astype(jnp.float32) * (1.0 + scale_vector) + shift_vector).astype(jnp.bfloat16)

def neighbour_attention(queries, key_rows, value_rows, context_keys, context_values, offset_bias):
    heads_total = offset_bias.shape[0]
    grid_rows = queries.shape[0] // GRID_W
    block_count = GRID_W // COL_BLOCK
    strip_width = COL_BLOCK + WIN_COLS
    strip_start, inside, column_offset = column_tables()
    query_grid = queries.astype(jnp.float32).reshape(grid_rows, block_count, COL_BLOCK, heads_total, HEAD_DIM)
    key_grid = key_rows.astype(jnp.float32).reshape(grid_rows, GRID_W, heads_total, HEAD_DIM)
    value_grid = value_rows.astype(jnp.float32).reshape(grid_rows, GRID_W, heads_total, HEAD_DIM)
    far_keys = context_keys.astype(jnp.float32).reshape(-1, heads_total, HEAD_DIM)
    far_values = context_values.astype(jnp.float32).reshape(-1, heads_total, HEAD_DIM)
    factor = HEAD_DIM ** (-0.5)
    bias_table = offset_bias.astype(jnp.float32)

    def one_row(grid_row):
        first_row = jnp.clip(grid_row - WIN_ROWS // 2, 0, grid_rows - WIN_ROWS)
        key_window = lax.dynamic_slice_in_dim(key_grid, first_row, WIN_ROWS, 0)
        value_window = lax.dynamic_slice_in_dim(value_grid, first_row, WIN_ROWS, 0)
        key_strip = jnp.stack([key_window[:, int(column_begin):int(column_begin) + strip_width] for column_begin in strip_start], axis=1)
        value_strip = jnp.stack([value_window[:, int(column_begin):int(column_begin) + strip_width] for column_begin in strip_start], axis=1)
        query_row = lax.dynamic_index_in_dim(query_grid, grid_row, 0, keepdims=False)
        row_offset = first_row + jnp.arange(WIN_ROWS, dtype=jnp.int32) - grid_row + WIN_ROWS - 1
        bias_rows = bias_table[:, row_offset]
        bias_full = bias_rows[:, :, column_offset]
        near_scores = jnp.einsum('nqhd,wnkhd->hnqwk', query_row, key_strip) * factor + jnp.transpose(bias_full, (0, 2, 3, 1, 4))
        near_scores = jnp.where(inside[None, :, :, None, :], near_scores, masked_score)
        far_scores = jnp.einsum('nqhd,chd->hnqc', query_row, far_keys) * factor
        score_peak = jnp.maximum(lax.optimization_barrier(jnp.max(near_scores, axis=(3, 4))), lax.optimization_barrier(jnp.max(far_scores, axis=3)))
        near_exp = jnp.exp(near_scores - score_peak[..., None, None])
        far_exp = jnp.exp(far_scores - score_peak[..., None])
        denominator = lax.optimization_barrier(jnp.sum(near_exp, axis=(3, 4))) + lax.optimization_barrier(jnp.sum(far_exp, axis=3))
        near_weights = (near_exp / denominator[..., None, None]).astype(jnp.bfloat16).astype(jnp.float32)
        far_weights = (far_exp / denominator[..., None]).astype(jnp.bfloat16).astype(jnp.float32)
        output = jnp.einsum('hnqwk,wnkhd->nqhd', near_weights, value_strip) + jnp.einsum('hnqc,chd->nqhd', far_weights, far_values)
        return output.astype(jnp.bfloat16).reshape(GRID_W, heads_total * HEAD_DIM)
    rows_out = lax.map(one_row, jnp.arange(grid_rows, dtype=jnp.int32))
    return rows_out.reshape(grid_rows * GRID_W, heads_total * HEAD_DIM)

def reference(latent, condition, context_tokens, context_condition, shift_weight, scale_weight, gate_weight, norm_gain, query_weight, key_weight, value_weight, out_weight, offset_bias):
    cond_act = jax.nn.silu(condition.astype(jnp.float32)).astype(jnp.bfloat16)
    context_act = jax.nn.silu(context_condition.astype(jnp.float32)).astype(jnp.bfloat16)
    shift_vector = jnp.dot(cond_act, shift_weight, preferred_element_type=jnp.float32)
    scale_vector = jnp.dot(cond_act, scale_weight, preferred_element_type=jnp.float32)
    gate_vector = jnp.dot(cond_act, gate_weight, preferred_element_type=jnp.float32)
    context_shift = jnp.dot(context_act, shift_weight, preferred_element_type=jnp.float32)
    context_scale = jnp.dot(context_act, scale_weight, preferred_element_type=jnp.float32)
    hidden = modulate_rows(latent, norm_gain, shift_vector, scale_vector)
    context_hidden = modulate_rows(context_tokens, norm_gain, context_shift, context_scale)
    queries = jnp.dot(hidden, query_weight, preferred_element_type=jnp.float32).astype(jnp.bfloat16)
    key_rows = jnp.dot(hidden, key_weight, preferred_element_type=jnp.float32).astype(jnp.bfloat16)
    value_rows = jnp.dot(hidden, value_weight, preferred_element_type=jnp.float32).astype(jnp.bfloat16)
    context_keys = jnp.dot(context_hidden, key_weight, preferred_element_type=jnp.float32).astype(jnp.bfloat16)
    context_values = jnp.dot(context_hidden, value_weight, preferred_element_type=jnp.float32).astype(jnp.bfloat16)
    attended = neighbour_attention(queries, key_rows, value_rows, context_keys, context_values, offset_bias)
    branch = jnp.dot(attended, out_weight, preferred_element_type=jnp.float32)
    return (latent.astype(jnp.float32) + gate_vector * branch).astype(jnp.bfloat16)
```

```python
import functools
import math

import jax
import jax.numpy as jnp
import numpy as np
from jax import lax
from jax.experimental import pallas as pl
from jax.experimental.pallas import tpu as pltpu
from jax.sharding import PartitionSpec as P

HEAD_DIM = 64
GRID_W = 64
WIN_ROWS = 8
WIN_COLS = 16
ROW_OFFSETS = 2 * WIN_ROWS - 1
COL_OFFSETS = 2 * WIN_COLS - 1
LANES = 128

epsilon = 1e-06
masked_score = -1e30
log2e = math.log2(math.e)
SMEM = pltpu.SMEM
VMEM = pltpu.VMEM
f32 = jnp.float32
bf16 = jnp.bfloat16


def shift_along(block, axis, step):
    count = lax.axis_size(axis)
    return lax.ppermute(block, axis, [(i, (i + step) % count) for i in range(count)])


def whole(memory_space=VMEM):
    return pl.BlockSpec(memory_space=memory_space)


def call(kernel, out_shape, *, vmem=32 << 20, **kwargs):
    return pl.pallas_call(
        kernel,
        out_shape=out_shape,
        compiler_params=pltpu.CompilerParams(vmem_limit_bytes=vmem),
        **kwargs,
    )


def modulation_kernel(sp_ref, cond_ref, ctx_ref, shift_ref, scale_ref, gate_ref, out_ref):
    rows = shift_ref.shape[0]
    part = pl.ds(pl.multiple_of(sp_ref[0] * rows, LANES), rows)

    def act(ref):
        v = ref[:, part].astype(f32)
        return (v / (1.0 + jnp.exp(-v))).astype(bf16)

    both = jnp.concatenate([act(cond_ref), act(ctx_ref)] + [jnp.zeros((14, rows), bf16)], axis=0)
    shift = jnp.dot(both, shift_ref[...], preferred_element_type=f32)
    scale = jnp.dot(both, scale_ref[...], preferred_element_type=f32)
    gate = jnp.dot(both, gate_ref[...], preferred_element_type=f32)
    out_ref[0:2, :] = shift[0:2]
    out_ref[2:4, :] = scale[0:2]
    out_ref[4:6, :] = gate[0:2]
    out_ref[6:8, :] = jnp.zeros_like(out_ref[6:8, :])


def modulation_terms(sp_index, condition, context_condition, shift_weight, scale_weight, gate_weight):
    return call(
        modulation_kernel,
        jax.ShapeDtypeStruct((8, shift_weight.shape[1]), f32),
        in_specs=[whole(SMEM)] + [whole()] * 5,
        out_specs=whole(),
    )(
        sp_index,
        condition.reshape(1, -1),
        context_condition.reshape(1, -1),
        shift_weight,
        scale_weight,
        gate_weight,
    )


def bias_kernel(rows_ref, out_ref):
    pairs = rows_ref.shape[1]
    key = lax.broadcasted_iota(jnp.int32, (GRID_W, LANES), 0)
    query = lax.broadcasted_iota(jnp.int32, (GRID_W, LANES), 1) % GRID_W
    first = jnp.clip(query - WIN_COLS // 2, 0, GRID_W - WIN_COLS)
    inside = (key >= first) & (key < first + WIN_COLS)
    for offset in range(ROW_OFFSETS):
        for pair in range(pairs):
            line = jnp.broadcast_to(rows_ref[offset, pair : pair + 1, :], (GRID_W, LANES))
            skewed = pltpu.roll(line, 0, 1, stride=1, stride_axis=0)
            out_ref[offset * GRID_W : (offset + 1) * GRID_W, pair * LANES : (pair + 1) * LANES] = (
                jnp.where(inside, skewed * log2e, masked_score)
            )


def bias_table(offset_bias):
    heads = offset_bias.shape[0]
    pairs = heads // 2
    flipped = jnp.flip(offset_bias, axis=2).reshape(pairs, 2, ROW_OFFSETS, COL_OFFSETS)
    even, odd = flipped[:, 0], flipped[:, 1]
    gap = jnp.zeros((pairs, ROW_OFFSETS, GRID_W - COL_OFFSETS), f32)
    lines = jnp.concatenate(
        [even[..., WIN_COLS - 1 :], gap, odd, gap, even[..., : WIN_COLS - 1]], axis=-1
    )
    return call(
        bias_kernel,
        jax.ShapeDtypeStruct((ROW_OFFSETS * GRID_W, heads * HEAD_DIM), f32),
        in_specs=[whole()],
        out_specs=whole(),
    )(jnp.transpose(lines, (1, 0, 2)))


def modulators(tp, pieces, gain_ref, scale_row, shift_row, a_ref, b_ref):
    width = pieces[0].shape[1]
    count = len(pieces)
    for step, piece in enumerate(pieces):
        owner = lax.rem(tp - step + count, count)
        part = pl.ds(pl.multiple_of(owner * width, LANES), width)
        a_ref[:, part] = gain_ref[:, part].astype(f32) * (1.0 + piece[scale_row : scale_row + 1, :])
        b_ref[:, part] = piece[shift_row : shift_row + 1, :]


def modulated(x_ref, a_ref, b_ref):
    values = x_ref[...].astype(f32)
    inverse = lax.rsqrt(jnp.mean(values * values, axis=-1, keepdims=True) + epsilon)
    return ((values * inverse) * a_ref[...] + b_ref[...]).astype(bf16)


def context_kernel(count, tp_ref, x_ref, gain_ref, wk_ref, wv_ref, *rest):
    pieces, (out_ref, a_ref, b_ref) = rest[:count], rest[count:]
    modulators(tp_ref[0], pieces, gain_ref, 3, 1, a_ref, b_ref)
    hidden = modulated(x_ref, a_ref, b_ref)
    out_ref[0] = jnp.dot(hidden, wk_ref[...], preferred_element_type=f32).astype(bf16)
    out_ref[1] = jnp.dot(hidden, wv_ref[...], preferred_element_type=f32).astype(bf16)


def context_pairs(tp_index, tokens, gain, wk, wv, pieces):
    width = tokens.shape[1]
    return call(
        functools.partial(context_kernel, len(pieces)),
        jax.ShapeDtypeStruct((2, tokens.shape[0], wk.shape[1]), bf16),
        in_specs=[whole(SMEM)] + [whole()] * (4 + len(pieces)),
        out_specs=whole(),
        scratch_shapes=[VMEM((1, width), f32), VMEM((1, width), f32)],
    )(tp_index, tokens, gain, wk, wv, *pieces)


def projection_kernel(count, tp_ref, x_ref, gain_ref, wq_ref, wk_ref, wv_ref, *rest):
    pieces = rest[:count]
    q_ref, k_ref, vt_ref, low_ref, high_ref, a_ref, b_ref = rest[count:]
    step = pl.program_id(0)

    @pl.when(step == 0)
    def _():
        modulators(tp_ref[0], pieces, gain_ref, 2, 0, a_ref, b_ref)

    hidden = modulated(x_ref, a_ref, b_ref)
    queries = jnp.dot(hidden, wq_ref[...], preferred_element_type=f32)
    q_ref[...] = (queries * (log2e * HEAD_DIM ** (-0.5))).astype(bf16)
    keys = jnp.dot(hidden, wk_ref[...], preferred_element_type=f32).astype(bf16)
    values = jnp.dot(hidden, wv_ref[...], preferred_element_type=f32).T.astype(bf16)
    k_ref[...] = keys
    vt_ref[...] = values

    @pl.when(step == 0)
    def _():
        low_ref[0] = keys
        low_ref[1] = values.T

    @pl.when(step == pl.num_programs(0) - 1)
    def _():
        high_ref[0] = keys
        high_ref[1] = values.T


def projections(tp_index, latent, gain, wq, wk, wv, pieces):
    tokens, width = latent.shape
    out = wq.shape[1]
    tile = WIN_ROWS // 2 * GRID_W
    resident = lambda shape: pl.BlockSpec(shape, lambda i: (0,) * len(shape))
    single = lambda shape: pl.BlockSpec(
        shape, lambda i: (0,) * len(shape), pipeline_mode=pl.Buffered(1)
    )
    return call(
        functools.partial(projection_kernel, len(pieces)),
        (
            jax.ShapeDtypeStruct((tokens, out), bf16),
            jax.ShapeDtypeStruct((tokens, out), bf16),
            jax.ShapeDtypeStruct((out, tokens), bf16),
            jax.ShapeDtypeStruct((2, tile, out), bf16),
            jax.ShapeDtypeStruct((2, tile, out), bf16),
        ),
        grid=(tokens // tile,),
        in_specs=[
            whole(SMEM),
            pl.BlockSpec((tile, width), lambda i: (i, 0)),
            single((1, width)),
            single(wq.shape),
            single(wk.shape),
            single(wv.shape),
        ]
        + [single(piece.shape) for piece in pieces],
        out_specs=(
            pl.BlockSpec((tile, out), lambda i: (i, 0)),
            pl.BlockSpec((tile, out), lambda i: (i, 0)),
            pl.BlockSpec((out, tile), lambda i: (0, i)),
            resident((2, tile, out)),
            resident((2, tile, out)),
        ),
        scratch_shapes=[VMEM((1, width), f32), VMEM((1, width), f32)],
    )(tp_index, latent, gain, wq, wk, wv, *pieces)


def attention_kernel(count, sp_count, sp_ref, q_ref, k_ref, vt_ref, low_ref, high_ref, t_ref, *rest):
    contexts = rest[:count]
    out_ref, kp_ref, vte_ref, vto_ref, kc_ref, vc_ref = rest[count : count + 6]
    scores = rest[count + 6 : count + 8]
    probs = rest[count + 8 : count + 10]
    tokens, width = q_ref.shape
    heads = width // HEAD_DIM
    grid_rows = tokens // GRID_W
    halo_rows = WIN_ROWS // 2
    halo = halo_rows * GRID_W
    near = WIN_ROWS * GRID_W
    padded = tokens + 2 * halo
    context = contexts[0].shape[1]

    kp_ref[0:halo, :] = low_ref[0]
    kp_ref[halo : halo + tokens, :] = k_ref[...]
    kp_ref[halo + tokens :, :] = high_ref[0]
    vte_ref[0:width, 0:halo] = low_ref[1].T
    vte_ref[0:width, halo : halo + tokens] = vt_ref[...]
    vte_ref[0:width, halo + tokens :] = high_ref[1].T
    ones = jnp.ones((16, padded), bf16)
    vte_ref[width:, :] = ones
    vto_ref[width:, :] = ones
    vto_ref[0:width, 0 : padded - LANES] = jnp.concatenate(
        [
            vte_ref[0:width, GRID_W : padded - LANES],
            vte_ref[0:width, padded - LANES : padded - LANES + GRID_W],
        ],
        axis=1,
    )
    for index, ref in enumerate(contexts):
        kc_ref[index * context : (index + 1) * context, :] = ref[0]
    vc_ref[0:width, :] = jnp.concatenate([ref[1] for ref in contexts], axis=0).T
    vc_ref[width:, :] = jnp.ones((16, vc_ref.shape[1]), bf16)

    lane_head = lax.broadcasted_iota(jnp.int32, (1, width), 1) // HEAD_DIM
    head_mask = [(lane_head == h).astype(f32).astype(bf16) for h in range(heads)]
    lower = lax.broadcasted_iota(jnp.int32, (HEAD_DIM, LANES), 1) < GRID_W
    sp = sp_ref[0]
    total_rows = grid_rows * sp_count

    def attend(row, s_ref, p_ref):
        global_row = sp * grid_rows + row
        first = jnp.clip(global_row - halo_rows, 0, total_rows - WIN_ROWS)
        start = first - sp * grid_rows + halo_rows
        offset = first - global_row + WIN_ROWS - 1
        q = q_ref[pl.ds(pl.multiple_of(row * GRID_W, GRID_W), GRID_W), :]
        big = jnp.concatenate([q * mask for mask in head_mask], axis=0)
        keys = kp_ref[pl.ds(pl.multiple_of(start * GRID_W, GRID_W), near), :]
        dims = (((1,), (1,)), ((), ()))
        near_scores = lax.dot_general(keys, big, dims, preferred_element_type=f32)
        near_scores += t_ref[pl.ds(pl.multiple_of(offset * GRID_W, GRID_W), near), :]
        far_scores = lax.dot_general(kc_ref[...], big, dims, preferred_element_type=f32)
        s_ref[0:near, :] = near_scores
        s_ref[near:, :] = far_scores
        peak = jnp.maximum(
            jnp.max(near_scores, axis=0, keepdims=True), jnp.max(far_scores, axis=0, keepdims=True)
        )
        p_ref[...] = jnp.exp2(s_ref[...] - peak).astype(bf16)
        pair = start // 2
        lanes = pl.ds(pl.multiple_of(pair * LANES, LANES), near)
        values = jnp.where(start % 2 == 0, vte_ref[:, lanes], vto_ref[:, lanes])
        out = jnp.dot(values, p_ref[0:near, :], preferred_element_type=f32)
        out += jnp.dot(vc_ref[...], p_ref[near:, :], preferred_element_type=f32)
        return out[0:width] * (1.0 / out[width : width + 1])

    def rows_pair(index, carry):
        left = attend(2 * index, scores[0], probs[0])
        right = attend(2 * index + 1, scores[1], probs[1])
        lanes = pl.ds(pl.multiple_of(index * LANES, LANES), LANES)
        for pair in range(heads // 2):
            cols = slice(pair * LANES, (pair + 1) * LANES)
            for half in range(2):
                rows = slice(pair * LANES + half * HEAD_DIM, pair * LANES + (half + 1) * HEAD_DIM)
                a, b = left[rows, cols], right[rows, cols]
                if half == 0:
                    b = pltpu.roll(b, GRID_W, 1)
                else:
                    a = pltpu.roll(a, GRID_W, 1)
                out_ref[rows, lanes] = jnp.where(lower, a, b).astype(bf16)
        return carry

    lax.fori_loop(0, grid_rows // 2, rows_pair, 0)


def attention(sp_index, queries, keys, values_t, low, high, table, contexts):
    tokens, width = queries.shape
    halo = WIN_ROWS // 2 * GRID_W
    padded = tokens + 2 * halo
    count = len(contexts)
    far = count * contexts[0].shape[1]
    total = WIN_ROWS * GRID_W + far
    return call(
        functools.partial(attention_kernel, count, lax.axis_size("sp")),
        jax.ShapeDtypeStruct((width, tokens), bf16),
        in_specs=[whole(SMEM)] + [whole()] * (6 + count),
        out_specs=whole(),
        scratch_shapes=[
            VMEM((padded, width), bf16),
            VMEM((width + 16, padded), bf16),
            VMEM((width + 16, padded), bf16),
            VMEM((far, width), bf16),
            VMEM((width + 16, far), bf16),
            VMEM((total, width), f32),
            VMEM((total, width), f32),
            VMEM((total, width), bf16),
            VMEM((total, width), bf16),
        ],
    )(sp_index, queries, keys, values_t, low, high, table, *contexts)


def output_kernel(count, tp_ref, x_ref, w_ref, *rest):
    blocks, pieces, out_ref = rest[:count], rest[count : 2 * count], rest[2 * count]
    tp = tp_ref[0]
    step = pl.program_id(0)
    height = blocks[0].shape[0]
    dims = (((0,), (0,)), ((), ()))
    total = None
    for index, block in enumerate(blocks):
        owner = lax.rem(tp - index + count, count)
        rows = pl.ds(pl.multiple_of(owner * height, height), height)
        term = lax.dot_general(block[...], w_ref[rows, :], dims, preferred_element_type=f32)
        total = term if total is None else total + term
    gate = jnp.zeros((1, out_ref.shape[1]), f32)
    for index, piece in enumerate(pieces):
        owner = lax.rem(tp - index + count, count)
        gate = jnp.where(owner == step, piece[4:5, :], gate)
    out_ref[...] = (x_ref[...].astype(f32) + gate * total).astype(bf16)


def output(tp_index, latent, weight, blocks, pieces):
    tokens, width = latent.shape
    count = len(blocks)
    share = tokens // count
    tile = width // count
    grid_spec = pltpu.PrefetchScalarGridSpec(
        num_scalar_prefetch=1,
        grid=(count,),
        in_specs=[
            pl.BlockSpec((share, tile), lambda i, tp: (tp[0], i)),
            pl.BlockSpec((weight.shape[0], tile), lambda i, tp: (0, i)),
        ]
        + [pl.BlockSpec(block.shape, lambda i, tp: (0, 0)) for block in blocks]
        + [pl.BlockSpec(piece.shape, lambda i, tp: (0, 0)) for piece in pieces],
        out_specs=pl.BlockSpec((share, tile), lambda i, tp: (0, i)),
    )
    return call(
        functools.partial(output_kernel, count),
        jax.ShapeDtypeStruct((share, width), bf16),
        grid_spec=grid_spec,
    )(tp_index, latent, weight, *blocks, *pieces)


def gathered(block, axis):
    return [block] + [shift_along(block, axis, step) for step in range(1, lax.axis_size(axis))]


def local(
    latent,
    condition,
    context_tokens,
    context_condition,
    shift_weight,
    scale_weight,
    gate_weight,
    norm_gain,
    query_weight,
    key_weight,
    value_weight,
    out_weight,
    offset_bias,
):
    sp_index = lax.axis_index("sp").astype(jnp.int32).reshape(1)
    tp_index = lax.axis_index("tp").astype(jnp.int32).reshape(1)
    tp_count = lax.axis_size("tp")
    gain = norm_gain.reshape(1, -1)
    terms = modulation_terms(
        sp_index, condition, context_condition, shift_weight, scale_weight, gate_weight
    )
    summed = functools.reduce(jnp.add, gathered(terms, "sp"))
    pieces = gathered(summed, "tp")
    table = bias_table(offset_bias)
    own_pairs = context_pairs(tp_index, context_tokens, gain, key_weight, value_weight, pieces)
    contexts = gathered(own_pairs, "sp")
    queries, keys, values_t, low, high = projections(
        tp_index, latent, gain, query_weight, key_weight, value_weight, pieces
    )
    count = lax.axis_size("sp")
    from_left = lax.ppermute(high, "sp", [(i, i + 1) for i in range(count - 1)])
    from_right = lax.ppermute(low, "sp", [(i + 1, i) for i in range(count - 1)])
    attended = attention(
        sp_index, queries, keys, values_t, from_left, from_right, table, contexts
    )
    share = latent.shape[0] // tp_count
    blocks = []
    for step in range(tp_count):
        target = lax.rem(tp_index[0] + step, tp_count)
        block = lax.dynamic_slice_in_dim(attended, target * share, share, 1)
        blocks.append(block if step == 0 else shift_along(block, "tp", step))
    return output(tp_index, latent, out_weight, blocks, pieces)


def solution(mesh):
    placed = (
        P(("grp", "sp"), None),
        P("grp"),
        P(("grp", "sp"), None),
        P(),
        P("sp", "tp"),
        P("sp", "tp"),
        P("sp", "tp"),
        P(),
        P(None, "tp"),
        P(None, "tp"),
        P(None, "tp"),
        P(),
        P("tp", None, None),
    )
    return jax.shard_map(
        local, mesh=mesh, in_specs=placed, out_specs=P(("grp", "sp", "tp"), None), check_vma=False
    )
```

```python
import functools
import math

import jax
import jax.numpy as jnp
from jax import lax
from jax.experimental import pallas as pl
from jax.experimental.pallas import tpu as pltpu
from jax.sharding import PartitionSpec as P

HEAD_DIM = 64
GRID_W = 64
WIN_ROWS = 8
WIN_COLS = 16
ROW_OFFSETS = 2 * WIN_ROWS - 1
COL_OFFSETS = 2 * WIN_COLS - 1
LANES = 128
HALO_ROWS = WIN_ROWS // 2
TILE = HALO_ROWS * GRID_W
NEAR = WIN_ROWS * GRID_W
ONES = 16

epsilon = 1e-06
masked_score = -1e30
log2e = math.log2(math.e)
SMEM = pltpu.SMEM
VMEM = pltpu.VMEM
f32 = jnp.float32
bf16 = jnp.bfloat16


def shift_along(block, axis, step):
    count = lax.axis_size(axis)
    return lax.ppermute(block, axis, [(i, (i + step) % count) for i in range(count)])


HBM = pltpu.HBM


def whole(memory_space=VMEM):
    return pl.BlockSpec(memory_space=memory_space)


def call(kernel, out_shape, *, vmem=16 << 20, flops=0, **kwargs):
    cost = pl.CostEstimate(flops=flops, transcendentals=0, bytes_accessed=0)
    return pl.pallas_call(
        kernel,
        out_shape=out_shape,
        compiler_params=pltpu.CompilerParams(vmem_limit_bytes=vmem),
        cost_estimate=cost if flops else None,
        **kwargs,
    )


def in_hbm(values):
    return [pltpu.with_memory_space_constraint(value, HBM) for value in values]


def array(shape, dtype=bf16):
    return jax.ShapeDtypeStruct(tuple(shape), dtype)


def modulation_kernel(sp_ref, tp_ref, gain_in_ref, *refs):
    inputs, (out_ref, spot_ref, gain_ref, cond_ref, ctx_ref, weights_ref, sems) = refs[:5], refs[5:]
    spot_ref[0] = sp_ref[0]
    spot_ref[1] = tp_ref[0]
    rows = weights_ref.shape[1]
    part = pl.ds(pl.multiple_of(sp_ref[0] * rows, LANES), rows)
    copies = [
        pltpu.make_async_copy(inputs[0].at[:, part], cond_ref, sems.at[0]),
        pltpu.make_async_copy(inputs[1].at[:, part], ctx_ref, sems.at[1]),
    ]
    copies += [
        pltpu.make_async_copy(inputs[2 + i], weights_ref.at[i], sems.at[2 + i]) for i in range(3)
    ]
    for copy in copies:
        copy.start()

    def act(ref):
        v = ref[...].astype(f32)
        return (v / (1.0 + jnp.exp(-v))).astype(bf16)

    copies[0].wait()
    copies[1].wait()
    both = jnp.concatenate([act(cond_ref), act(ctx_ref), jnp.zeros((14, rows), bf16)], axis=0)
    for index in range(3):
        copies[2 + index].wait()
        terms = jnp.dot(both, weights_ref[index], preferred_element_type=f32)
        out_ref[2 * index : 2 * index + 2, :] = terms[0:2]
    out_ref[6:8, :] = jnp.zeros_like(out_ref[6:8, :])
    gain_ref[...] = gain_in_ref[...].astype(f32)


def modulation_terms(sp_index, tp_index, gain, condition, context_condition, *weights):
    rows, width = weights[0].shape
    return call(
        modulation_kernel,
        [array((8, width), f32), array((2,), jnp.int32), array(gain.shape, f32)],
        in_specs=[whole(SMEM)] * 2 + [whole()] + [whole(HBM)] * 5,
        out_specs=[whole(), whole(SMEM), whole()],
        scratch_shapes=[
            VMEM((1, rows), bf16),
            VMEM((1, rows), bf16),
            VMEM((3, rows, width), bf16),
            pltpu.SemaphoreType.DMA((5,)),
        ],
    )(sp_index, tp_index, gain, *in_hbm((condition.reshape(1, -1), context_condition.reshape(1, -1), *weights)))


def sum_kernel(token_ref, *refs):
    total = refs[0][...]
    for ref in refs[1:-1]:
        total += ref[...]
    refs[-1][...] = total


def summed_terms(token, partials):
    return call(
        sum_kernel,
        array(partials[0].shape, f32),
        in_specs=[whole()] * (1 + len(partials)),
        out_specs=whole(),
    )(token, *partials)


def stage_kernel(token_ref, bias_ref, latent_ref, *refs):
    weights, targets = refs[:3], refs[3:-3]
    table_ref, lines_ref, sems = refs[-3:]
    tiles = len(targets) - 3
    sources = [latent_ref.at[i * TILE : (i + 1) * TILE] for i in range(tiles)]
    sources = [*sources[:1], *sources[-1:], *weights, *sources[1:-1]]
    targets = [targets[0], targets[tiles - 1], *targets[tiles:], *targets[1 : tiles - 1]]
    copies = [
        pltpu.make_async_copy(source, target, sems.at[index])
        for index, (source, target) in enumerate(zip(sources, targets))
    ]
    for copy in copies:
        copy.start()
    heads = bias_ref.shape[0]
    lane = lax.broadcasted_iota(jnp.int32, (ROW_OFFSETS + 1, LANES), 1)
    for head in range(heads):
        lines_ref[:, :] = jnp.zeros_like(lines_ref)
        lines_ref[0:ROW_OFFSETS, 0:COL_OFFSETS] = bias_ref[head] * log2e
        lines = lines_ref[...]
        first = pltpu.roll(lines, LANES - (WIN_COLS - 1), 1)
        second = pltpu.roll(lines, GRID_W - (WIN_COLS - 1), 1)
        for pair in range((ROW_OFFSETS + 1) // 2):
            line = first[2 * pair : 2 * pair + 1] + second[2 * pair + 1 : 2 * pair + 2]
            line = jnp.broadcast_to(line, (GRID_W, LANES))
            table_ref[head * GRID_W : (head + 1) * GRID_W, pair * LANES : (pair + 1) * LANES] = (
                pltpu.roll(line, 0, 1, stride=1, stride_axis=0)
            )
    for copy in copies:
        copy.wait()


def flip_kernel(token_ref, table_ref, out_ref):
    width = table_ref.shape[0]
    key = lax.broadcasted_iota(jnp.int32, (LANES, LANES), 0) % GRID_W
    query = lax.broadcasted_iota(jnp.int32, (LANES, LANES), 1) % GRID_W
    first = jnp.clip(query - WIN_COLS // 2, 0, GRID_W - WIN_COLS)
    inside = (key >= first) & (key < first + WIN_COLS)
    for row in range((ROW_OFFSETS + 1) // 2):
        for col in range(width // LANES):
            rows, cols = slice(row * LANES, (row + 1) * LANES), slice(col * LANES, (col + 1) * LANES)
            out_ref[rows, cols] = jnp.where(inside, table_ref[cols, rows].T, masked_score)


def staged(token, offset_bias, latent, *weights):
    heads = offset_bias.shape[0]
    rows = (ROW_OFFSETS + 1) * GRID_W
    tiles = latent.shape[0] // TILE
    sources = (latent, *weights)
    out = call(
        stage_kernel,
        [array((TILE, latent.shape[1]))] * tiles
        + [array(weight.shape) for weight in weights]
        + [array((heads * HEAD_DIM, rows), f32)],
        in_specs=[whole(), whole()] + [whole(HBM)] * len(sources),
        out_specs=[whole()] * (tiles + len(weights) + 1),
        scratch_shapes=[
            VMEM((ROW_OFFSETS + 1, LANES), f32),
            pltpu.SemaphoreType.DMA((tiles + len(weights),)),
        ],
        flops=5_000_000_000,
    )(token, offset_bias, *in_hbm(sources))
    return out[:tiles], out[tiles:-1], out[-1]


def bias_table(token, rows):
    return call(
        flip_kernel,
        array(rows.shape[::-1], f32),
        in_specs=[whole()] * 2,
        out_specs=whole(),
        flops=1_000_000_000,
    )(token, rows)


def modulators(tp, pieces, gain_ref, scale_row, shift_row, a_ref, b_ref):
    width = pieces[0].shape[1]
    count = len(pieces)
    for step, piece in enumerate(pieces):
        owner = lax.rem(tp - step + count, count)
        part = pl.ds(pl.multiple_of(owner * width, LANES), width)
        a_ref[:, part] = gain_ref[:, part] * (1.0 + piece[scale_row : scale_row + 1, :])
        b_ref[:, part] = piece[shift_row : shift_row + 1, :]


def modulated(x, a, b):
    values = x.astype(f32)
    inverse = lax.rsqrt(jnp.mean(values * values, axis=-1, keepdims=True) + epsilon)
    return ((values * inverse) * a + b).astype(bf16)


query_factor = log2e * HEAD_DIM ** (-0.5)


def edge_kernel(count, spot_ref, first_x_ref, last_x_ref, gain_ref, wq_ref, wk_ref, wv_ref, *rest):
    pieces = rest[:count]
    q_ref, low_ref, high_ref, a_ref, b_ref, first_ref, second_ref = rest[count:]
    modulators(spot_ref[1], pieces, gain_ref, 2, 0, a_ref, b_ref)
    scratch = (first_ref, second_ref)
    outs = (low_ref, high_ref)
    for x_ref, ref in zip((first_x_ref, last_x_ref), scratch):
        ref[...] = modulated(x_ref[...], a_ref[...], b_ref[...])
    for ref, out_ref in zip(scratch, outs):
        out_ref[0] = jnp.dot(ref[...], wk_ref[...], preferred_element_type=f32).astype(bf16)
        out_ref[1] = jnp.dot(ref[...], wv_ref[...], preferred_element_type=f32).astype(bf16)
    for index, ref in enumerate(scratch):
        queries = jnp.dot(ref[...], wq_ref[...], preferred_element_type=f32)
        q_ref[index * TILE : (index + 1) * TILE] = (queries * query_factor).astype(bf16)


def edge_projections(spot, first, last, gain, weights, pieces):
    width = first.shape[1]
    out = weights[0].shape[1]
    return call(
        functools.partial(edge_kernel, len(pieces)),
        [
            array((2 * TILE, out)),
            array((2, TILE, out)),
            array((2, TILE, out)),
            array((1, width), f32),
            array((1, width), f32),
        ],
        in_specs=[whole(SMEM)] + [whole()] * (6 + len(pieces)),
        out_specs=[whole()] * 5,
        scratch_shapes=[VMEM((TILE, width), bf16), VMEM((TILE, width), bf16)],
        flops=2_000_000_000,
    )(spot, first, last, gain, *weights, *pieces)


def main_kernel(count, spot_ref, a_ref, b_ref, gain_ref, wq_ref, wk_ref, wv_ref, qe_ref, low_ref, high_ref, *rest):
    inner, rest = rest[: count[2]], rest[count[2] :]
    contexts, pieces = rest[: count[0]], rest[count[0] : count[0] + count[1]]
    q_ref, k_ref, v_ref, kc_ref, vc_ref, ac_ref, bc_ref, *scratch = rest[sum(count[:2]) :]
    tokens, width = k_ref.shape
    tiles = tokens // TILE
    modulators(spot_ref[1], pieces, gain_ref, 3, 1, ac_ref, bc_ref)

    def load(index):
        ref = scratch[index % 2]
        if index < tiles - 1:
            ref[...] = modulated(inner[index - 1][...], a_ref[...], b_ref[...])
        else:
            height = contexts[0].shape[0]
            for part, context in enumerate(contexts):
                ref[part * height : (part + 1) * height] = modulated(
                    context[...], ac_ref[...], bc_ref[...]
                )

    def values_at(start, values):
        turned = values.T
        v_ref[0, 0:width, start : start + TILE] = turned.astype(bf16)
        rolled = pltpu.roll(turned, TILE - GRID_W, 1).astype(bf16)
        v_ref[1, 0:width, start : start + TILE - GRID_W] = rolled[:, 0 : TILE - GRID_W]
        if start:
            v_ref[1, 0:width, start - GRID_W : start] = rolled[:, TILE - GRID_W :]

    def multiply(index):
        hidden = scratch[index % 2][...]
        keys = jnp.dot(hidden, wk_ref[...], preferred_element_type=f32).astype(bf16)
        values = jnp.dot(hidden, wv_ref[...], preferred_element_type=f32)
        if index < tiles - 1:
            rows = slice(index * TILE, (index + 1) * TILE)
            queries = jnp.dot(hidden, wq_ref[...], preferred_element_type=f32)
            q_ref[rows] = (queries * query_factor).astype(bf16)
            k_ref[rows] = keys
            values_at(index * TILE, values)
        else:
            far = kc_ref.shape[0]
            kc_ref[...] = keys[0:far]
            vc_ref[0:width, :] = values[0:far].T.astype(bf16)

    load(1)
    q_ref[0:TILE] = qe_ref[0:TILE]
    q_ref[tokens - TILE :] = qe_ref[TILE:]
    k_ref[0:TILE] = low_ref[0]
    k_ref[tokens - TILE :] = high_ref[0]
    v_ref[0, width:, :] = jnp.ones((ONES, tokens), bf16)
    v_ref[1, width:, :] = jnp.ones((ONES, tokens), bf16)
    vc_ref[width:, :] = jnp.ones((ONES, vc_ref.shape[1]), bf16)
    values_at(0, low_ref[1].astype(f32))
    for index in range(1, tiles):
        if index + 1 < tiles:
            load(index + 1)
        multiply(index)
    values_at(tokens - TILE, high_ref[1].astype(f32))
    v_ref[1, 0:width, tokens - GRID_W :] = jnp.zeros((width, GRID_W), bf16)


def main_projections(spot, inner, a, b, gain, weights, edges, contexts, pieces):
    width = inner[0].shape[1]
    tokens = (len(inner) + 2) * TILE
    out = weights[0].shape[1]
    far = len(contexts) * contexts[0].shape[0]
    return call(
        functools.partial(main_kernel, (len(contexts), len(pieces), len(inner))),
        [
            array((tokens, out)),
            array((tokens, out)),
            array((2, out + ONES, tokens)),
            array((far, out)),
            array((out + ONES, far)),
        ],
        in_specs=[whole(SMEM)] + [whole()] * (9 + len(inner) + len(contexts) + len(pieces)),
        out_specs=[whole()] * 5,
        scratch_shapes=[
            VMEM((1, width), f32),
            VMEM((1, width), f32),
            VMEM((TILE, width), bf16),
            VMEM((TILE, width), bf16),
        ],
        flops=5_000_000_000,
    )(spot, a, b, gain, *weights, *edges, *inner, *contexts, *pieces)


def attend_rows(rows, q_ref, kc_ref, vc_ref, t_ref, out_ref, scores, probs):
    width = q_ref.shape[1]
    heads = width // HEAD_DIM
    lane_head = lax.broadcasted_iota(jnp.int32, (1, width), 1) // HEAD_DIM
    head_mask = [(lane_head == h).astype(f32).astype(bf16) for h in range(heads)]
    lower = lax.broadcasted_iota(jnp.int32, (HEAD_DIM, LANES), 1) < GRID_W
    dims = (((1,), (1,)), ((), ()))

    def score(index):
        row, k_ref, _, start, offset = rows[index]
        s_ref = scores[index % len(scores)]
        q = q_ref[row * GRID_W : (row + 1) * GRID_W, :]
        big = jnp.concatenate([q * mask for mask in head_mask], axis=0)
        keys = k_ref[part(start * GRID_W, GRID_W, NEAR), :]
        near = lax.dot_general(keys, big, dims, preferred_element_type=f32)
        near += t_ref[part(offset * GRID_W, GRID_W, NEAR), :]
        far = lax.dot_general(kc_ref[...], big, dims, preferred_element_type=f32)
        s_ref[0:NEAR, :] = near
        s_ref[NEAR:, :] = far
        return jnp.maximum(
            jnp.max(near, axis=0, keepdims=True), jnp.max(far, axis=0, keepdims=True)
        )

    def weigh(index, peak):
        s_ref, p_ref = scores[index % len(scores)], probs[index % len(probs)]
        p_ref[...] = jnp.exp2(s_ref[...] - peak).astype(bf16)

    def gather(index):
        _, _, v_ref, start, _ = rows[index]
        p_ref = probs[index % len(probs)]
        values = v_ref[start % 2, :, part(start // 2 * LANES, LANES, NEAR)]
        out = jnp.dot(values, p_ref[0:NEAR, :], preferred_element_type=f32)
        out += jnp.dot(vc_ref[...], p_ref[NEAR:, :], preferred_element_type=f32)
        return out[0:width] * (1.0 / out[width : width + 1])

    def store(index, left, right):
        row = rows[index][0]
        lanes = slice(row * GRID_W, row * GRID_W + LANES)
        for pair in range(heads // 2):
            cols = slice(pair * LANES, (pair + 1) * LANES)
            for half in range(2):
                at = slice(pair * LANES + half * HEAD_DIM, pair * LANES + (half + 1) * HEAD_DIM)
                a, b = left[at, cols], right[at, cols]
                if half == 0:
                    b = pltpu.roll(b, GRID_W, 1)
                else:
                    a = pltpu.roll(a, GRID_W, 1)
                out_ref[at, lanes] = jnp.where(lower, a, b).astype(bf16)

    peaks, outs = {}, {}
    for index in range(len(rows) + 2):
        if index < len(rows):
            peaks[index] = score(index)
        if 0 <= index - 1 < len(rows):
            weigh(index - 1, peaks.pop(index - 1))
        if 0 <= index - 2:
            outs[index - 2] = gather(index - 2)
            if (index - 2) % 2:
                store(index - 3, outs.pop(index - 3), outs.pop(index - 2))


def part(start, unit, size):
    if isinstance(start, int):
        return slice(start, start + size)
    return pl.ds(pl.multiple_of(start, unit), size)


def inner_kernel(q_ref, k_ref, v_ref, kc_ref, vc_ref, t_ref, out_ref, *scratch):
    grid_rows = q_ref.shape[0] // GRID_W
    rows = [
        (row, k_ref, v_ref, row - HALO_ROWS, WIN_ROWS - 1 - HALO_ROWS)
        for row in range(HALO_ROWS, grid_rows - HALO_ROWS)
    ]
    attend_rows(rows, q_ref, kc_ref, vc_ref, t_ref, out_ref, scratch[0:2], scratch[2:4])


def outer_kernel(sp_count, spot_ref, done_ref, latent_ref, weight_ref, q_ref, k_ref, v_ref, kc_ref, vc_ref, t_ref, low_ref, high_ref, out_ref, own_ref, held_ref, *rest):
    share, tp_count = own_ref.shape[0], q_ref.shape[0] // own_ref.shape[0]
    aligned = share % LANES == 0
    block_refs, rest = (rest[:tp_count], rest[tp_count:]) if aligned else ((), rest)
    sems, *scratch = rest
    copies = [
        pltpu.make_async_copy(weight_ref, held_ref, sems.at[0]),
        pltpu.make_async_copy(
            latent_ref.at[part(spot_ref[1] * share, GRID_W, share)], own_ref, sems.at[1]
        ),
    ]
    for copy in copies:
        copy.start()
    tokens, width = q_ref.shape
    grid_rows = tokens // GRID_W
    kl_ref, kh_ref, vl_ref, vh_ref = scratch[0:4]
    strip = 3 * TILE
    ones = jnp.ones((ONES, strip), bf16)
    kl_ref[0:TILE] = low_ref[0]
    kl_ref[TILE:] = k_ref[0 : 2 * TILE]
    kh_ref[0 : 2 * TILE] = k_ref[tokens - 2 * TILE :]
    kh_ref[2 * TILE :] = high_ref[0]
    low = low_ref[1].astype(f32).T
    high = high_ref[1].astype(f32).T
    for ref in (vl_ref, vh_ref):
        ref[0, width:, :] = ones
        ref[1, width:, :] = ones
    rolled = pltpu.roll(low, TILE - GRID_W, 1).astype(bf16)
    vl_ref[0, 0:width, 0:TILE] = low.astype(bf16)
    vl_ref[0, 0:width, TILE:] = v_ref[0, 0:width, 0 : 2 * TILE]
    vl_ref[1, 0:width, 0 : TILE - GRID_W] = rolled[:, 0 : TILE - GRID_W]
    first = pltpu.roll(v_ref[0, 0:width, 0:LANES].astype(f32), GRID_W, 1).astype(bf16)
    vl_ref[1, 0:width, TILE - GRID_W : TILE] = first[:, GRID_W:]
    vl_ref[1, 0:width, TILE:] = v_ref[1, 0:width, 0 : 2 * TILE]
    rolled = pltpu.roll(high, TILE - GRID_W, 1).astype(bf16)
    vh_ref[0, 0:width, 0 : 2 * TILE] = v_ref[0, 0:width, tokens - 2 * TILE :]
    vh_ref[0, 0:width, 2 * TILE :] = high.astype(bf16)
    vh_ref[1, 0:width, 0 : 2 * TILE] = v_ref[1, 0:width, tokens - 2 * TILE :]
    vh_ref[1, 0:width, 2 * TILE - GRID_W : 2 * TILE] = rolled[:, TILE - GRID_W :]
    vh_ref[1, 0:width, 2 * TILE : strip - GRID_W] = rolled[:, 0 : TILE - GRID_W]
    vh_ref[1, 0:width, strip - GRID_W :] = jnp.zeros((width, GRID_W), bf16)
    sp = spot_ref[0]
    total = grid_rows * sp_count
    rows = []
    for row in (*range(HALO_ROWS), *range(grid_rows - HALO_ROWS, grid_rows)):
        own = sp * grid_rows
        first = jnp.clip(own + row - HALO_ROWS, 0, total - WIN_ROWS)
        offset = first - (own + row) + WIN_ROWS - 1
        if row < HALO_ROWS:
            rows.append((row, kl_ref, vl_ref, first - own + HALO_ROWS, offset))
        else:
            rows.append((row, kh_ref, vh_ref, first - own - (grid_rows - WIN_ROWS), offset))
    attend_rows(rows, q_ref, kc_ref, vc_ref, t_ref, out_ref, scratch[4:6], scratch[6:8])
    for step, block_ref in enumerate(block_refs):
        target = lax.rem(spot_ref[1] + step, tp_count)
        block_ref[...] = out_ref[:, part(target * share, LANES, share)]
    for copy in copies:
        copy.wait()


def attention_scratch(total, width):
    return [VMEM((total, width), f32)] * 2 + [VMEM((total, width), bf16)] * 2


def inner_attention(queries, keys, values, far_keys, far_values, table):
    tokens, width = queries.shape
    return call(
        inner_kernel,
        array((width, tokens)),
        in_specs=[whole()] * 6,
        out_specs=whole(),
        scratch_shapes=attention_scratch(NEAR + far_keys.shape[0], width),
        flops=6_000_000_000,
    )(queries, keys, values, far_keys, far_values, table)


def outer_attention(spot, latent, weight, done, queries, keys, values, far_keys, far_values, table, low, high):
    tokens, width = queries.shape
    strip = 3 * TILE
    tp_count = lax.axis_size("tp")
    share = tokens // tp_count
    blocks = [array((width, share))] * (tp_count if share % LANES == 0 else 0)
    attended, own, held, *blocks = call(
        functools.partial(outer_kernel, lax.axis_size("sp")),
        [array((width, tokens)), array((share, latent.shape[1])), array(weight.shape), *blocks],
        in_specs=[whole(SMEM), whole()] + [whole(HBM)] * 2 + [whole()] * 8,
        out_specs=[whole()] * (3 + len(blocks)),
        input_output_aliases={1: 0},
        scratch_shapes=[pltpu.SemaphoreType.DMA((2,))]
        + [VMEM((strip, width), bf16)] * 2
        + [VMEM((2, width + ONES, strip), bf16)] * 2
        + attention_scratch(NEAR + far_keys.shape[0], width),
        flops=3_000_000_000,
    )(
        spot,
        done,
        *in_hbm((latent, weight)),
        queries,
        keys,
        values,
        far_keys,
        far_values,
        table,
        low,
        high,
    )
    if not blocks:
        for step in range(tp_count):
            target = lax.rem(spot[1] + step, tp_count)
            blocks.append(lax.dynamic_slice_in_dim(attended, target * share, share, 1))
    return own, held, blocks


def output_kernel(count, spot_ref, x_ref, w_ref, *rest):
    blocks, pieces = rest[:count], rest[count : 2 * count]
    out_ref, gate_ref = rest[2 * count :]
    tp = spot_ref[1]
    height, _ = blocks[0].shape
    dims = (((0,), (0,)), ((), ()))
    tile = w_ref.shape[1] // count
    for index, piece in enumerate(pieces):
        owner = lax.rem(tp - index + count, count)
        gate_ref[:, part(owner * tile, LANES, tile)] = piece[4:5, :]
    for step in range(count):
        cols = slice(step * tile, (step + 1) * tile)
        total = None
        for index, block in enumerate(blocks):
            owner = lax.rem(tp - index + count, count)
            weight = w_ref[part(owner * height, LANES, height), cols]
            term = lax.dot_general(block[...], weight, dims, preferred_element_type=f32)
            total = term if total is None else total + term
        out_ref[:, cols] = (x_ref[:, cols].astype(f32) + gate_ref[:, cols] * total).astype(bf16)


def output(spot, x, weight, blocks, pieces):
    count = len(blocks)
    share = x.shape[0]
    return call(
        functools.partial(output_kernel, count),
        array((share, x.shape[1])),
        in_specs=[whole(SMEM)] + [whole()] * (2 + 2 * count),
        out_specs=whole(),
        scratch_shapes=[VMEM((1, x.shape[1]), f32)],
        flops=2_000_000_000,
    )(spot, x, weight, *blocks, *pieces)


def gathered(block, axis):
    return [block] + [shift_along(block, axis, step) for step in range(1, lax.axis_size(axis))]


def local(
    latent,
    condition,
    context_tokens,
    context_condition,
    shift_weight,
    scale_weight,
    gate_weight,
    norm_gain,
    query_weight,
    key_weight,
    value_weight,
    out_weight,
    offset_bias,
):
    sp_index = lax.axis_index("sp").astype(jnp.int32).reshape(1)
    tp_index = lax.axis_index("tp").astype(jnp.int32).reshape(1)
    gain = norm_gain.reshape(1, -1)
    terms, spot, gain = modulation_terms(
        sp_index, tp_index, gain, condition, context_condition, shift_weight, scale_weight, gate_weight
    )
    partials = gathered(terms, "sp")
    tiles, weights, rows = staged(
        terms, offset_bias, latent, query_weight, key_weight, value_weight
    )
    summed = summed_terms(rows, partials)
    pieces = gathered(summed, "tp")
    table = bias_table(summed, rows)
    context_tokens, summed = lax.optimization_barrier((context_tokens, summed))
    contexts = gathered(context_tokens, "sp")
    *edges, a, b = edge_projections(spot, tiles[0], tiles[-1], gain, weights, pieces)
    count = lax.axis_size("sp")
    from_left = lax.ppermute(edges[2], "sp", [(i, i + 1) for i in range(count - 1)])
    from_right = lax.ppermute(edges[1], "sp", [(i + 1, i) for i in range(count - 1)])
    fields = main_projections(spot, tiles[1:-1], a, b, gain, weights, edges, contexts, pieces)
    inner = inner_attention(*fields, table)
    own, wo, blocks = outer_attention(
        spot, latent, out_weight, inner, *fields, table, from_left, from_right
    )
    received = blocks[:1] + [
        shift_along(block, "tp", step) for step, block in enumerate(blocks) if step
    ]
    return output(spot, own, wo, received, pieces)


def solution(mesh):
    placed = (
        P(("grp", "sp"), None),
        P("grp"),
        P(("grp", "sp"), None),
        P(),
        P("sp", "tp"),
        P("sp", "tp"),
        P("sp", "tp"),
        P(),
        P(None, "tp"),
        P(None, "tp"),
        P(None, "tp"),
        P(),
        P("tp", None, None),
    )
    return jax.shard_map(
        local, mesh=mesh, in_specs=placed, out_specs=P(("grp", "sp", "tp"), None), check_vma=False
    )
```

```python
import functools
import math

import jax
import jax.numpy as jnp
from jax import lax
from jax.experimental import pallas as pl
from jax.experimental.pallas import tpu as pltpu
from jax.sharding import PartitionSpec as P

HEAD_DIM = 64
GRID_W = 64
WIN_ROWS = 8
WIN_COLS = 16
ROW_OFFSETS = 2 * WIN_ROWS - 1
COL_OFFSETS = 2 * WIN_COLS - 1
LANES = 128
HALO_ROWS = WIN_ROWS // 2
TILE = HALO_ROWS * GRID_W
NEAR = WIN_ROWS * GRID_W
ONES = 16

epsilon = 1e-06
masked_score = -1e30
log2e = math.log2(math.e)
VMEM = pltpu.VMEM
f32 = jnp.float32
bf16 = jnp.bfloat16


def shift_along(block, axis, step):
    count = lax.axis_size(axis)
    return lax.ppermute(block, axis, [(i, (i + step) % count) for i in range(count)])


HBM = pltpu.HBM


def exchange(block, axis, step):
    count = lax.axis_size(axis)
    if count & (count - 1):
        return shift_along(block, axis, step)
    return lax.ppermute(block, axis, [(i, i ^ step) for i in range(count)])


def origin(axis, step):
    count = lax.axis_size(axis)
    index = lax.axis_index(axis)
    if count & (count - 1):
        return lax.rem(index - step + count, count)
    return jnp.bitwise_xor(index, step)


def target(axis, step):
    count = lax.axis_size(axis)
    index = lax.axis_index(axis)
    if count & (count - 1):
        return lax.rem(index + step, count)
    return jnp.bitwise_xor(index, step)


def whole(memory_space=VMEM):
    return pl.BlockSpec(memory_space=memory_space)


def call(kernel, out_shape, *, vmem=16 << 20, flops=0, **kwargs):
    cost = pl.CostEstimate(flops=flops, transcendentals=0, bytes_accessed=0)
    return pl.pallas_call(
        kernel,
        out_shape=out_shape,
        compiler_params=pltpu.CompilerParams(vmem_limit_bytes=vmem),
        cost_estimate=cost if flops else None,
        **kwargs,
    )


def in_hbm(values):
    return [pltpu.with_memory_space_constraint(value, HBM) for value in values]


def array(shape, dtype=bf16):
    return jax.ShapeDtypeStruct(tuple(shape), dtype)


def modulation_kernel(*refs):
    inputs, (out_ref, gain_ref, line_ref, cond_ref, ctx_ref, act_ref, weights_ref, sems) = refs[:6], refs[6:]
    rows = weights_ref.shape[1]
    mine = pl.ds(pl.multiple_of(lax.axis_index("sp") * rows, LANES), rows)
    targets = (cond_ref, ctx_ref, *(weights_ref.at[i] for i in range(3)), line_ref)
    copies = [
        pltpu.make_async_copy(source, target, sems.at[index])
        for index, (source, target) in enumerate(zip(inputs, targets))
    ]
    for copy in copies:
        copy.start()

    act_ref[...] = jnp.zeros_like(act_ref)
    for row, ref in enumerate((cond_ref, ctx_ref)):
        copies[row].wait()
        v = ref[...].reshape(1, -1).astype(f32)
        act_ref[row : row + 1, :] = v / (1.0 + jnp.exp(-v))
    both = act_ref[:, mine].astype(bf16)
    for index in range(3):
        copies[2 + index].wait()
        terms = jnp.dot(both, weights_ref[index], preferred_element_type=f32)
        out_ref[2 * index : 2 * index + 2, :] = terms[0:2]
    out_ref[6:8, :] = jnp.zeros_like(out_ref[6:8, :])
    copies[5].wait()
    gain_ref[...] = line_ref[...].reshape(gain_ref.shape).astype(f32)


def modulation_terms(condition, context_condition, *rest):
    rows, width = rest[0].shape
    whole_line = VMEM(condition.shape, bf16)
    return call(
        modulation_kernel,
        [array((8, width), f32), array((1, *rest[-1].shape), f32)],
        in_specs=[whole(HBM)] * 6,
        out_specs=[whole()] * 2,
        scratch_shapes=[
            whole_line,
            whole_line,
            whole_line,
            VMEM((16, *condition.shape), f32),
            VMEM((3, rows, width), bf16),
            pltpu.SemaphoreType.DMA((6,)),
        ],
    )(*in_hbm((condition, context_condition, *rest)))


def sum_kernel(token_ref, *refs):
    total = refs[0][...]
    for ref in refs[1:-1]:
        total += ref[...]
    refs[-1][...] = total


def summed_terms(token, partials):
    return call(
        sum_kernel,
        array(partials[0].shape, f32),
        in_specs=[whole()] * (1 + len(partials)),
        out_specs=whole(),
    )(token, *partials)


def rows_kernel(token_ref, source_ref, *refs):
    table_ref, bias_ref, lines_ref, sems = refs[-4:]
    count = (len(refs) - 4) // 2
    pairs = [(source_ref, bias_ref), *zip(refs[:count], refs[count:-4])]
    copies = [
        pltpu.make_async_copy(source, target, sems.at[index])
        for index, (source, target) in enumerate(pairs)
    ]
    for copy in copies:
        copy.start()
    copies[0].wait()
    heads = bias_ref.shape[1]
    for head in range(heads):
        lines_ref[:, :] = jnp.zeros_like(lines_ref)
        lines_ref[0:ROW_OFFSETS, 0:COL_OFFSETS] = bias_ref[:, head, :] * log2e
        lines = lines_ref[...]
        first = pltpu.roll(lines, LANES - (WIN_COLS - 1), 1)
        second = pltpu.roll(lines, GRID_W - (WIN_COLS - 1), 1)
        for pair in range((ROW_OFFSETS + 1) // 2):
            line = first[2 * pair : 2 * pair + 1] + second[2 * pair + 1 : 2 * pair + 2]
            line = jnp.broadcast_to(line, (GRID_W, LANES))
            table_ref[head * GRID_W : (head + 1) * GRID_W, pair * LANES : (pair + 1) * LANES] = (
                pltpu.roll(line, 0, 1, stride=1, stride_axis=0)
            )
    for copy in copies[1:]:
        copy.wait()


def bias_rows(token, offset_bias, *weights):
    heads = offset_bias.shape[0]
    rows = (ROW_OFFSETS + 1) * GRID_W
    return call(
        rows_kernel,
        [array(weight.shape) for weight in weights] + [array((heads * HEAD_DIM, rows), f32)],
        in_specs=[whole()] + [whole(HBM)] * (1 + len(weights)),
        out_specs=[whole()] * (1 + len(weights)),
        scratch_shapes=[
            VMEM((ROW_OFFSETS, heads, COL_OFFSETS), f32),
            VMEM((ROW_OFFSETS + 1, LANES), f32),
            pltpu.SemaphoreType.DMA((1 + len(weights),)),
        ],
        flops=500_000_000,
    )(token, *in_hbm((jnp.transpose(offset_bias, (1, 0, 2)), *weights)))


def flip_kernel(token_ref, table_ref, out_ref):
    width = table_ref.shape[0]
    key = lax.broadcasted_iota(jnp.int32, (LANES, LANES), 0) % GRID_W
    query = lax.broadcasted_iota(jnp.int32, (LANES, LANES), 1) % GRID_W
    first = jnp.clip(query - WIN_COLS // 2, 0, GRID_W - WIN_COLS)
    inside = (key >= first) & (key < first + WIN_COLS)
    for row in range((ROW_OFFSETS + 1) // 2):
        for col in range(width // LANES):
            rows, cols = slice(row * LANES, (row + 1) * LANES), slice(col * LANES, (col + 1) * LANES)
            out_ref[rows, cols] = jnp.where(inside, table_ref[cols, rows].T, masked_score)


def bias_table(token, rows):
    return call(
        flip_kernel,
        array(rows.shape[::-1], f32),
        in_specs=[whole()] * 2,
        out_specs=whole(),
        flops=1_000_000_000,
    )(token, rows)


def modulators(pieces, gain_ref, scale_row, shift_row, a_ref, b_ref):
    width = pieces[0].shape[1]
    for step, piece in enumerate(pieces):
        owner = origin("tp", step)
        part = pl.ds(pl.multiple_of(owner * width, LANES), width)
        a_ref[:, part] = gain_ref[:, part] * (1.0 + piece[scale_row : scale_row + 1, :])
        b_ref[:, part] = piece[shift_row : shift_row + 1, :]


def modulated(x, a, b):
    values = x.astype(f32)
    inverse = lax.rsqrt(jnp.mean(values * values, axis=-1, keepdims=True) + epsilon)
    return ((values * inverse) * a + b).astype(bf16)


query_factor = log2e * HEAD_DIM ** (-0.5)


def edge_kernel(count, x_ref, context_ref, gain_ref, wq_ref, wk_ref, wv_ref, *rest):
    pieces = rest[:count]
    q_ref, low_ref, high_ref, even_ref, odd_ref, far_ref, a_ref, b_ref, ac_ref, bc_ref, first_ref, second_ref = rest[count:]
    modulators(pieces, gain_ref, 3, 1, ac_ref, bc_ref)
    hidden = modulated(context_ref[...], ac_ref[...], bc_ref[...])
    far_ref[0] = jnp.dot(hidden, wk_ref[...], preferred_element_type=f32).astype(bf16)
    far_ref[1] = jnp.dot(hidden, wv_ref[...], preferred_element_type=f32).astype(bf16)
    modulators(pieces, gain_ref, 2, 0, a_ref, b_ref)
    scratch = (first_ref, second_ref)
    outs = (low_ref, high_ref)
    tokens = x_ref.shape[0]
    for start, ref in zip((0, tokens - TILE), scratch):
        ref[...] = modulated(x_ref[start : start + TILE], a_ref[...], b_ref[...])
    for ref, out_ref in zip(scratch, outs):
        out_ref[0] = jnp.dot(ref[...], wk_ref[...], preferred_element_type=f32).astype(bf16)
        out_ref[1] = jnp.dot(ref[...], wv_ref[...], preferred_element_type=f32).astype(bf16)
    even = lax.axis_index("sp") % 2 == 0
    even_ref[...] = jnp.where(even, high_ref[...], low_ref[...])
    odd_ref[...] = jnp.where(even, low_ref[...], high_ref[...])
    for index, ref in enumerate(scratch):
        queries = jnp.dot(ref[...], wq_ref[...], preferred_element_type=f32)
        q_ref[index * TILE : (index + 1) * TILE] = (queries * query_factor).astype(bf16)


def edge_projections(latent, context, gain, weights, pieces):
    width = latent.shape[1]
    out = weights[0].shape[1]
    return call(
        functools.partial(edge_kernel, len(pieces)),
        [
            array((2 * TILE, out)),
            *[array((2, TILE, out))] * 4,
            array((2, context.shape[0], out)),
            array((1, width), f32),
            array((1, width), f32),
        ],
        in_specs=[whole()] * (6 + len(pieces)),
        out_specs=[whole()] * 8,
        scratch_shapes=[
            VMEM((1, width), f32),
            VMEM((1, width), f32),
            VMEM((TILE, width), bf16),
            VMEM((TILE, width), bf16),
        ],
        flops=2_000_000_000,
    )(latent, context, gain, *weights, *pieces)


def main_kernel(x_ref, a_ref, b_ref, wq_ref, wk_ref, wv_ref, qe_ref, low_ref, high_ref, *rest):
    q_ref, k_ref, v_ref, *scratch = rest
    tokens, width = k_ref.shape
    tiles = tokens // TILE

    def load(index):
        rows = slice(index * TILE, (index + 1) * TILE)
        scratch[index % 2][...] = modulated(x_ref[rows], a_ref[...], b_ref[...])

    def values_at(start, values):
        turned = values.T
        v_ref[0, 0:width, start : start + TILE] = turned.astype(bf16)
        rolled = pltpu.roll(turned, TILE - GRID_W, 1).astype(bf16)
        v_ref[1, 0:width, start : start + TILE - GRID_W] = rolled[:, 0 : TILE - GRID_W]
        if start:
            v_ref[1, 0:width, start - GRID_W : start] = rolled[:, TILE - GRID_W :]

    def multiply(index):
        hidden = scratch[index % 2][...]
        keys = jnp.dot(hidden, wk_ref[...], preferred_element_type=f32).astype(bf16)
        values = jnp.dot(hidden, wv_ref[...], preferred_element_type=f32)
        rows = slice(index * TILE, (index + 1) * TILE)
        queries = jnp.dot(hidden, wq_ref[...], preferred_element_type=f32)
        q_ref[rows] = (queries * query_factor).astype(bf16)
        k_ref[rows] = keys
        values_at(index * TILE, values)

    load(1)
    q_ref[0:TILE] = qe_ref[0:TILE]
    q_ref[tokens - TILE :] = qe_ref[TILE:]
    k_ref[0:TILE] = low_ref[0]
    k_ref[tokens - TILE :] = high_ref[0]
    v_ref[0, width:, :] = jnp.ones((ONES, tokens), bf16)
    v_ref[1, width:, :] = jnp.ones((ONES, tokens), bf16)
    values_at(0, low_ref[1].astype(f32))
    for index in range(1, tiles - 1):
        if index + 2 < tiles:
            load(index + 1)
        multiply(index)
    values_at(tokens - TILE, high_ref[1].astype(f32))
    v_ref[1, 0:width, tokens - GRID_W :] = jnp.zeros((width, GRID_W), bf16)


def main_projections(latent, a, b, weights, edges):
    tokens, width = latent.shape
    out = weights[0].shape[1]
    return call(
        main_kernel,
        [array((tokens, out)), array((tokens, out)), array((2, out + ONES, tokens))],
        in_specs=[whole()] * 9,
        out_specs=[whole()] * 3,
        scratch_shapes=[VMEM((TILE, width), bf16), VMEM((TILE, width), bf16)],
        flops=5_000_000_000,
    )(latent, a, b, *weights, *edges)


def attend_rows(rows, q_ref, kc_ref, vc_ref, t_ref, out_ref, scores, probs):
    width = q_ref.shape[1]
    heads = width // HEAD_DIM
    lane_head = lax.broadcasted_iota(jnp.int32, (1, width), 1) // HEAD_DIM
    head_mask = [(lane_head == h).astype(f32).astype(bf16) for h in range(heads)]
    lower = lax.broadcasted_iota(jnp.int32, (HEAD_DIM, LANES), 1) < GRID_W
    dims = (((1,), (1,)), ((), ()))

    def score(index):
        row, k_ref, _, start, offset = rows[index]
        s_ref = scores[index % len(scores)]
        q = q_ref[row * GRID_W : (row + 1) * GRID_W, :]
        big = jnp.concatenate([q * mask for mask in head_mask], axis=0)
        keys = k_ref[part(start * GRID_W, GRID_W, NEAR), :]
        near = lax.dot_general(keys, big, dims, preferred_element_type=f32)
        near += t_ref[part(offset * GRID_W, GRID_W, NEAR), :]
        far = lax.dot_general(kc_ref[...], big, dims, preferred_element_type=f32)
        s_ref[0:NEAR, :] = near
        s_ref[NEAR:, :] = far
        return jnp.maximum(
            jnp.max(near, axis=0, keepdims=True), jnp.max(far, axis=0, keepdims=True)
        )

    def weigh(index, peak):
        s_ref, p_ref = scores[index % len(scores)], probs[index % len(probs)]
        p_ref[...] = jnp.exp2(s_ref[...] - peak).astype(bf16)

    def gather(index):
        _, _, v_ref, start, _ = rows[index]
        p_ref = probs[index % len(probs)]
        values = v_ref[start % 2, :, part(start // 2 * LANES, LANES, NEAR)]
        out = jnp.dot(values, p_ref[0:NEAR, :], preferred_element_type=f32)
        out += jnp.dot(vc_ref[...], p_ref[NEAR:, :], preferred_element_type=f32)
        return out[0:width] * (1.0 / out[width : width + 1])

    def store(index, left, right):
        row = rows[index][0]
        lanes = slice(row * GRID_W, row * GRID_W + LANES)
        for pair in range(heads // 2):
            cols = slice(pair * LANES, (pair + 1) * LANES)
            for half in range(2):
                at = slice(pair * LANES + half * HEAD_DIM, pair * LANES + (half + 1) * HEAD_DIM)
                a, b = left[at, cols], right[at, cols]
                if half == 0:
                    b = pltpu.roll(b, GRID_W, 1)
                else:
                    a = pltpu.roll(a, GRID_W, 1)
                out_ref[at, lanes] = jnp.where(lower, a, b).astype(bf16)

    peaks, outs = {}, {}
    for index in range(len(rows) + 2):
        if index < len(rows):
            peaks[index] = score(index)
        if 0 <= index - 1 < len(rows):
            weigh(index - 1, peaks.pop(index - 1))
        if 0 <= index - 2:
            outs[index - 2] = gather(index - 2)
            if (index - 2) % 2:
                store(index - 3, outs.pop(index - 3), outs.pop(index - 2))


def part(start, unit, size):
    if isinstance(start, int):
        return slice(start, start + size)
    return pl.ds(pl.multiple_of(start, unit), size)


def inner_kernel(count, q_ref, k_ref, v_ref, t_ref, *rest):
    contexts, (out_ref, kc_ref, vc_ref, *scratch) = rest[:count], rest[count:]
    width = q_ref.shape[1]
    grid_rows = q_ref.shape[0] // GRID_W
    height = contexts[0].shape[1]
    for index, context in enumerate(contexts):
        kc_ref[index * height : (index + 1) * height] = context[0]
    far_values = jnp.concatenate([context[1] for context in contexts], axis=0)
    vc_ref[0:width, :] = far_values.astype(f32).T.astype(bf16)
    vc_ref[width:, :] = jnp.ones((ONES, vc_ref.shape[1]), bf16)
    rows = [
        (row, k_ref, v_ref, row - HALO_ROWS, WIN_ROWS - 1 - HALO_ROWS)
        for row in range(HALO_ROWS, grid_rows - HALO_ROWS)
    ]
    attend_rows(rows, q_ref, kc_ref, vc_ref, t_ref, out_ref, scratch[0:2], scratch[2:4])


def outer_kernel(sp_count, done_ref, latent_ref, weight_ref, q_ref, k_ref, v_ref, kc_ref, vc_ref, t_ref, first_ref, second_ref, out_ref, own_ref, held_ref, *rest):
    share, tp_count = own_ref.shape[0], q_ref.shape[0] // own_ref.shape[0]
    aligned = share % LANES == 0
    block_refs, rest = (rest[:tp_count], rest[tp_count:]) if aligned else ((), rest)
    sems, *scratch = rest
    copies = [
        pltpu.make_async_copy(weight_ref, held_ref, sems.at[0]),
        pltpu.make_async_copy(
            latent_ref.at[part(lax.axis_index("tp") * share, GRID_W, share)], own_ref, sems.at[1]
        ),
    ]
    for copy in copies:
        copy.start()
    tokens, width = q_ref.shape
    grid_rows = tokens // GRID_W
    kl_ref, kh_ref, vl_ref, vh_ref = scratch[0:4]
    strip = 3 * TILE
    ones = jnp.ones((ONES, strip), bf16)
    even = lax.axis_index("sp") % 2 == 0
    low_halo = jnp.where(even, second_ref[...], first_ref[...])
    high_halo = jnp.where(even, first_ref[...], second_ref[...])
    kl_ref[0:TILE] = low_halo[0]
    kl_ref[TILE:] = k_ref[0 : 2 * TILE]
    kh_ref[0 : 2 * TILE] = k_ref[tokens - 2 * TILE :]
    kh_ref[2 * TILE :] = high_halo[0]
    low = low_halo[1].astype(f32).T
    high = high_halo[1].astype(f32).T
    for ref in (vl_ref, vh_ref):
        ref[0, width:, :] = ones
        ref[1, width:, :] = ones
    rolled = pltpu.roll(low, TILE - GRID_W, 1).astype(bf16)
    vl_ref[0, 0:width, 0:TILE] = low.astype(bf16)
    vl_ref[0, 0:width, TILE:] = v_ref[0, 0:width, 0 : 2 * TILE]
    vl_ref[1, 0:width, 0 : TILE - GRID_W] = rolled[:, 0 : TILE - GRID_W]
    first = pltpu.roll(v_ref[0, 0:width, 0:LANES].astype(f32), GRID_W, 1).astype(bf16)
    vl_ref[1, 0:width, TILE - GRID_W : TILE] = first[:, GRID_W:]
    vl_ref[1, 0:width, TILE:] = v_ref[1, 0:width, 0 : 2 * TILE]
    rolled = pltpu.roll(high, TILE - GRID_W, 1).astype(bf16)
    vh_ref[0, 0:width, 0 : 2 * TILE] = v_ref[0, 0:width, tokens - 2 * TILE :]
    vh_ref[0, 0:width, 2 * TILE :] = high.astype(bf16)
    vh_ref[1, 0:width, 0 : 2 * TILE] = v_ref[1, 0:width, tokens - 2 * TILE :]
    vh_ref[1, 0:width, 2 * TILE - GRID_W : 2 * TILE] = rolled[:, TILE - GRID_W :]
    vh_ref[1, 0:width, 2 * TILE : strip - GRID_W] = rolled[:, 0 : TILE - GRID_W]
    vh_ref[1, 0:width, strip - GRID_W :] = jnp.zeros((width, GRID_W), bf16)
    sp = lax.axis_index("sp")
    total = grid_rows * sp_count
    rows = []
    for row in (*range(HALO_ROWS), *range(grid_rows - HALO_ROWS, grid_rows)):
        own = sp * grid_rows
        first = jnp.clip(own + row - HALO_ROWS, 0, total - WIN_ROWS)
        offset = first - (own + row) + WIN_ROWS - 1
        if row < HALO_ROWS:
            rows.append((row, kl_ref, vl_ref, first - own + HALO_ROWS, offset))
        else:
            rows.append((row, kh_ref, vh_ref, first - own - (grid_rows - WIN_ROWS), offset))
    attend_rows(rows, q_ref, kc_ref, vc_ref, t_ref, out_ref, scratch[4:6], scratch[6:8])
    for step, block_ref in enumerate(block_refs):
        block_ref[...] = out_ref[:, part(target("tp", step) * share, LANES, share)]
    for copy in copies:
        copy.wait()


def attention_scratch(total, width):
    return [VMEM((total, width), f32)] * 2 + [VMEM((total, width), bf16)] * 2


def inner_attention(queries, keys, values, table, contexts):
    tokens, width = queries.shape
    far = len(contexts) * contexts[0].shape[1]
    return call(
        functools.partial(inner_kernel, len(contexts)),
        [array((width, tokens)), array((far, width)), array((width + ONES, far))],
        in_specs=[whole()] * (4 + len(contexts)),
        out_specs=[whole()] * 3,
        scratch_shapes=attention_scratch(NEAR + far, width),
        flops=6_000_000_000,
    )(queries, keys, values, table, *contexts)


def outer_attention(latent, weight, done, queries, keys, values, far_keys, far_values, table, low, high):
    tokens, width = queries.shape
    strip = 3 * TILE
    tp_count = lax.axis_size("tp")
    share = tokens // tp_count
    blocks = [array((width, share))] * (tp_count if share % LANES == 0 else 0)
    attended, own, held, *blocks = call(
        functools.partial(outer_kernel, lax.axis_size("sp")),
        [array((width, tokens)), array((share, latent.shape[1])), array(weight.shape), *blocks],
        in_specs=[whole()] + [whole(HBM)] * 2 + [whole()] * 8,
        out_specs=[whole()] * (3 + len(blocks)),
        input_output_aliases={0: 0},
        scratch_shapes=[pltpu.SemaphoreType.DMA((2,))]
        + [VMEM((strip, width), bf16)] * 2
        + [VMEM((2, width + ONES, strip), bf16)] * 2
        + attention_scratch(NEAR + far_keys.shape[0], width),
        flops=3_000_000_000,
    )(
        done,
        *in_hbm((latent, weight)),
        queries,
        keys,
        values,
        far_keys,
        far_values,
        table,
        low,
        high,
    )
    if not blocks:
        for step in range(tp_count):
            start = target("tp", step) * share
            blocks.append(lax.dynamic_slice_in_dim(attended, start, share, 1))
    return own, held, blocks


def output_kernel(count, x_ref, w_ref, *rest):
    blocks, pieces = rest[:count], rest[count : 2 * count]
    out_ref, gate_ref = rest[2 * count :]
    height, _ = blocks[0].shape
    dims = (((0,), (0,)), ((), ()))
    tile = w_ref.shape[1] // count
    for index, piece in enumerate(pieces):
        owner = origin("tp", index)
        gate_ref[:, part(owner * tile, LANES, tile)] = piece[4:5, :]
    for step in range(count):
        cols = slice(step * tile, (step + 1) * tile)
        total = None
        for index, block in enumerate(blocks):
            owner = origin("tp", index)
            weight = w_ref[part(owner * height, LANES, height), cols]
            term = lax.dot_general(block[...], weight, dims, preferred_element_type=f32)
            total = term if total is None else total + term
        out_ref[:, cols] = (x_ref[:, cols].astype(f32) + gate_ref[:, cols] * total).astype(bf16)


def output(x, weight, blocks, pieces):
    count = len(blocks)
    share = x.shape[0]
    return call(
        functools.partial(output_kernel, count),
        array((share, x.shape[1])),
        in_specs=[whole()] * (2 + 2 * count),
        out_specs=whole(),
        scratch_shapes=[VMEM((1, x.shape[1]), f32)],
        flops=2_000_000_000,
    )(x, weight, *blocks, *pieces)


def gathered(block, axis):
    return [block] + [exchange(block, axis, step) for step in range(1, lax.axis_size(axis))]


def local(
    latent,
    condition,
    context_tokens,
    context_condition,
    shift_weight,
    scale_weight,
    gate_weight,
    norm_gain,
    query_weight,
    key_weight,
    value_weight,
    out_weight,
    offset_bias,
):
    terms, gain = modulation_terms(
        condition, context_condition, shift_weight, scale_weight, gate_weight, norm_gain
    )
    partials = gathered(terms, "sp")
    *weights, rows = bias_rows(terms, offset_bias, query_weight, key_weight, value_weight)
    summed = summed_terms(rows, partials)
    pieces = gathered(summed, "tp")
    table = bias_table(summed, rows)
    *edges, far, a, b = edge_projections(
        latent, context_tokens, gain, weights, pieces
    )
    count = lax.axis_size("sp")
    contexts = gathered(far, "sp")
    pairs = [(i, i ^ 1) for i in range(count) if i ^ 1 < count]
    first = lax.ppermute(edges[3], "sp", pairs)
    pairs = [(i, j) for i in range(count) for j in [((i + 1) ^ 1) - 1] if 0 <= j < count]
    second = lax.ppermute(edges[4], "sp", pairs)
    fields = main_projections(latent, a, b, weights, edges[:3])
    inner, *fars = inner_attention(*fields, table, contexts)
    own, wo, blocks = outer_attention(
        latent, out_weight, inner, *fields, *fars, table, first, second
    )
    received = blocks[:1] + [
        exchange(block, "tp", step) for step, block in enumerate(blocks) if step
    ]
    return output(own, wo, received, pieces)


def solution(mesh):
    placed = (
        P(("grp", "sp"), None),
        P("grp"),
        P(("grp", "sp"), None),
        P(),
        P("sp", "tp"),
        P("sp", "tp"),
        P("sp", "tp"),
        P(),
        P(None, "tp"),
        P(None, "tp"),
        P(None, "tp"),
        P(),
        P("tp", None, None),
    )
    return jax.shard_map(
        local, mesh=mesh, in_specs=placed, out_specs=P(("grp", "sp", "tp"), None), check_vma=False
    )
```

```python
import functools
import math

import jax
import jax.numpy as jnp
from jax import lax
from jax.experimental import pallas as pl
from jax.experimental.pallas import tpu as pltpu
from jax.sharding import PartitionSpec as P

HEAD_DIM = 64
GRID_W = 64
WIN_ROWS = 8
WIN_COLS = 16
ROW_OFFSETS = 2 * WIN_ROWS - 1
COL_OFFSETS = 2 * WIN_COLS - 1
LANES = 128
HALO_ROWS = WIN_ROWS // 2
TILE = HALO_ROWS * GRID_W
NEAR = WIN_ROWS * GRID_W
ONES = 16

epsilon = 1e-06
masked_score = -1e30
log2e = math.log2(math.e)
VMEM = pltpu.VMEM
f32 = jnp.float32
bf16 = jnp.bfloat16


def shift_along(block, axis, step):
    count = lax.axis_size(axis)
    return lax.ppermute(block, axis, [(i, (i + step) % count) for i in range(count)])


HBM = pltpu.HBM


def exchange(block, axis, step):
    count = lax.axis_size(axis)
    if count & (count - 1):
        return shift_along(block, axis, step)
    return lax.ppermute(block, axis, [(i, i ^ step) for i in range(count)])


def origin(axis, step):
    count = lax.axis_size(axis)
    index = lax.axis_index(axis)
    if count & (count - 1):
        return lax.rem(index - step + count, count)
    return jnp.bitwise_xor(index, step)


def target(axis, step):
    count = lax.axis_size(axis)
    index = lax.axis_index(axis)
    if count & (count - 1):
        return lax.rem(index + step, count)
    return jnp.bitwise_xor(index, step)


def whole(memory_space=VMEM):
    return pl.BlockSpec(memory_space=memory_space)


def call(kernel, out_shape, *, vmem=16 << 20, flops=0, **kwargs):
    cost = pl.CostEstimate(flops=flops, transcendentals=0, bytes_accessed=0)
    return pl.pallas_call(
        kernel,
        out_shape=out_shape,
        compiler_params=pltpu.CompilerParams(vmem_limit_bytes=vmem),
        cost_estimate=cost if flops else None,
        **kwargs,
    )


def in_hbm(values):
    return [pltpu.with_memory_space_constraint(value, HBM) for value in values]


def array(shape, dtype=bf16):
    return jax.ShapeDtypeStruct(tuple(shape), dtype)


def modulation_kernel(*refs):
    inputs, (out_ref, gain_ref, line_ref, cond_ref, ctx_ref, act_ref, weights_ref, sems) = refs[:6], refs[6:]
    rows = weights_ref.shape[1]
    mine = pl.ds(pl.multiple_of(lax.axis_index("sp") * rows, LANES), rows)
    targets = (cond_ref, ctx_ref, *(weights_ref.at[i] for i in range(3)), line_ref)
    copies = [
        pltpu.make_async_copy(source, target, sems.at[index])
        for index, (source, target) in enumerate(zip(inputs, targets))
    ]
    for copy in copies:
        copy.start()

    act_ref[...] = jnp.zeros_like(act_ref)
    for row, ref in enumerate((cond_ref, ctx_ref)):
        copies[row].wait()
        v = ref[...].reshape(1, -1).astype(f32)
        act_ref[row : row + 1, :] = v / (1.0 + jnp.exp(-v))
    both = act_ref[:, mine].astype(bf16)
    for index in range(3):
        copies[2 + index].wait()
        terms = jnp.dot(both, weights_ref[index], preferred_element_type=f32)
        out_ref[2 * index : 2 * index + 2, :] = terms[0:2]
    out_ref[6:8, :] = jnp.zeros_like(out_ref[6:8, :])
    copies[5].wait()
    gain_ref[...] = line_ref[...].reshape(gain_ref.shape).astype(f32)


def modulation_terms(condition, context_condition, *rest):
    rows, width = rest[0].shape
    whole_line = VMEM(condition.shape, bf16)
    return call(
        modulation_kernel,
        [array((8, width), f32), array((1, *rest[-1].shape), f32)],
        in_specs=[whole(HBM)] * 6,
        out_specs=[whole()] * 2,
        scratch_shapes=[
            whole_line,
            whole_line,
            whole_line,
            VMEM((16, *condition.shape), f32),
            VMEM((3, rows, width), bf16),
            pltpu.SemaphoreType.DMA((6,)),
        ],
    )(*in_hbm((condition, context_condition, *rest)))


def sum_kernel(token_ref, *refs):
    total = refs[0][...]
    for ref in refs[1:-1]:
        total += ref[...]
    refs[-1][...] = total


def summed_terms(token, partials):
    return call(
        sum_kernel,
        array(partials[0].shape, f32),
        in_specs=[whole()] * (1 + len(partials)),
        out_specs=whole(),
    )(token, *partials)


def rows_kernel(token_ref, source_ref, *refs):
    table_ref, bias_ref, lines_ref, sems = refs[-4:]
    count = (len(refs) - 4) // 2
    pairs = [(source_ref, bias_ref), *zip(refs[:count], refs[count:-4])]
    copies = [
        pltpu.make_async_copy(source, target, sems.at[index])
        for index, (source, target) in enumerate(pairs)
    ]
    for copy in copies:
        copy.start()
    copies[0].wait()
    heads = bias_ref.shape[1]
    for head in range(heads):
        lines_ref[:, :] = jnp.zeros_like(lines_ref)
        lines_ref[0:ROW_OFFSETS, 0:COL_OFFSETS] = bias_ref[:, head, :] * log2e
        lines = lines_ref[...]
        first = pltpu.roll(lines, LANES - (WIN_COLS - 1), 1)
        second = pltpu.roll(lines, GRID_W - (WIN_COLS - 1), 1)
        for pair in range((ROW_OFFSETS + 1) // 2):
            line = first[2 * pair : 2 * pair + 1] + second[2 * pair + 1 : 2 * pair + 2]
            line = jnp.broadcast_to(line, (GRID_W, LANES))
            table_ref[head * GRID_W : (head + 1) * GRID_W, pair * LANES : (pair + 1) * LANES] = (
                pltpu.roll(line, 0, 1, stride=1, stride_axis=0)
            )
    for copy in copies[1:]:
        copy.wait()


def bias_rows(token, offset_bias, *weights):
    heads = offset_bias.shape[0]
    rows = (ROW_OFFSETS + 1) * GRID_W
    return call(
        rows_kernel,
        [array(weight.shape) for weight in weights] + [array((heads * HEAD_DIM, rows), f32)],
        in_specs=[whole()] + [whole(HBM)] * (1 + len(weights)),
        out_specs=[whole()] * (1 + len(weights)),
        scratch_shapes=[
            VMEM((ROW_OFFSETS, heads, COL_OFFSETS), f32),
            VMEM((ROW_OFFSETS + 1, LANES), f32),
            pltpu.SemaphoreType.DMA((1 + len(weights),)),
        ],
        flops=500_000_000,
    )(token, *in_hbm((jnp.transpose(offset_bias, (1, 0, 2)), *weights)))


def flip_kernel(token_ref, table_ref, out_ref):
    width = table_ref.shape[0]
    key = lax.broadcasted_iota(jnp.int32, (LANES, LANES), 0) % GRID_W
    query = lax.broadcasted_iota(jnp.int32, (LANES, LANES), 1) % GRID_W
    first = jnp.clip(query - WIN_COLS // 2, 0, GRID_W - WIN_COLS)
    inside = (key >= first) & (key < first + WIN_COLS)
    for row in range((ROW_OFFSETS + 1) // 2):
        for col in range(width // LANES):
            rows, cols = slice(row * LANES, (row + 1) * LANES), slice(col * LANES, (col + 1) * LANES)
            out_ref[rows, cols] = jnp.where(inside, table_ref[cols, rows].T, masked_score)


def bias_table(token, rows):
    return call(
        flip_kernel,
        array(rows.shape[::-1], f32),
        in_specs=[whole()] * 2,
        out_specs=whole(),
        flops=1_000_000_000,
    )(token, rows)


def modulators(pieces, gain_ref, scale_row, shift_row, a_ref, b_ref):
    width = pieces[0].shape[1]
    for step, piece in enumerate(pieces):
        owner = origin("tp", step)
        part = pl.ds(pl.multiple_of(owner * width, LANES), width)
        a_ref[:, part] = gain_ref[:, part] * (1.0 + piece[scale_row : scale_row + 1, :])
        b_ref[:, part] = piece[shift_row : shift_row + 1, :]


def modulated(x, a, b):
    values = x.astype(f32)
    inverse = lax.rsqrt(jnp.mean(values * values, axis=-1, keepdims=True) + epsilon)
    return ((values * inverse) * a + b).astype(bf16)


query_factor = log2e * HEAD_DIM ** (-0.5)


def edge_kernel(count, x_ref, context_ref, gain_ref, wq_ref, wk_ref, wv_ref, *rest):
    pieces = rest[:count]
    q_ref, low_ref, high_ref, even_ref, odd_ref, far_ref, a_ref, b_ref, ac_ref, bc_ref, first_ref, second_ref = rest[count:]
    modulators(pieces, gain_ref, 3, 1, ac_ref, bc_ref)
    hidden = modulated(context_ref[...], ac_ref[...], bc_ref[...])
    far_ref[0] = jnp.dot(hidden, wk_ref[...], preferred_element_type=f32).astype(bf16)
    far_ref[1] = jnp.dot(hidden, wv_ref[...], preferred_element_type=f32).astype(bf16)
    modulators(pieces, gain_ref, 2, 0, a_ref, b_ref)
    scratch = (first_ref, second_ref)
    outs = (low_ref, high_ref)
    tokens = x_ref.shape[0]
    for start, ref in zip((0, tokens - TILE), scratch):
        ref[...] = modulated(x_ref[start : start + TILE], a_ref[...], b_ref[...])
    for ref, out_ref in zip(scratch, outs):
        out_ref[0] = jnp.dot(ref[...], wk_ref[...], preferred_element_type=f32).astype(bf16)
        out_ref[1] = jnp.dot(ref[...], wv_ref[...], preferred_element_type=f32).astype(bf16)
    even = lax.axis_index("sp") % 2 == 0
    even_ref[...] = jnp.where(even, high_ref[...], low_ref[...])
    odd_ref[...] = jnp.where(even, low_ref[...], high_ref[...])
    for index, ref in enumerate(scratch):
        queries = jnp.dot(ref[...], wq_ref[...], preferred_element_type=f32)
        q_ref[index * TILE : (index + 1) * TILE] = (queries * query_factor).astype(bf16)


def edge_projections(latent, context, gain, weights, pieces):
    width = latent.shape[1]
    out = weights[0].shape[1]
    return call(
        functools.partial(edge_kernel, len(pieces)),
        [
            array((2 * TILE, out)),
            *[array((2, TILE, out))] * 4,
            array((2, context.shape[0], out)),
            array((1, width), f32),
            array((1, width), f32),
        ],
        in_specs=[whole()] * (6 + len(pieces)),
        out_specs=[whole()] * 8,
        scratch_shapes=[
            VMEM((1, width), f32),
            VMEM((1, width), f32),
            VMEM((TILE, width), bf16),
            VMEM((TILE, width), bf16),
        ],
        flops=2_000_000_000,
    )(latent, context, gain, *weights, *pieces)


def main_kernel(x_ref, a_ref, b_ref, wq_ref, wk_ref, wv_ref, qe_ref, low_ref, high_ref, *rest):
    q_ref, k_ref, v_ref, *scratch = rest
    tokens, width = k_ref.shape
    tiles = tokens // TILE

    def load(index):
        rows = slice(index * TILE, (index + 1) * TILE)
        scratch[index % 2][...] = modulated(x_ref[rows], a_ref[...], b_ref[...])

    def values_at(start, values):
        turned = values.T
        v_ref[0, 0:width, start : start + TILE] = turned.astype(bf16)
        rolled = pltpu.roll(turned, TILE - GRID_W, 1).astype(bf16)
        v_ref[1, 0:width, start : start + TILE - GRID_W] = rolled[:, 0 : TILE - GRID_W]
        if start:
            v_ref[1, 0:width, start - GRID_W : start] = rolled[:, TILE - GRID_W :]

    def multiply(index):
        hidden = scratch[index % 2][...]
        keys = jnp.dot(hidden, wk_ref[...], preferred_element_type=f32).astype(bf16)
        values = jnp.dot(hidden, wv_ref[...], preferred_element_type=f32)
        rows = slice(index * TILE, (index + 1) * TILE)
        queries = jnp.dot(hidden, wq_ref[...], preferred_element_type=f32)
        q_ref[rows] = (queries * query_factor).astype(bf16)
        k_ref[rows] = keys
        values_at(index * TILE, values)

    load(1)
    q_ref[0:TILE] = qe_ref[0:TILE]
    q_ref[tokens - TILE :] = qe_ref[TILE:]
    k_ref[0:TILE] = low_ref[0]
    k_ref[tokens - TILE :] = high_ref[0]
    v_ref[0, width:, :] = jnp.ones((ONES, tokens), bf16)
    v_ref[1, width:, :] = jnp.ones((ONES, tokens), bf16)
    values_at(0, low_ref[1].astype(f32))
    for index in range(1, tiles - 1):
        if index + 2 < tiles:
            load(index + 1)
        multiply(index)
    values_at(tokens - TILE, high_ref[1].astype(f32))
    v_ref[1, 0:width, tokens - GRID_W :] = jnp.zeros((width, GRID_W), bf16)


def main_projections(latent, a, b, weights, edges):
    tokens, width = latent.shape
    out = weights[0].shape[1]
    return call(
        main_kernel,
        [array((tokens, out)), array((tokens, out)), array((2, out + ONES, tokens))],
        in_specs=[whole()] * 9,
        out_specs=[whole()] * 3,
        scratch_shapes=[VMEM((TILE, width), bf16), VMEM((TILE, width), bf16)],
        flops=5_000_000_000,
    )(latent, a, b, *weights, *edges)


def attend_rows(rows, q_ref, kc_ref, vc_ref, t_ref, out_ref, scores, probs):
    width = q_ref.shape[1]
    heads = width // HEAD_DIM
    lane_head = lax.broadcasted_iota(jnp.int32, (1, width), 1) // HEAD_DIM
    head_mask = [(lane_head == h).astype(f32).astype(bf16) for h in range(heads)]
    lower = lax.broadcasted_iota(jnp.int32, (HEAD_DIM, LANES), 1) < GRID_W
    dims = (((1,), (1,)), ((), ()))

    def score(index):
        row, k_ref, _, start, offset = rows[index]
        s_ref = scores[index % len(scores)]
        q = q_ref[row * GRID_W : (row + 1) * GRID_W, :]
        big = jnp.concatenate([q * mask for mask in head_mask], axis=0)
        keys = k_ref[part(start * GRID_W, GRID_W, NEAR), :]
        near = lax.dot_general(keys, big, dims, preferred_element_type=f32)
        near += t_ref[part(offset * GRID_W, GRID_W, NEAR), :]
        far = lax.dot_general(kc_ref[...], big, dims, preferred_element_type=f32)
        s_ref[0:NEAR, :] = near
        s_ref[NEAR:, :] = far
        return jnp.maximum(
            jnp.max(near, axis=0, keepdims=True), jnp.max(far, axis=0, keepdims=True)
        )

    def weigh(index, peak):
        s_ref, p_ref = scores[index % len(scores)], probs[index % len(probs)]
        p_ref[...] = jnp.exp2(s_ref[...] - peak).astype(bf16)

    def gather(index):
        _, _, v_ref, start, _ = rows[index]
        p_ref = probs[index % len(probs)]
        values = v_ref[start % 2, :, part(start // 2 * LANES, LANES, NEAR)]
        out = jnp.dot(values, p_ref[0:NEAR, :], preferred_element_type=f32)
        out += jnp.dot(vc_ref[...], p_ref[NEAR:, :], preferred_element_type=f32)
        return out[0:width] * (1.0 / out[width : width + 1])

    def store(index, left, right):
        row = rows[index][0]
        lanes = slice(row * GRID_W, row * GRID_W + LANES)
        for pair in range(heads // 2):
            cols = slice(pair * LANES, (pair + 1) * LANES)
            for half in range(2):
                at = slice(pair * LANES + half * HEAD_DIM, pair * LANES + (half + 1) * HEAD_DIM)
                a, b = left[at, cols], right[at, cols]
                if half == 0:
                    b = pltpu.roll(b, GRID_W, 1)
                else:
                    a = pltpu.roll(a, GRID_W, 1)
                out_ref[at, lanes] = jnp.where(lower, a, b).astype(bf16)

    peaks, outs = {}, {}
    for index in range(len(rows) + 2):
        if index < len(rows):
            peaks[index] = score(index)
        if 0 <= index - 1 < len(rows):
            weigh(index - 1, peaks.pop(index - 1))
        if 0 <= index - 2:
            outs[index - 2] = gather(index - 2)
            if (index - 2) % 2:
                store(index - 3, outs.pop(index - 3), outs.pop(index - 2))


def part(start, unit, size):
    if isinstance(start, int):
        return slice(start, start + size)
    return pl.ds(pl.multiple_of(start, unit), size)


def inner_kernel(count, q_ref, k_ref, v_ref, t_ref, *rest):
    contexts, (out_ref, kc_ref, vc_ref, *scratch) = rest[:count], rest[count:]
    width = q_ref.shape[1]
    grid_rows = q_ref.shape[0] // GRID_W
    height = contexts[0].shape[1]
    for index, context in enumerate(contexts):
        kc_ref[index * height : (index + 1) * height] = context[0]
    far_values = jnp.concatenate([context[1] for context in contexts], axis=0)
    vc_ref[0:width, :] = far_values.astype(f32).T.astype(bf16)
    vc_ref[width:, :] = jnp.ones((ONES, vc_ref.shape[1]), bf16)
    rows = [
        (row, k_ref, v_ref, row - HALO_ROWS, WIN_ROWS - 1 - HALO_ROWS)
        for row in range(HALO_ROWS, grid_rows - HALO_ROWS)
    ]
    attend_rows(rows, q_ref, kc_ref, vc_ref, t_ref, out_ref, scratch[0:2], scratch[2:4])


def outer_kernel(sp_count, done_ref, q_ref, k_ref, v_ref, kc_ref, vc_ref, t_ref, first_ref, second_ref, out_ref, *rest):
    tokens, width = q_ref.shape
    grid_rows = tokens // GRID_W
    block_refs, scratch = rest[:-8], rest[-8:]
    kl_ref, kh_ref, vl_ref, vh_ref = scratch[0:4]
    strip = 3 * TILE
    ones = jnp.ones((ONES, strip), bf16)
    even = lax.axis_index("sp") % 2 == 0
    low_halo = jnp.where(even, second_ref[...], first_ref[...])
    high_halo = jnp.where(even, first_ref[...], second_ref[...])
    kl_ref[0:TILE] = low_halo[0]
    kl_ref[TILE:] = k_ref[0 : 2 * TILE]
    kh_ref[0 : 2 * TILE] = k_ref[tokens - 2 * TILE :]
    kh_ref[2 * TILE :] = high_halo[0]
    low = low_halo[1].astype(f32).T
    high = high_halo[1].astype(f32).T
    for ref in (vl_ref, vh_ref):
        ref[0, width:, :] = ones
        ref[1, width:, :] = ones
    rolled = pltpu.roll(low, TILE - GRID_W, 1).astype(bf16)
    vl_ref[0, 0:width, 0:TILE] = low.astype(bf16)
    vl_ref[0, 0:width, TILE:] = v_ref[0, 0:width, 0 : 2 * TILE]
    vl_ref[1, 0:width, 0 : TILE - GRID_W] = rolled[:, 0 : TILE - GRID_W]
    first = pltpu.roll(v_ref[0, 0:width, 0:LANES].astype(f32), GRID_W, 1).astype(bf16)
    vl_ref[1, 0:width, TILE - GRID_W : TILE] = first[:, GRID_W:]
    vl_ref[1, 0:width, TILE:] = v_ref[1, 0:width, 0 : 2 * TILE]
    rolled = pltpu.roll(high, TILE - GRID_W, 1).astype(bf16)
    vh_ref[0, 0:width, 0 : 2 * TILE] = v_ref[0, 0:width, tokens - 2 * TILE :]
    vh_ref[0, 0:width, 2 * TILE :] = high.astype(bf16)
    vh_ref[1, 0:width, 0 : 2 * TILE] = v_ref[1, 0:width, tokens - 2 * TILE :]
    vh_ref[1, 0:width, 2 * TILE - GRID_W : 2 * TILE] = rolled[:, TILE - GRID_W :]
    vh_ref[1, 0:width, 2 * TILE : strip - GRID_W] = rolled[:, 0 : TILE - GRID_W]
    vh_ref[1, 0:width, strip - GRID_W :] = jnp.zeros((width, GRID_W), bf16)
    sp = lax.axis_index("sp")
    total = grid_rows * sp_count
    rows = []
    for row in (*range(HALO_ROWS), *range(grid_rows - HALO_ROWS, grid_rows)):
        own = sp * grid_rows
        first = jnp.clip(own + row - HALO_ROWS, 0, total - WIN_ROWS)
        offset = first - (own + row) + WIN_ROWS - 1
        if row < HALO_ROWS:
            rows.append((row, kl_ref, vl_ref, first - own + HALO_ROWS, offset))
        else:
            rows.append((row, kh_ref, vh_ref, first - own - (grid_rows - WIN_ROWS), offset))
    attend_rows(rows, q_ref, kc_ref, vc_ref, t_ref, out_ref, scratch[4:6], scratch[6:8])
    for step, block_ref in enumerate(block_refs):
        share = block_ref.shape[1]
        block_ref[...] = out_ref[:, part(target("tp", step) * share, LANES, share)]


def attention_scratch(total, width):
    return [VMEM((total, width), f32)] * 2 + [VMEM((total, width), bf16)] * 2


def inner_attention(queries, keys, values, table, contexts):
    tokens, width = queries.shape
    far = len(contexts) * contexts[0].shape[1]
    return call(
        functools.partial(inner_kernel, len(contexts)),
        [array((width, tokens)), array((far, width)), array((width + ONES, far))],
        in_specs=[whole()] * (4 + len(contexts)),
        out_specs=[whole()] * 3,
        scratch_shapes=attention_scratch(NEAR + far, width),
        flops=6_000_000_000,
    )(queries, keys, values, table, *contexts)


def outer_attention(done, queries, keys, values, far_keys, far_values, table, first, second):
    tokens, width = queries.shape
    strip = 3 * TILE
    tp_count = lax.axis_size("tp")
    share = tokens // tp_count
    blocks = [array((width, share))] * (tp_count if share % LANES == 0 else 0)
    attended, *blocks = call(
        functools.partial(outer_kernel, lax.axis_size("sp")),
        [array((width, tokens)), *blocks],
        in_specs=[whole()] * 9,
        out_specs=[whole()] * (1 + len(blocks)),
        input_output_aliases={0: 0},
        scratch_shapes=[VMEM((strip, width), bf16)] * 2
        + [VMEM((2, width + ONES, strip), bf16)] * 2
        + attention_scratch(NEAR + far_keys.shape[0], width),
        flops=3_000_000_000,
    )(done, queries, keys, values, far_keys, far_values, table, first, second)
    if not blocks:
        for step in range(tp_count):
            start = target("tp", step) * share
            blocks.append(lax.dynamic_slice_in_dim(attended, start, share, 1))
    return blocks


def output_kernel(count, x_ref, w_ref, *rest):
    blocks, pieces = rest[:count], rest[count : 2 * count]
    out_ref, gate_ref, held_ref, block_ref, sems = rest[2 * count :]
    height, share = blocks[0].shape
    dims = (((0,), (0,)), ((), ()))
    tile = w_ref.shape[1] // count
    for index in range(count):
        gate_ref[:, part(origin("tp", index) * tile, LANES, tile)] = pieces[index][4:5, :]
        rows = part(origin("tp", index) * height, LANES, height)
        block_ref[rows, :] = blocks[index][...]
    mine = part(lax.axis_index("tp") * share, GRID_W, share)
    copies = []
    for step in range(count):
        cols = slice(step * tile, (step + 1) * tile)
        total = lax.dot_general(block_ref[...], w_ref[:, cols], dims, preferred_element_type=f32)
        held_ref[:, cols] = (
            x_ref[mine, cols].astype(f32) + gate_ref[:, cols] * total
        ).astype(bf16)
        copies.append(
            pltpu.make_async_copy(held_ref.at[:, cols], out_ref.at[:, cols], sems.at[step])
        )
        copies[-1].start()
    for copy in copies:
        copy.wait()


def output(x, weight, blocks, pieces):
    count = len(blocks)
    share = x.shape[0] // count
    return call(
        functools.partial(output_kernel, count),
        array((share, x.shape[1])),
        in_specs=[whole()] * (2 + 2 * count),
        out_specs=whole(HBM),
        scratch_shapes=[
            VMEM((1, x.shape[1]), f32),
            VMEM((share, x.shape[1]), bf16),
            VMEM((weight.shape[0], share), bf16),
            pltpu.SemaphoreType.DMA((count,)),
        ],
        flops=2_000_000_000,
    )(x, weight, *blocks, *pieces)


def gathered(block, axis):
    return [block] + [exchange(block, axis, step) for step in range(1, lax.axis_size(axis))]


def local(
    latent,
    condition,
    context_tokens,
    context_condition,
    shift_weight,
    scale_weight,
    gate_weight,
    norm_gain,
    query_weight,
    key_weight,
    value_weight,
    out_weight,
    offset_bias,
):
    terms, gain = modulation_terms(
        condition, context_condition, shift_weight, scale_weight, gate_weight, norm_gain
    )
    partials = gathered(terms, "sp")
    *weights, rows = bias_rows(terms, offset_bias, query_weight, key_weight, value_weight)
    summed = summed_terms(rows, partials)
    pieces = gathered(summed, "tp")
    table = bias_table(summed, rows)
    *edges, far, a, b = edge_projections(
        latent, context_tokens, gain, weights, pieces
    )
    count = lax.axis_size("sp")
    contexts = gathered(far, "sp")
    pairs = [(i, i ^ 1) for i in range(count) if i ^ 1 < count]
    first = lax.ppermute(edges[3], "sp", pairs)
    pairs = [(i, j) for i in range(count) for j in [((i + 1) ^ 1) - 1] if 0 <= j < count]
    second = lax.ppermute(edges[4], "sp", pairs)
    fields = main_projections(latent, a, b, weights, edges[:3])
    inner, *fars = inner_attention(*fields, table, contexts)
    blocks = outer_attention(inner, *fields, *fars, table, first, second)
    received = blocks[:1] + [
        exchange(block, "tp", step) for step, block in enumerate(blocks) if step
    ]
    return output(latent, out_weight, received, pieces)


def solution(mesh):
    placed = (
        P(("grp", "sp"), None),
        P("grp"),
        P(("grp", "sp"), None),
        P(),
        P("sp", "tp"),
        P("sp", "tp"),
        P("sp", "tp"),
        P(),
        P(None, "tp"),
        P(None, "tp"),
        P(None, "tp"),
        P(),
        P("tp", None, None),
    )
    return jax.shard_map(
        local, mesh=mesh, in_specs=placed, out_specs=P(("grp", "sp", "tp"), None), check_vma=False
    )
```

```python
import functools
import math

import jax
import jax.numpy as jnp
from jax import lax
from jax.experimental import pallas as pl
from jax.experimental.pallas import tpu as pltpu
from jax.sharding import PartitionSpec as P


HEAD_DIM = 64
GRID_W = 64
WIN_ROWS = 8
WIN_COLS = 16
ROW_OFFSETS = 2 * WIN_ROWS - 1
COL_OFFSETS = 2 * WIN_COLS - 1
LANES = 128
HALO_ROWS = WIN_ROWS // 2
TILE = HALO_ROWS * GRID_W
NEAR = WIN_ROWS * GRID_W
ONES = 16

epsilon = 1e-06
masked_score = -1e30
log2e = math.log2(math.e)
VMEM = pltpu.VMEM
f32 = jnp.float32
bf16 = jnp.bfloat16


def shift_along(block, axis, step):
    count = lax.axis_size(axis)
    return lax.ppermute(block, axis, [(i, (i + step) % count) for i in range(count)])


HBM = pltpu.HBM


def exchange(block, axis, step):
    count = lax.axis_size(axis)
    if count & (count - 1):
        return shift_along(block, axis, step)
    return lax.ppermute(block, axis, [(i, i ^ step) for i in range(count)])


def origin(axis, step):
    count = lax.axis_size(axis)
    index = lax.axis_index(axis)
    if count & (count - 1):
        return lax.rem(index - step + count, count)
    return jnp.bitwise_xor(index, step)


def target(axis, step):
    count = lax.axis_size(axis)
    index = lax.axis_index(axis)
    if count & (count - 1):
        return lax.rem(index + step, count)
    return jnp.bitwise_xor(index, step)


def whole(memory_space=VMEM):
    return pl.BlockSpec(memory_space=memory_space)


def call(kernel, out_shape, *, vmem=16 << 20, flops=0, **kwargs):
    cost = pl.CostEstimate(flops=flops, transcendentals=0, bytes_accessed=0)
    return pl.pallas_call(
        kernel,
        out_shape=out_shape,
        compiler_params=pltpu.CompilerParams(vmem_limit_bytes=vmem),
        cost_estimate=cost if flops else None,
        **kwargs,
    )


def in_hbm(values):
    return [pltpu.with_memory_space_constraint(value, HBM) for value in values]


def array(shape, dtype=bf16):
    return jax.ShapeDtypeStruct(tuple(shape), dtype)


def modulation_kernel(*refs):
    inputs, (out_ref, gain_ref, line_ref, cond_ref, ctx_ref, act_ref, weights_ref, sems) = refs[:6], refs[6:]
    rows = weights_ref.shape[1]
    mine = pl.ds(pl.multiple_of(lax.axis_index("sp") * rows, LANES), rows)
    targets = (cond_ref, ctx_ref, *(weights_ref.at[i] for i in range(3)), line_ref)
    copies = [
        pltpu.make_async_copy(source, target, sems.at[index])
        for index, (source, target) in enumerate(zip(inputs, targets))
    ]
    for copy in copies:
        copy.start()

    act_ref[...] = jnp.zeros_like(act_ref)
    for row, ref in enumerate((cond_ref, ctx_ref)):
        copies[row].wait()
        v = ref[...].reshape(1, -1).astype(f32)
        act_ref[row : row + 1, :] = v / (1.0 + jnp.exp(-v))
    both = act_ref[:, mine].astype(bf16)
    for index in range(3):
        copies[2 + index].wait()
        terms = jnp.dot(both, weights_ref[index], preferred_element_type=f32)
        out_ref[2 * index : 2 * index + 2, :] = terms[0:2]
    out_ref[6:8, :] = jnp.zeros_like(out_ref[6:8, :])
    copies[5].wait()
    gain_ref[...] = line_ref[...].reshape(gain_ref.shape).astype(f32)


def modulation_terms(condition, context_condition, *rest):
    rows, width = rest[0].shape
    whole_line = VMEM(condition.shape, bf16)
    return call(
        modulation_kernel,
        [array((8, width), f32), array((1, *rest[-1].shape), f32)],
        in_specs=[whole(HBM)] * 6,
        out_specs=[whole()] * 2,
        scratch_shapes=[
            whole_line,
            whole_line,
            whole_line,
            VMEM((16, *condition.shape), f32),
            VMEM((3, rows, width), bf16),
            pltpu.SemaphoreType.DMA((6,)),
        ],
        flops=3_000_000_000,
    )(*in_hbm((condition, context_condition, *rest)))


def sum_kernel(token_ref, *refs):
    total = refs[0][...]
    for ref in refs[1:-1]:
        total += ref[...]
    refs[-1][...] = total


def summed_terms(token, partials):
    return call(
        sum_kernel,
        array(partials[0].shape, f32),
        in_specs=[whole()] * (1 + len(partials)),
        out_specs=whole(),
    )(token, *partials)


def rows_kernel(token_ref, source_ref, *refs):
    table_ref, bias_ref, lines_ref, sems = refs[-4:]
    count = (len(refs) - 4) // 2
    pairs = [(source_ref, bias_ref), *zip(refs[:count], refs[count:-4])]
    copies = [
        pltpu.make_async_copy(source, target, sems.at[index])
        for index, (source, target) in enumerate(pairs)
    ]
    for copy in copies:
        copy.start()
    copies[0].wait()
    heads = bias_ref.shape[1]
    for head in range(heads):
        lines_ref[:, :] = jnp.zeros_like(lines_ref)
        lines_ref[0:ROW_OFFSETS, 0:COL_OFFSETS] = bias_ref[:, head, :] * log2e
        lines = lines_ref[...]
        first = pltpu.roll(lines, LANES - (WIN_COLS - 1), 1)
        second = pltpu.roll(lines, GRID_W - (WIN_COLS - 1), 1)
        for pair in range((ROW_OFFSETS + 1) // 2):
            line = first[2 * pair : 2 * pair + 1] + second[2 * pair + 1 : 2 * pair + 2]
            line = jnp.broadcast_to(line, (GRID_W, LANES))
            table_ref[head * GRID_W : (head + 1) * GRID_W, pair * LANES : (pair + 1) * LANES] = (
                pltpu.roll(line, 0, 1, stride=1, stride_axis=0)
            )
    for copy in copies[1:]:
        copy.wait()


def bias_rows(token, offset_bias, *weights):
    heads = offset_bias.shape[0]
    rows = (ROW_OFFSETS + 1) * GRID_W
    return call(
        rows_kernel,
        [array(weight.shape) for weight in weights] + [array((heads * HEAD_DIM, rows), f32)],
        in_specs=[whole()] + [whole(HBM)] * (1 + len(weights)),
        out_specs=[whole()] * (1 + len(weights)),
        scratch_shapes=[
            VMEM((ROW_OFFSETS, heads, COL_OFFSETS), f32),
            VMEM((ROW_OFFSETS + 1, LANES), f32),
            pltpu.SemaphoreType.DMA((1 + len(weights),)),
        ],
        flops=500_000_000,
    )(token, *in_hbm((jnp.transpose(offset_bias, (1, 0, 2)), *weights)))


def flip_kernel(token_ref, table_ref, weight_ref, held_ref, out_ref, sem):
    copy = pltpu.make_async_copy(weight_ref, held_ref, sem)
    copy.start()
    width = table_ref.shape[0]
    key = lax.broadcasted_iota(jnp.int32, (LANES, LANES), 0) % GRID_W
    query = lax.broadcasted_iota(jnp.int32, (LANES, LANES), 1) % GRID_W
    first = jnp.clip(query - WIN_COLS // 2, 0, GRID_W - WIN_COLS)
    inside = (key >= first) & (key < first + WIN_COLS)
    for row in range((ROW_OFFSETS + 1) // 2):
        for col in range(width // LANES):
            rows, cols = slice(row * LANES, (row + 1) * LANES), slice(col * LANES, (col + 1) * LANES)
            out_ref[rows, cols] = jnp.where(inside, table_ref[cols, rows].T, masked_score)
    copy.wait()


def bias_table(token, rows, weight):
    return call(
        flip_kernel,
        [array(weight.shape), array(rows.shape[::-1], f32)],
        in_specs=[whole()] * 2 + [whole(HBM)],
        out_specs=[whole()] * 2,
        scratch_shapes=[pltpu.SemaphoreType.DMA],
        flops=1_000_000_000,
    )(token, rows, *in_hbm([weight]))


def modulators(pieces, gain_ref, scale_row, shift_row, a_ref, b_ref):
    width = pieces[0].shape[1]
    for step, piece in enumerate(pieces):
        owner = origin("tp", step)
        part = pl.ds(pl.multiple_of(owner * width, LANES), width)
        a_ref[:, part] = gain_ref[:, part] * (1.0 + piece[scale_row : scale_row + 1, :])
        b_ref[:, part] = piece[shift_row : shift_row + 1, :]


def modulated(x, a, b):
    values = x.astype(f32)
    inverse = lax.rsqrt(jnp.mean(values * values, axis=-1, keepdims=True) + epsilon)
    return ((values * inverse) * a + b).astype(bf16)


query_factor = log2e * HEAD_DIM ** (-0.5)


def edge_kernel(count, x_ref, context_ref, gain_ref, wq_ref, wk_ref, wv_ref, *rest):
    pieces = rest[:count]
    q_ref, low_ref, high_ref, even_ref, odd_ref, far_ref, a_ref, b_ref, ac_ref, bc_ref, first_ref, second_ref = rest[count:]
    modulators(pieces, gain_ref, 3, 1, ac_ref, bc_ref)
    hidden = modulated(context_ref[...], ac_ref[...], bc_ref[...])
    far_ref[0] = jnp.dot(hidden, wk_ref[...], preferred_element_type=f32).astype(bf16)
    far_ref[1] = jnp.dot(hidden, wv_ref[...], preferred_element_type=f32).astype(bf16)
    modulators(pieces, gain_ref, 2, 0, a_ref, b_ref)
    scratch = (first_ref, second_ref)
    outs = (low_ref, high_ref)
    tokens = x_ref.shape[0]
    for start, ref in zip((0, tokens - TILE), scratch):
        ref[...] = modulated(x_ref[start : start + TILE], a_ref[...], b_ref[...])
    for ref, out_ref in zip(scratch, outs):
        out_ref[0] = jnp.dot(ref[...], wk_ref[...], preferred_element_type=f32).astype(bf16)
        out_ref[1] = jnp.dot(ref[...], wv_ref[...], preferred_element_type=f32).astype(bf16)
    even = lax.axis_index("sp") % 2 == 0
    even_ref[...] = jnp.where(even, high_ref[...], low_ref[...])
    odd_ref[...] = jnp.where(even, low_ref[...], high_ref[...])
    for index, ref in enumerate(scratch):
        queries = jnp.dot(ref[...], wq_ref[...], preferred_element_type=f32)
        q_ref[index * TILE : (index + 1) * TILE] = (queries * query_factor).astype(bf16)


def edge_projections(latent, context, gain, weights, pieces):
    width = latent.shape[1]
    out = weights[0].shape[1]
    return call(
        functools.partial(edge_kernel, len(pieces)),
        [
            array((2 * TILE, out)),
            *[array((2, TILE, out))] * 4,
            array((2, context.shape[0], out)),
            array((1, width), f32),
            array((1, width), f32),
        ],
        in_specs=[whole()] * (6 + len(pieces)),
        out_specs=[whole()] * 8,
        scratch_shapes=[
            VMEM((1, width), f32),
            VMEM((1, width), f32),
            VMEM((TILE, width), bf16),
            VMEM((TILE, width), bf16),
        ],
        flops=2_000_000_000,
    )(latent, context, gain, *weights, *pieces)


def main_kernel(x_ref, a_ref, b_ref, wq_ref, wk_ref, wv_ref, qe_ref, low_ref, high_ref, *rest):
    q_ref, k_ref, v_ref, *scratch = rest
    tokens, width = k_ref.shape
    tiles = tokens // TILE

    def load(index):
        rows = slice(index * TILE, (index + 1) * TILE)
        scratch[index % 2][...] = modulated(x_ref[rows], a_ref[...], b_ref[...])

    def values_at(start, values):
        turned = values.T
        v_ref[0, 0:width, start : start + TILE] = turned.astype(bf16)
        rolled = pltpu.roll(turned, TILE - GRID_W, 1).astype(bf16)
        v_ref[1, 0:width, start : start + TILE - GRID_W] = rolled[:, 0 : TILE - GRID_W]
        if start:
            v_ref[1, 0:width, start - GRID_W : start] = rolled[:, TILE - GRID_W :]

    def multiply(index):
        hidden = scratch[index % 2][...]
        keys = jnp.dot(hidden, wk_ref[...], preferred_element_type=f32).astype(bf16)
        values = jnp.dot(hidden, wv_ref[...], preferred_element_type=f32)
        rows = slice(index * TILE, (index + 1) * TILE)
        queries = jnp.dot(hidden, wq_ref[...], preferred_element_type=f32)
        q_ref[rows] = (queries * query_factor).astype(bf16)
        k_ref[rows] = keys
        values_at(index * TILE, values)

    load(1)
    q_ref[0:TILE] = qe_ref[0:TILE]
    q_ref[tokens - TILE :] = qe_ref[TILE:]
    k_ref[0:TILE] = low_ref[0]
    k_ref[tokens - TILE :] = high_ref[0]
    v_ref[0, width:, :] = jnp.ones((ONES, tokens), bf16)
    v_ref[1, width:, :] = jnp.ones((ONES, tokens), bf16)
    values_at(0, low_ref[1].astype(f32))
    for index in range(1, tiles - 1):
        if index + 2 < tiles:
            load(index + 1)
        multiply(index)
    values_at(tokens - TILE, high_ref[1].astype(f32))
    v_ref[1, 0:width, tokens - GRID_W :] = jnp.zeros((width, GRID_W), bf16)


def main_projections(latent, a, b, weights, edges):
    tokens, width = latent.shape
    out = weights[0].shape[1]
    return call(
        main_kernel,
        [array((tokens, out)), array((tokens, out)), array((2, out + ONES, tokens))],
        in_specs=[whole()] * 9,
        out_specs=[whole()] * 3,
        scratch_shapes=[VMEM((TILE, width), bf16), VMEM((TILE, width), bf16)],
        flops=5_000_000_000,
    )(latent, a, b, *weights, *edges)


def attend_rows(rows, q_ref, kc_ref, vc_ref, t_ref, out_ref, scores, probs):
    width = q_ref.shape[1]
    heads = width // HEAD_DIM
    lane_head = lax.broadcasted_iota(jnp.int32, (1, width), 1) // HEAD_DIM
    head_mask = [(lane_head == h).astype(f32).astype(bf16) for h in range(heads)]
    lower = lax.broadcasted_iota(jnp.int32, (HEAD_DIM, LANES), 1) < GRID_W
    dims = (((1,), (1,)), ((), ()))

    def score(index):
        row, k_ref, _, start, offset = rows[index]
        s_ref = scores[index % len(scores)]
        q = q_ref[row * GRID_W : (row + 1) * GRID_W, :]
        big = jnp.concatenate([q * mask for mask in head_mask], axis=0)
        keys = k_ref[part(start * GRID_W, GRID_W, NEAR), :]
        near = lax.dot_general(keys, big, dims, preferred_element_type=f32)
        near += t_ref[part(offset * GRID_W, GRID_W, NEAR), :]
        far = lax.dot_general(kc_ref[...], big, dims, preferred_element_type=f32)
        s_ref[0:NEAR, :] = near
        s_ref[NEAR:, :] = far
        return jnp.maximum(
            jnp.max(near, axis=0, keepdims=True), jnp.max(far, axis=0, keepdims=True)
        )

    def weigh(index, peak):
        s_ref, p_ref = scores[index % len(scores)], probs[index % len(probs)]
        p_ref[...] = jnp.exp2(s_ref[...] - peak).astype(bf16)

    def gather(index):
        _, _, v_ref, start, _ = rows[index]
        p_ref = probs[index % len(probs)]
        values = v_ref[start % 2, :, part(start // 2 * LANES, LANES, NEAR)]
        out = jnp.dot(values, p_ref[0:NEAR, :], preferred_element_type=f32)
        out += jnp.dot(vc_ref[...], p_ref[NEAR:, :], preferred_element_type=f32)
        return out[0:width] * (1.0 / out[width : width + 1])

    def store(index, left, right):
        row = rows[index][0]
        lanes = slice(row * GRID_W, row * GRID_W + LANES)
        for pair in range(heads // 2):
            cols = slice(pair * LANES, (pair + 1) * LANES)
            for half in range(2):
                at = slice(pair * LANES + half * HEAD_DIM, pair * LANES + (half + 1) * HEAD_DIM)
                a, b = left[at, cols], right[at, cols]
                if half == 0:
                    b = pltpu.roll(b, GRID_W, 1)
                else:
                    a = pltpu.roll(a, GRID_W, 1)
                out_ref[at, lanes] = jnp.where(lower, a, b).astype(bf16)

    peaks, outs = {}, {}
    for index in range(len(rows) + 2):
        if index < len(rows):
            peaks[index] = score(index)
        if 0 <= index - 1 < len(rows):
            weigh(index - 1, peaks.pop(index - 1))
        if 0 <= index - 2:
            outs[index - 2] = gather(index - 2)
            if (index - 2) % 2:
                store(index - 3, outs.pop(index - 3), outs.pop(index - 2))


def part(start, unit, size):
    if isinstance(start, int):
        return slice(start, start + size)
    return pl.ds(pl.multiple_of(start, unit), size)


def is_free(row, grid_rows):
    return HALO_ROWS <= row < grid_rows - HALO_ROWS


def phases(tokens):
    count = lax.axis_size("tp")
    share = tokens // count
    rows = range(tokens // GRID_W)
    if share % LANES or share < 2 * LANES:
        return rows, range(0)
    each = share // GRID_W
    late = [r for r in rows if (r < 2 if r < each else r % each >= each - 2)]
    return [r for r in rows if r not in late], late


def far_refs(contexts, kc_ref, vc_ref):
    width = kc_ref.shape[1]
    height = contexts[0].shape[1]
    for index, context in enumerate(contexts):
        kc_ref[index * height : (index + 1) * height] = context[0]
    far_values = jnp.concatenate([context[1] for context in contexts], axis=0)
    vc_ref[0:width, :] = far_values.astype(f32).T.astype(bf16)
    vc_ref[width:, :] = jnp.ones((ONES, vc_ref.shape[1]), bf16)


def row_plan(rows, grid_rows, sp_count, k_ref, v_ref, strips):
    own = lax.axis_index("sp") * grid_rows
    total = grid_rows * sp_count
    plan = []
    for row in rows:
        if is_free(row, grid_rows):
            plan.append((row, k_ref, v_ref, row - HALO_ROWS, WIN_ROWS - 1 - HALO_ROWS))
            continue
        kl_ref, kh_ref, vl_ref, vh_ref = strips
        first = jnp.clip(own + row - HALO_ROWS, 0, total - WIN_ROWS)
        offset = first - (own + row) + WIN_ROWS - 1
        if row < HALO_ROWS:
            plan.append((row, kl_ref, vl_ref, first - own + HALO_ROWS, offset))
        else:
            plan.append((row, kh_ref, vh_ref, first - own - (grid_rows - WIN_ROWS), offset))
    return plan


def inner_kernel(count, rows, q_ref, k_ref, v_ref, t_ref, *rest):
    contexts, (out_ref, kc_ref, vc_ref, *scratch) = rest[:count], rest[count:]
    far_refs(contexts, kc_ref, vc_ref)
    plan = row_plan(rows, q_ref.shape[0] // GRID_W, 0, k_ref, v_ref, None)
    attend_rows(plan, q_ref, kc_ref, vc_ref, t_ref, out_ref, scratch[0:2], scratch[2:4])


def fill_strips(k_ref, v_ref, first_ref, second_ref, strips):
    tokens, width = k_ref.shape
    kl_ref, kh_ref, vl_ref, vh_ref = strips
    strip = 3 * TILE
    ones = jnp.ones((ONES, strip), bf16)
    even = lax.axis_index("sp") % 2 == 0
    low_halo = jnp.where(even, second_ref[...], first_ref[...])
    high_halo = jnp.where(even, first_ref[...], second_ref[...])
    kl_ref[0:TILE] = low_halo[0]
    kl_ref[TILE:] = k_ref[0 : 2 * TILE]
    kh_ref[0 : 2 * TILE] = k_ref[tokens - 2 * TILE :]
    kh_ref[2 * TILE :] = high_halo[0]
    low = low_halo[1].astype(f32).T
    high = high_halo[1].astype(f32).T
    for ref in (vl_ref, vh_ref):
        ref[0, width:, :] = ones
        ref[1, width:, :] = ones
    rolled = pltpu.roll(low, TILE - GRID_W, 1).astype(bf16)
    vl_ref[0, 0:width, 0:TILE] = low.astype(bf16)
    vl_ref[0, 0:width, TILE:] = v_ref[0, 0:width, 0 : 2 * TILE]
    vl_ref[1, 0:width, 0 : TILE - GRID_W] = rolled[:, 0 : TILE - GRID_W]
    first = pltpu.roll(v_ref[0, 0:width, 0:LANES].astype(f32), GRID_W, 1).astype(bf16)
    vl_ref[1, 0:width, TILE - GRID_W : TILE] = first[:, GRID_W:]
    vl_ref[1, 0:width, TILE:] = v_ref[1, 0:width, 0 : 2 * TILE]
    rolled = pltpu.roll(high, TILE - GRID_W, 1).astype(bf16)
    vh_ref[0, 0:width, 0 : 2 * TILE] = v_ref[0, 0:width, tokens - 2 * TILE :]
    vh_ref[0, 0:width, 2 * TILE :] = high.astype(bf16)
    vh_ref[1, 0:width, 0 : 2 * TILE] = v_ref[1, 0:width, tokens - 2 * TILE :]
    vh_ref[1, 0:width, 2 * TILE - GRID_W : 2 * TILE] = rolled[:, TILE - GRID_W :]
    vh_ref[1, 0:width, 2 * TILE : strip - GRID_W] = rolled[:, 0 : TILE - GRID_W]
    vh_ref[1, 0:width, strip - GRID_W :] = jnp.zeros((width, GRID_W), bf16)


def split_blocks(out_ref, block_refs, late):
    for step, block_ref in enumerate(block_refs):
        size = block_ref.shape[1]
        owner = target("tp", step)
        share = out_ref.shape[1] // len(block_refs)
        inside = jnp.where(owner == 0, 0, share - size)
        inside = inside if late else share - size - inside
        start = owner * share + inside
        block_ref[...] = out_ref[:, part(start, LANES, size)]


def middle_kernel(rows, sp_count, done_ref, latent_ref, q_ref, k_ref, v_ref, kc_ref, vc_ref, t_ref, first_ref, second_ref, out_ref, own_ref, *rest):
    strips, block_refs, (sem, *scratch) = rest[:4], rest[4:-5], rest[-5:]
    share = own_ref.shape[0]
    mine = part(lax.axis_index("tp") * share, GRID_W, share)
    copy = pltpu.make_async_copy(latent_ref.at[mine], own_ref, sem)
    copy.start()
    fill_strips(k_ref, v_ref, first_ref, second_ref, strips)
    plan = row_plan(rows, q_ref.shape[0] // GRID_W, sp_count, k_ref, v_ref, strips)
    attend_rows(plan, q_ref, kc_ref, vc_ref, t_ref, out_ref, scratch[0:2], scratch[2:4])
    split_blocks(out_ref, block_refs, False)
    copy.wait()


def late_kernel(rows, sp_count, q_ref, k_ref, v_ref, kc_ref, vc_ref, t_ref, *rest):
    strips, block_refs, (out_ref, *scratch) = rest[:4], rest[4:-5], rest[-5:]
    plan = row_plan(rows, q_ref.shape[0] // GRID_W, sp_count, k_ref, v_ref, strips)
    attend_rows(plan, q_ref, kc_ref, vc_ref, t_ref, out_ref, scratch[0:2], scratch[2:4])
    split_blocks(out_ref, block_refs, True)


def attention_scratch(total, width):
    return [VMEM((total, width), f32)] * 2 + [VMEM((total, width), bf16)] * 2


def inner_attention(queries, keys, values, table, contexts):
    tokens, width = queries.shape
    far = len(contexts) * contexts[0].shape[1]
    rows = [r for r in phases(tokens)[0] if is_free(r, tokens // GRID_W)]
    rows = [r for r in rows if r ^ 1 in rows]
    return call(
        functools.partial(inner_kernel, len(contexts), rows),
        [array((width, tokens)), array((far, width)), array((width + ONES, far))],
        in_specs=[whole()] * (4 + len(contexts)),
        out_specs=[whole()] * 3,
        scratch_shapes=attention_scratch(NEAR + far, width),
        flops=4_000_000_000,
    )(queries, keys, values, table, *contexts)


def middle_attention(done, latent, queries, keys, values, far_keys, far_values, table, first, second):
    tokens, width = queries.shape
    strip = 3 * TILE
    count = lax.axis_size("tp")
    early, late = phases(tokens)
    rows = [
        r for r in early if not (is_free(r, tokens // GRID_W) and is_free(r ^ 1, tokens // GRID_W))
    ]
    block = array((width, len(early) * GRID_W // count))
    attended, own, *rest = call(
        functools.partial(middle_kernel, rows, lax.axis_size("sp")),
        [
            array((width, tokens)),
            array((tokens // count, latent.shape[1])),
            *[array((strip, width))] * 2,
            *[array((2, width + ONES, strip))] * 2,
            *[block] * (count if late else 0),
        ],
        in_specs=[whole(), whole(HBM)] + [whole()] * 8,
        out_specs=[whole()] * (6 + (count if late else 0)),
        input_output_aliases={0: 0},
        scratch_shapes=[pltpu.SemaphoreType.DMA]
        + attention_scratch(NEAR + far_keys.shape[0], width),
        flops=2_000_000_000,
    )(done, *in_hbm([latent]), queries, keys, values, far_keys, far_values, table, first, second)
    strips, blocks = rest[:4], rest[4:]
    if not late:
        share = tokens // count
        blocks = [
            lax.dynamic_slice_in_dim(attended, target("tp", step) * share, share, 1)
            for step in range(count)
        ]
    return own, strips, list(blocks)


def late_attention(queries, keys, values, far_keys, far_values, table, strips):
    tokens, width = queries.shape
    count = lax.axis_size("tp")
    late = phases(tokens)[1]
    if not late:
        return []
    return list(
        call(
            functools.partial(late_kernel, late, lax.axis_size("sp")),
            [array((width, len(late) * GRID_W // count))] * count,
            in_specs=[whole()] * 10,
            out_specs=[whole()] * count,
            scratch_shapes=[VMEM((width, tokens), bf16)]
            + attention_scratch(NEAR + far_keys.shape[0], width),
            flops=3_000_000_000,
        )(queries, keys, values, far_keys, far_values, table, *strips)
    )


def output_kernel(count, late, *refs):
    x_ref, w_ref, *arrays, out_ref, gate_ref, held_ref, block_ref, sems = refs[late:]
    pieces, blocks = arrays[:count], arrays[count:]
    height, size = blocks[0].shape
    share = out_ref.shape[0]
    tile = w_ref.shape[1] // count
    tp = lax.axis_index("tp")
    for index in range(count):
        gate_ref[:, part(origin("tp", index) * tile, LANES, tile)] = pieces[index][4:5, :]
        rows = part(origin("tp", index) * height, LANES, height)
        block_ref[:, rows] = blocks[index][...].astype(f32).T.astype(bf16)
    inside = jnp.where(tp == 0, 0, share - size)
    inside = inside if late else share - size - inside
    mine = part(inside, GRID_W, size)
    copies = []
    for step in range(count):
        cols = slice(step * tile, (step + 1) * tile)
        total = jnp.dot(block_ref[...], w_ref[:, cols], preferred_element_type=f32)
        held_ref[:, cols] = (
            x_ref[mine, cols].astype(f32) + gate_ref[:, cols] * total
        ).astype(bf16)
        copies.append(
            pltpu.make_async_copy(held_ref.at[:, cols], out_ref.at[mine, cols], sems.at[step])
        )
        copies[-1].start()
    for copy in copies:
        copy.wait()


def output(x, weight, blocks, pieces, done=None):
    count = len(blocks)
    share, width = x.shape
    size = blocks[0].shape[1]
    late = done is not None
    return call(
        functools.partial(output_kernel, count, late),
        array((share, width)),
        in_specs=[whole(HBM)] * late + [whole()] * (2 + len(pieces) + len(blocks)),
        out_specs=whole(HBM),
        input_output_aliases={0: 0} if late else {},
        scratch_shapes=[
            VMEM((1, width), f32),
            VMEM((size, width), bf16),
            VMEM((size, weight.shape[0]), bf16),
            pltpu.SemaphoreType.DMA((count,)),
        ],
        flops=2_000_000_000,
    )(*([done] if late else []), x, weight, *pieces, *blocks)


def gathered(block, axis):
    return [block] + [exchange(block, axis, step) for step in range(1, lax.axis_size(axis))]


def sent(blocks):
    return blocks[:1] + [exchange(blocks[step], "tp", step) for step in range(1, len(blocks))]


def local(
    latent,
    condition,
    context_tokens,
    context_condition,
    shift_weight,
    scale_weight,
    gate_weight,
    norm_gain,
    query_weight,
    key_weight,
    value_weight,
    out_weight,
    offset_bias,
):
    terms, gain = modulation_terms(
        condition, context_condition, shift_weight, scale_weight, gate_weight, norm_gain
    )
    partials = gathered(terms, "sp")
    wk, wv, rows = bias_rows(terms, offset_bias, key_weight, value_weight)
    summed = summed_terms(rows, partials)
    pieces = gathered(summed, "tp")
    wq, table = bias_table(summed, rows, query_weight)
    weights = (wq, wk, wv)
    *edges, far, a, b = edge_projections(
        latent, context_tokens, gain, weights, pieces
    )
    count = lax.axis_size("sp")
    contexts = gathered(far, "sp")
    pairs = [(i, i ^ 1) for i in range(count) if i ^ 1 < count]
    first = lax.ppermute(edges[3], "sp", pairs)
    pairs = [(i, j) for i in range(count) for j in [((i + 1) ^ 1) - 1] if 0 <= j < count]
    second = lax.ppermute(edges[4], "sp", pairs)
    fields = main_projections(latent, a, b, weights, edges[:3])
    inner, *fars = inner_attention(*fields, table, contexts)
    own, strips, early = middle_attention(inner, latent, *fields, *fars, table, first, second)
    early = sent(early)
    late = late_attention(*fields, *fars, table, strips)
    late = sent(late)
    done = output(own, out_weight, early, pieces)
    if not late:
        return done
    return output(own, out_weight, late, pieces, done)


def solution(mesh):
    placed = (
        P(("grp", "sp"), None),
        P("grp"),
        P(("grp", "sp"), None),
        P(),
        P("sp", "tp"),
        P("sp", "tp"),
        P("sp", "tp"),
        P(),
        P(None, "tp"),
        P(None, "tp"),
        P(None, "tp"),
        P(),
        P("tp", None, None),
    )
    return jax.shard_map(
        local, mesh=mesh, in_specs=placed, out_specs=P(("grp", "sp", "tp"), None), check_vma=False
    )
```

```python
import functools
import math

import jax
import jax.numpy as jnp
from jax import lax
from jax.experimental import pallas as pl
from jax.experimental.pallas import tpu as pltpu
from jax.sharding import PartitionSpec as P


HEAD_DIM = 64
GRID_W = 64
WIN_ROWS = 8
WIN_COLS = 16
ROW_OFFSETS = 2 * WIN_ROWS - 1
COL_OFFSETS = 2 * WIN_COLS - 1
LANES = 128
HALO_ROWS = WIN_ROWS // 2
TILE = HALO_ROWS * GRID_W
NEAR = WIN_ROWS * GRID_W
ONES = 16

epsilon = 1e-06
masked_score = -1e30
log2e = math.log2(math.e)
VMEM = pltpu.VMEM
f32 = jnp.float32
bf16 = jnp.bfloat16


def shift_along(block, axis, step):
    count = lax.axis_size(axis)
    return lax.ppermute(block, axis, [(i, (i + step) % count) for i in range(count)])


HBM = pltpu.HBM


def exchange(block, axis, step):
    count = lax.axis_size(axis)
    if count & (count - 1):
        return shift_along(block, axis, step)
    return lax.ppermute(block, axis, [(i, i ^ step) for i in range(count)])


def origin(axis, step):
    count = lax.axis_size(axis)
    index = lax.axis_index(axis)
    if count & (count - 1):
        return lax.rem(index - step + count, count)
    return jnp.bitwise_xor(index, step)


def target(axis, step):
    count = lax.axis_size(axis)
    index = lax.axis_index(axis)
    if count & (count - 1):
        return lax.rem(index + step, count)
    return jnp.bitwise_xor(index, step)


def whole(memory_space=VMEM):
    return pl.BlockSpec(memory_space=memory_space)


def call(kernel, out_shape, *, vmem=16 << 20, flops=0, **kwargs):
    cost = pl.CostEstimate(flops=flops, transcendentals=0, bytes_accessed=0)
    return pl.pallas_call(
        kernel,
        out_shape=out_shape,
        compiler_params=pltpu.CompilerParams(vmem_limit_bytes=vmem),
        cost_estimate=cost if flops else None,
        **kwargs,
    )


def in_hbm(values):
    return [pltpu.with_memory_space_constraint(value, HBM) for value in values]


def array(shape, dtype=bf16):
    return jax.ShapeDtypeStruct(tuple(shape), dtype)


def modulation_kernel(*refs):
    inputs, (out_ref, gain_ref, line_ref, cond_ref, ctx_ref, act_ref, weights_ref, sems) = refs[:6], refs[6:]
    rows = weights_ref.shape[1]
    mine = pl.ds(pl.multiple_of(lax.axis_index("sp") * rows, LANES), rows)
    targets = (cond_ref, ctx_ref, *(weights_ref.at[i] for i in range(3)), line_ref)
    copies = [
        pltpu.make_async_copy(source, target, sems.at[index])
        for index, (source, target) in enumerate(zip(inputs, targets))
    ]
    for copy in copies:
        copy.start()

    act_ref[...] = jnp.zeros_like(act_ref)
    for row, ref in enumerate((cond_ref, ctx_ref)):
        copies[row].wait()
        v = ref[...].reshape(1, -1).astype(f32)
        act_ref[row : row + 1, :] = v / (1.0 + jnp.exp(-v))
    both = act_ref[:, mine].astype(bf16)
    for index in range(3):
        copies[2 + index].wait()
        terms = jnp.dot(both, weights_ref[index], preferred_element_type=f32)
        out_ref[2 * index : 2 * index + 2, :] = terms[0:2]
    out_ref[6:8, :] = jnp.zeros_like(out_ref[6:8, :])
    copies[5].wait()
    gain_ref[...] = line_ref[...].reshape(gain_ref.shape).astype(f32)


def modulation_terms(condition, context_condition, *rest):
    rows, width = rest[0].shape
    whole_line = VMEM(condition.shape, bf16)
    return call(
        modulation_kernel,
        [array((8, width), f32), array((1, *rest[-1].shape), f32)],
        in_specs=[whole(HBM)] * 6,
        out_specs=[whole()] * 2,
        scratch_shapes=[
            whole_line,
            whole_line,
            whole_line,
            VMEM((16, *condition.shape), f32),
            VMEM((3, rows, width), bf16),
            pltpu.SemaphoreType.DMA((6,)),
        ],
        flops=3_000_000_000,
    )(*in_hbm((condition, context_condition, *rest)))


def sum_kernel(token_ref, *refs):
    total = refs[0][...]
    for ref in refs[1:-1]:
        total += ref[...]
    refs[-1][...] = total


def summed_terms(token, partials):
    return call(
        sum_kernel,
        array(partials[0].shape, f32),
        in_specs=[whole()] * (1 + len(partials)),
        out_specs=whole(),
    )(token, *partials)


def rows_kernel(token_ref, source_ref, *refs):
    table_ref, bias_ref, lines_ref, sems = refs[-4:]
    count = (len(refs) - 4) // 2
    pairs = [(source_ref, bias_ref), *zip(refs[:count], refs[count:-4])]
    copies = [
        pltpu.make_async_copy(source, target, sems.at[index])
        for index, (source, target) in enumerate(pairs)
    ]
    for copy in copies:
        copy.start()
    copies[0].wait()
    heads = bias_ref.shape[1]
    for head in range(heads):
        lines_ref[:, :] = jnp.zeros_like(lines_ref)
        lines_ref[0:ROW_OFFSETS, 0:COL_OFFSETS] = bias_ref[:, head, :] * log2e
        lines = lines_ref[...]
        first = pltpu.roll(lines, LANES - (WIN_COLS - 1), 1)
        second = pltpu.roll(lines, GRID_W - (WIN_COLS - 1), 1)
        for pair in range((ROW_OFFSETS + 1) // 2):
            line = first[2 * pair : 2 * pair + 1] + second[2 * pair + 1 : 2 * pair + 2]
            line = jnp.broadcast_to(line, (GRID_W, LANES))
            table_ref[head * GRID_W : (head + 1) * GRID_W, pair * LANES : (pair + 1) * LANES] = (
                pltpu.roll(line, 0, 1, stride=1, stride_axis=0)
            )
    for copy in copies[1:]:
        copy.wait()


def bias_rows(token, offset_bias, *weights):
    heads = offset_bias.shape[0]
    rows = (ROW_OFFSETS + 1) * GRID_W
    return call(
        rows_kernel,
        [array(weight.shape) for weight in weights] + [array((heads * HEAD_DIM, rows), f32)],
        in_specs=[whole()] + [whole(HBM)] * (1 + len(weights)),
        out_specs=[whole()] * (1 + len(weights)),
        scratch_shapes=[
            VMEM((ROW_OFFSETS, heads, COL_OFFSETS), f32),
            VMEM((ROW_OFFSETS + 1, LANES), f32),
            pltpu.SemaphoreType.DMA((1 + len(weights),)),
        ],
        flops=500_000_000,
    )(token, *in_hbm((jnp.transpose(offset_bias, (1, 0, 2)), *weights)))


def flip_kernel(token_ref, table_ref, *refs):
    *refs, out_ref, sems = refs
    count = len(refs) // 2
    copies = [
        pltpu.make_async_copy(refs[index], refs[count + index], sems.at[index])
        for index in range(count)
    ]
    for copy in copies:
        copy.start()
    width = table_ref.shape[0]
    key = lax.broadcasted_iota(jnp.int32, (LANES, LANES), 0) % GRID_W
    query = lax.broadcasted_iota(jnp.int32, (LANES, LANES), 1) % GRID_W
    first = jnp.clip(query - WIN_COLS // 2, 0, GRID_W - WIN_COLS)
    inside = (key >= first) & (key < first + WIN_COLS)
    for row in range((ROW_OFFSETS + 1) // 2):
        for col in range(width // LANES):
            rows, cols = slice(row * LANES, (row + 1) * LANES), slice(col * LANES, (col + 1) * LANES)
            out_ref[rows, cols] = jnp.where(inside, table_ref[cols, rows].T, masked_score)
    for copy in copies:
        copy.wait()


def bias_table(token, rows, *weights):
    return call(
        flip_kernel,
        [*(array(weight.shape) for weight in weights), array(rows.shape[::-1], f32)],
        in_specs=[whole()] * 2 + [whole(HBM)] * len(weights),
        out_specs=[whole()] * (1 + len(weights)),
        scratch_shapes=[pltpu.SemaphoreType.DMA((len(weights),))],
        flops=1_000_000_000,
    )(token, rows, *in_hbm(weights))


def modulators(pieces, gain_ref, scale_row, shift_row, a_ref, b_ref):
    width = pieces[0].shape[1]
    for step, piece in enumerate(pieces):
        owner = origin("tp", step)
        part = pl.ds(pl.multiple_of(owner * width, LANES), width)
        a_ref[:, part] = gain_ref[:, part] * (1.0 + piece[scale_row : scale_row + 1, :])
        b_ref[:, part] = piece[shift_row : shift_row + 1, :]


def modulated(x, a, b):
    values = x.astype(f32)
    inverse = lax.rsqrt(jnp.mean(values * values, axis=-1, keepdims=True) + epsilon)
    return ((values * inverse) * a + b).astype(bf16)


query_factor = log2e * HEAD_DIM ** (-0.5)


def edge_kernel(count, x_ref, context_ref, gain_ref, wk_ref, wv_ref, *rest):
    pieces = rest[:count]
    first_ref, second_ref, low_ref, high_ref, even_ref, odd_ref, far_ref, *rest = rest[count:]
    a_ref, b_ref, ac_ref, bc_ref = rest
    modulators(pieces, gain_ref, 3, 1, ac_ref, bc_ref)
    hidden = modulated(context_ref[...], ac_ref[...], bc_ref[...])
    far_ref[0] = jnp.dot(hidden, wk_ref[...], preferred_element_type=f32).astype(bf16)
    far_ref[1] = jnp.dot(hidden, wv_ref[...], preferred_element_type=f32).astype(bf16)
    modulators(pieces, gain_ref, 2, 0, a_ref, b_ref)
    scratch = (first_ref, second_ref)
    outs = (low_ref, high_ref)
    tokens = x_ref.shape[0]
    for start, ref in zip((0, tokens - TILE), scratch):
        ref[...] = modulated(x_ref[start : start + TILE], a_ref[...], b_ref[...])
    for ref, out_ref in zip(scratch, outs):
        out_ref[0] = jnp.dot(ref[...], wk_ref[...], preferred_element_type=f32).astype(bf16)
        out_ref[1] = jnp.dot(ref[...], wv_ref[...], preferred_element_type=f32).astype(bf16)
    even = lax.axis_index("sp") % 2 == 0
    even_ref[...] = jnp.where(even, high_ref[...], low_ref[...])
    odd_ref[...] = jnp.where(even, low_ref[...], high_ref[...])


def edge_projections(latent, context, gain, weights, pieces):
    width = latent.shape[1]
    out = weights[0].shape[1]
    return call(
        functools.partial(edge_kernel, len(pieces)),
        [
            *[array((TILE, width))] * 2,
            *[array((2, TILE, out))] * 4,
            array((2, context.shape[0], out)),
            array((1, width), f32),
            array((1, width), f32),
        ],
        in_specs=[whole()] * (5 + len(pieces)),
        out_specs=[whole()] * 9,
        scratch_shapes=[VMEM((1, width), f32)] * 2,
        flops=2_000_000_000,
    )(latent, context, gain, *weights[1:], *pieces)


def main_kernel(pad, x_ref, a_ref, b_ref, wq_ref, wk_ref, wv_ref, one_ref, two_ref, low_ref, high_ref, *rest):
    q_ref, k_ref, v_ref, *scratch = rest
    tokens, width = q_ref.shape
    tiles = tokens // TILE

    def load(index):
        rows = slice(index * TILE, (index + 1) * TILE)
        scratch[index % 2][...] = modulated(x_ref[rows], a_ref[...], b_ref[...])

    def values_at(start, values):
        turned = values.T
        start += pad
        v_ref[0, 0:width, start : start + TILE] = turned.astype(bf16)
        rolled = pltpu.roll(turned, TILE - GRID_W, 1).astype(bf16)
        v_ref[1, 0:width, start : start + TILE - GRID_W] = rolled[:, 0 : TILE - GRID_W]
        if start:
            v_ref[1, 0:width, start - GRID_W : start] = rolled[:, TILE - GRID_W :]

    def multiply(index):
        hidden = scratch[index % 2][...]
        keys = jnp.dot(hidden, wk_ref[...], preferred_element_type=f32).astype(bf16)
        values = jnp.dot(hidden, wv_ref[...], preferred_element_type=f32)
        rows = slice(index * TILE, (index + 1) * TILE)
        queries = jnp.dot(hidden, wq_ref[...], preferred_element_type=f32)
        q_ref[rows] = (queries * query_factor).astype(bf16)
        k_ref[pad + index * TILE : pad + (index + 1) * TILE] = keys
        values_at(index * TILE, values)

    load(1)
    for start, ref in ((0, one_ref), (tokens - TILE, two_ref)):
        queries = jnp.dot(ref[...], wq_ref[...], preferred_element_type=f32)
        q_ref[start : start + TILE] = (queries * query_factor).astype(bf16)
    k_ref[pad : pad + TILE] = low_ref[0]
    k_ref[pad + tokens - TILE : pad + tokens] = high_ref[0]
    for index in range(2):
        v_ref[index, width:, :] = jnp.ones((ONES, tokens + 2 * pad), bf16)
    values_at(0, low_ref[1].astype(f32))
    for index in range(1, tiles - 1):
        if index + 2 < tiles:
            load(index + 1)
        multiply(index)
    values_at(tokens - TILE, high_ref[1].astype(f32))
    if not pad:
        v_ref[1, 0:width, tokens - GRID_W :] = jnp.zeros((width, GRID_W), bf16)


def main_projections(latent, a, b, weights, edges, pad):
    tokens, width = latent.shape
    out = weights[0].shape[1]
    return call(
        functools.partial(main_kernel, pad),
        [
            array((tokens, out)),
            array((tokens + 2 * pad, out)),
            array((2, out + ONES, tokens + 2 * pad)),
        ],
        in_specs=[whole()] * 10,
        out_specs=[whole()] * 3,
        scratch_shapes=[VMEM((TILE, width), bf16), VMEM((TILE, width), bf16)],
        flops=5_000_000_000,
    )(latent, a, b, *weights, *edges)


def attend_rows(rows, q_ref, kc_ref, vc_ref, t_ref, out_ref, scores, probs, whole_rows=True):
    width = q_ref.shape[1]
    heads = width // HEAD_DIM
    lane_head = lax.broadcasted_iota(jnp.int32, (1, width), 1) // HEAD_DIM
    head_mask = [(lane_head == h).astype(f32).astype(bf16) for h in range(heads)]
    lower = lax.broadcasted_iota(jnp.int32, (HEAD_DIM, LANES), 1) < GRID_W
    dims = (((1,), (1,)), ((), ()))

    def score(index):
        row, k_ref, _, start, offset, _ = rows[index]
        s_ref = scores[index % len(scores)]
        q = q_ref[part(row * GRID_W, GRID_W, GRID_W), :]
        big = jnp.concatenate([q * mask for mask in head_mask], axis=0)
        keys = k_ref[part(start * GRID_W, GRID_W, NEAR), :]
        near = lax.dot_general(keys, big, dims, preferred_element_type=f32)
        near += t_ref[part(offset * GRID_W, GRID_W, NEAR), :]
        far = lax.dot_general(kc_ref[...], big, dims, preferred_element_type=f32)
        s_ref[0:NEAR, :] = near
        s_ref[NEAR:, :] = far
        return jnp.maximum(
            jnp.max(near, axis=0, keepdims=True), jnp.max(far, axis=0, keepdims=True)
        )

    def weigh(index, peak):
        s_ref, p_ref = scores[index % len(scores)], probs[index % len(probs)]
        p_ref[...] = jnp.exp2(s_ref[...] - peak).astype(bf16)

    def gather(index):
        _, _, v_ref, start, _, parity = rows[index]
        p_ref = probs[index % len(probs)]
        parity = start % 2 if parity is None else parity
        values = v_ref[parity, :, part(start // 2 * LANES, LANES, NEAR)]
        out = jnp.dot(values, p_ref[0:NEAR, :], preferred_element_type=f32)
        out += jnp.dot(vc_ref[...], p_ref[NEAR:, :], preferred_element_type=f32)
        return out[0:width] * (1.0 / out[width : width + 1])

    def store(index, left, right):
        row = rows[index][0] if whole_rows else index
        lanes = slice(row * GRID_W, row * GRID_W + LANES)
        for pair in range(heads // 2):
            cols = slice(pair * LANES, (pair + 1) * LANES)
            for half in range(2):
                at = slice(pair * LANES + half * HEAD_DIM, pair * LANES + (half + 1) * HEAD_DIM)
                a, b = left[at, cols], right[at, cols]
                if half == 0:
                    b = pltpu.roll(b, GRID_W, 1)
                else:
                    a = pltpu.roll(a, GRID_W, 1)
                out_ref[at, lanes] = jnp.where(lower, a, b).astype(bf16)

    peaks, outs = {}, {}
    for index in range(len(rows) + 2):
        if index < len(rows):
            peaks[index] = score(index)
        if 0 <= index - 1 < len(rows):
            weigh(index - 1, peaks.pop(index - 1))
        if 0 <= index - 2:
            outs[index - 2] = gather(index - 2)
            if (index - 2) % 2:
                store(index - 3, outs.pop(index - 3), outs.pop(index - 2))


def part(start, unit, size):
    if isinstance(start, int):
        return slice(start, start + size)
    return pl.ds(pl.multiple_of(start, unit), size)


def is_free(row, grid_rows):
    return HALO_ROWS <= row < grid_rows - HALO_ROWS


def phases(tokens):
    count = lax.axis_size("tp")
    share = tokens // count
    rows = range(tokens // GRID_W)
    if share % LANES or share < 2 * LANES:
        return rows, range(0)
    each = share // GRID_W
    late = [r for r in rows if (r < 2 if r < each else r % each >= each - 2)]
    return [r for r in rows if r not in late], late


def far_refs(contexts, kc_ref, vc_ref):
    width = kc_ref.shape[1]
    height = contexts[0].shape[1]
    for index, context in enumerate(contexts):
        kc_ref[index * height : (index + 1) * height] = context[0]
    far_values = jnp.concatenate([context[1] for context in contexts], axis=0)
    vc_ref[0:width, :] = far_values.astype(f32).T.astype(bf16)
    vc_ref[width:, :] = jnp.ones((ONES, vc_ref.shape[1]), bf16)


def row_plan(rows, grid_rows, sp_count, k_ref, v_ref, strips):
    own = lax.axis_index("sp") * grid_rows
    total = grid_rows * sp_count
    plan = []
    for row in rows:
        if is_free(row, grid_rows):
            plan.append((row, k_ref, v_ref, row - HALO_ROWS, WIN_ROWS - 1 - HALO_ROWS, None))
            continue
        kl_ref, kh_ref, vl_ref, vh_ref = strips
        first = jnp.clip(own + row - HALO_ROWS, 0, total - WIN_ROWS)
        offset = first - (own + row) + WIN_ROWS - 1
        if row < HALO_ROWS:
            plan.append((row, kl_ref, vl_ref, first - own + HALO_ROWS, offset, None))
        else:
            plan.append((row, kh_ref, vh_ref, first - own - (grid_rows - WIN_ROWS), offset, None))
    return plan


def inner_kernel(count, rows, q_ref, k_ref, v_ref, t_ref, *rest):
    contexts, (out_ref, kc_ref, vc_ref, *scratch) = rest[:count], rest[count:]
    far_refs(contexts, kc_ref, vc_ref)
    plan = row_plan(rows, q_ref.shape[0] // GRID_W, 0, k_ref, v_ref, None)
    attend_rows(plan, q_ref, kc_ref, vc_ref, t_ref, out_ref, scratch[0:2], scratch[2:4])


def fill_strips(k_ref, v_ref, first_ref, second_ref, strips):
    tokens, width = k_ref.shape
    kl_ref, kh_ref, vl_ref, vh_ref = strips
    strip = 3 * TILE
    ones = jnp.ones((ONES, strip), bf16)
    even = lax.axis_index("sp") % 2 == 0
    low_halo = jnp.where(even, second_ref[...], first_ref[...])
    high_halo = jnp.where(even, first_ref[...], second_ref[...])
    kl_ref[0:TILE] = low_halo[0]
    kl_ref[TILE:] = k_ref[0 : 2 * TILE]
    kh_ref[0 : 2 * TILE] = k_ref[tokens - 2 * TILE :]
    kh_ref[2 * TILE :] = high_halo[0]
    low = low_halo[1].astype(f32).T
    high = high_halo[1].astype(f32).T
    for ref in (vl_ref, vh_ref):
        ref[0, width:, :] = ones
        ref[1, width:, :] = ones
    rolled = pltpu.roll(low, TILE - GRID_W, 1).astype(bf16)
    vl_ref[0, 0:width, 0:TILE] = low.astype(bf16)
    vl_ref[0, 0:width, TILE:] = v_ref[0, 0:width, 0 : 2 * TILE]
    vl_ref[1, 0:width, 0 : TILE - GRID_W] = rolled[:, 0 : TILE - GRID_W]
    first = pltpu.roll(v_ref[0, 0:width, 0:LANES].astype(f32), GRID_W, 1).astype(bf16)
    vl_ref[1, 0:width, TILE - GRID_W : TILE] = first[:, GRID_W:]
    vl_ref[1, 0:width, TILE:] = v_ref[1, 0:width, 0 : 2 * TILE]
    rolled = pltpu.roll(high, TILE - GRID_W, 1).astype(bf16)
    vh_ref[0, 0:width, 0 : 2 * TILE] = v_ref[0, 0:width, tokens - 2 * TILE :]
    vh_ref[0, 0:width, 2 * TILE :] = high.astype(bf16)
    vh_ref[1, 0:width, 0 : 2 * TILE] = v_ref[1, 0:width, tokens - 2 * TILE :]
    vh_ref[1, 0:width, 2 * TILE - GRID_W : 2 * TILE] = rolled[:, TILE - GRID_W :]
    vh_ref[1, 0:width, 2 * TILE : strip - GRID_W] = rolled[:, 0 : TILE - GRID_W]
    vh_ref[1, 0:width, strip - GRID_W :] = jnp.zeros((width, GRID_W), bf16)


def split_blocks(out_ref, block_refs, late):
    for step, block_ref in enumerate(block_refs):
        size = block_ref.shape[1]
        owner = target("tp", step)
        share = out_ref.shape[1] // len(block_refs)
        inside = jnp.where(owner == 0, 0, share - size)
        inside = inside if late else share - size - inside
        start = owner * share + inside
        block_ref[...] = out_ref[:, part(start, LANES, size)]


def middle_kernel(rows, sp_count, done_ref, latent_ref, q_ref, k_ref, v_ref, kc_ref, vc_ref, t_ref, first_ref, second_ref, out_ref, own_ref, *rest):
    strips, block_refs, (sem, *scratch) = rest[:4], rest[4:-5], rest[-5:]
    share = own_ref.shape[0]
    mine = part(lax.axis_index("tp") * share, GRID_W, share)
    copy = pltpu.make_async_copy(latent_ref.at[mine], own_ref, sem)
    copy.start()
    fill_strips(k_ref, v_ref, first_ref, second_ref, strips)
    plan = row_plan(rows, q_ref.shape[0] // GRID_W, sp_count, k_ref, v_ref, strips)
    attend_rows(plan, q_ref, kc_ref, vc_ref, t_ref, out_ref, scratch[0:2], scratch[2:4])
    split_blocks(out_ref, block_refs, False)
    copy.wait()


def late_kernel(rows, sp_count, q_ref, k_ref, v_ref, kc_ref, vc_ref, t_ref, *rest):
    strips, block_refs, (out_ref, *scratch) = rest[:4], rest[4:-5], rest[-5:]
    plan = row_plan(rows, q_ref.shape[0] // GRID_W, sp_count, k_ref, v_ref, strips)
    attend_rows(plan, q_ref, kc_ref, vc_ref, t_ref, out_ref, scratch[0:2], scratch[2:4])
    split_blocks(out_ref, block_refs, True)


def attention_scratch(total, width):
    return [VMEM((total, width), f32)] * 2 + [VMEM((total, width), bf16)] * 2


def inner_attention(queries, keys, values, table, contexts):
    tokens, width = queries.shape
    far = len(contexts) * contexts[0].shape[1]
    rows = [r for r in phases(tokens)[0] if is_free(r, tokens // GRID_W)]
    rows = [r for r in rows if r ^ 1 in rows]
    return call(
        functools.partial(inner_kernel, len(contexts), rows),
        [array((width, tokens)), array((far, width)), array((width + ONES, far))],
        in_specs=[whole()] * (4 + len(contexts)),
        out_specs=[whole()] * 3,
        scratch_shapes=attention_scratch(NEAR + far, width),
        flops=4_000_000_000,
    )(queries, keys, values, table, *contexts)


def middle_attention(done, latent, queries, keys, values, far_keys, far_values, table, first, second):
    tokens, width = queries.shape
    strip = 3 * TILE
    count = lax.axis_size("tp")
    early, late = phases(tokens)
    rows = [
        r for r in early if not (is_free(r, tokens // GRID_W) and is_free(r ^ 1, tokens // GRID_W))
    ]
    block = array((width, len(early) * GRID_W // count))
    attended, own, *rest = call(
        functools.partial(middle_kernel, rows, lax.axis_size("sp")),
        [
            array((width, tokens)),
            array((tokens // count, latent.shape[1])),
            *[array((strip, width))] * 2,
            *[array((2, width + ONES, strip))] * 2,
            *[block] * (count if late else 0),
        ],
        in_specs=[whole(), whole(HBM)] + [whole()] * 8,
        out_specs=[whole()] * (6 + (count if late else 0)),
        input_output_aliases={0: 0},
        scratch_shapes=[pltpu.SemaphoreType.DMA]
        + attention_scratch(NEAR + far_keys.shape[0], width),
        flops=2_000_000_000,
    )(done, *in_hbm([latent]), queries, keys, values, far_keys, far_values, table, first, second)
    strips, blocks = rest[:4], rest[4:]
    if not late:
        share = tokens // count
        blocks = [
            lax.dynamic_slice_in_dim(attended, target("tp", step) * share, share, 1)
            for step in range(count)
        ]
    return own, strips, list(blocks)


def late_attention(queries, keys, values, far_keys, far_values, table, strips):
    tokens, width = queries.shape
    count = lax.axis_size("tp")
    late = phases(tokens)[1]
    if not late:
        return []
    return list(
        call(
            functools.partial(late_kernel, late, lax.axis_size("sp")),
            [array((width, len(late) * GRID_W // count))] * count,
            in_specs=[whole()] * 10,
            out_specs=[whole()] * count,
            scratch_shapes=[VMEM((width, tokens), bf16)]
            + attention_scratch(NEAR + far_keys.shape[0], width),
            flops=3_000_000_000,
        )(queries, keys, values, far_keys, far_values, table, *strips)
    )


def by_destination(tokens):
    each = tokens // GRID_W // 4
    return lax.axis_size("tp") == 4 and each % 2 == 0 and HALO_ROWS <= each


def free_target():
    return jnp.where(lax.axis_index("tp") < 2, 2, 1)


def halo_target():
    return jnp.where(lax.axis_index("tp") < 2, 3, 0)


def destination_plan(owner, tokens, sp_count, k_ref, v_ref, free):
    grid_rows = tokens // GRID_W
    each = grid_rows // 4
    own = lax.axis_index("sp") * grid_rows
    plan = []
    for index in range(each):
        row = owner * each + index
        if free:
            plan.append((row, k_ref, v_ref, row, WIN_ROWS - 1 - HALO_ROWS, index % 2))
            continue
        first = jnp.clip(own + row - HALO_ROWS, 0, grid_rows * sp_count - WIN_ROWS)
        offset = first - (own + row) + WIN_ROWS - 1
        plan.append((row, k_ref, v_ref, first - own + HALO_ROWS, offset, None))
    return plan


def first_kernel(count, k_in, v_in, q_ref, t_ref, *rest):
    contexts, (k_ref, v_ref, kc_ref, vc_ref, out_ref, *scratch) = rest[:count], rest[count:]
    far_refs(contexts, kc_ref, vc_ref)
    plan = destination_plan(free_target(), q_ref.shape[0], 0, k_ref, v_ref, True)
    attend_rows(
        plan, q_ref, kc_ref, vc_ref, t_ref, out_ref, scratch[0:2], scratch[2:4], whole_rows=False
    )


def second_kernel(sp_count, k_in, v_in, latent_ref, q_ref, kc_ref, vc_ref, t_ref, one_ref, two_ref, k_ref, v_ref, own_ref, out_ref, sem, *scratch):
    share = own_ref.shape[0]
    mine = part(lax.axis_index("tp") * share, GRID_W, share)
    copy = pltpu.make_async_copy(latent_ref.at[mine], own_ref, sem)
    copy.start()
    tokens, width = q_ref.shape
    even = lax.axis_index("sp") % 2 == 0
    low = jnp.where(even, two_ref[...], one_ref[...])
    high = jnp.where(even, one_ref[...], two_ref[...])
    end = TILE + tokens
    k_ref[0:TILE] = low[0]
    k_ref[end:] = high[0]
    turned = low[1].astype(f32).T
    rolled = pltpu.roll(turned, TILE - GRID_W, 1).astype(bf16)
    v_ref[0, 0:width, 0:TILE] = turned.astype(bf16)
    v_ref[1, 0:width, 0 : TILE - GRID_W] = rolled[:, 0 : TILE - GRID_W]
    turned = high[1].astype(f32).T
    rolled = pltpu.roll(turned, TILE - GRID_W, 1).astype(bf16)
    v_ref[0, 0:width, end:] = turned.astype(bf16)
    v_ref[1, 0:width, end - GRID_W : end] = rolled[:, TILE - GRID_W :]
    v_ref[1, 0:width, end : end + TILE - GRID_W] = rolled[:, 0 : TILE - GRID_W]
    v_ref[1, 0:width, end + TILE - GRID_W :] = jnp.zeros((width, GRID_W), bf16)
    plan = destination_plan(halo_target(), tokens, sp_count, k_ref, v_ref, False)
    attend_rows(
        plan, q_ref, kc_ref, vc_ref, t_ref, out_ref, scratch[0:2], scratch[2:4], whole_rows=False
    )
    copy.wait()


def near_kernel(step, sp_count, k_ref, v_ref, q_ref, kc_ref, vc_ref, t_ref, out_ref, *scratch):
    owner = target("tp", step)
    plan = destination_plan(owner, q_ref.shape[0], sp_count, k_ref, v_ref, False)
    attend_rows(
        plan, q_ref, kc_ref, vc_ref, t_ref, out_ref, scratch[0:2], scratch[2:4], whole_rows=False
    )


def destination_attention(latent, queries, keys, values, table, contexts, one, two):
    tokens, width = queries.shape
    far = len(contexts) * contexts[0].shape[1]
    sp_count = lax.axis_size("sp")
    share = tokens // 4
    scratch = attention_scratch(NEAR + far, width)
    padded = [array(keys.shape), array(values.shape)]
    keys, values, far_keys, far_values, block = call(
        functools.partial(first_kernel, len(contexts)),
        [*padded, array((far, width)), array((width + ONES, far)), array((width, share))],
        in_specs=[whole()] * (4 + len(contexts)),
        out_specs=[whole()] * 5,
        input_output_aliases={0: 0, 1: 1},
        scratch_shapes=scratch,
        flops=3_000_000_000,
    )(keys, values, queries, table, *contexts)
    x1 = exchange(block, "tp", 2)
    keys, values, own, block = call(
        functools.partial(second_kernel, sp_count),
        [*padded, array((share, latent.shape[1])), array((width, share))],
        in_specs=[whole()] * 2 + [whole(HBM)] + [whole()] * 6,
        out_specs=[whole()] * 4,
        input_output_aliases={0: 0, 1: 1},
        scratch_shapes=[pltpu.SemaphoreType.DMA] + scratch,
        flops=3_000_000_000,
    )(keys, values, *in_hbm([latent]), queries, far_keys, far_values, table, one, two)
    x2 = exchange(block, "tp", 2)
    blocks = []
    for step in (1, 0):
        blocks.append(
            call(
                functools.partial(near_kernel, step, sp_count),
                array((width, share)),
                in_specs=[whole()] * 6,
                out_specs=whole(),
                scratch_shapes=scratch,
                flops=3_000_000_000,
            )(keys, values, queries, far_keys, far_values, table)
        )
    neighbour = exchange(blocks[0], "tp", 1)
    passed1 = exchange(x1, "tp", 1)
    passed2 = exchange(x2, "tp", 1)
    return own, (blocks[1], neighbour, x1, x2, passed1, passed2)


def gather_kernel(x_ref, w_ref, *rest):
    pieces, blocks, (out_ref, gate_ref, held_ref, block_ref, sems) = rest[:4], rest[4:10], rest[10:]
    mine_ref, neighbour_ref, x1_ref, x2_ref, passed1_ref, passed2_ref = blocks
    height = mine_ref.shape[0]
    tile = w_ref.shape[1] // 4
    tp = lax.axis_index("tp")
    free = (tp == 1) | (tp == 2)
    for index in range(4):
        gate_ref[:, part(origin("tp", index) * tile, LANES, tile)] = pieces[index][4:5, :]
    values = (
        mine_ref[...],
        neighbour_ref[...],
        jnp.where(free, x1_ref[...], x2_ref[...]),
        jnp.where(free, passed1_ref[...], passed2_ref[...]),
    )
    for index, value in enumerate(values):
        rows = part(origin("tp", index) * height, LANES, height)
        block_ref[:, rows] = value.astype(f32).T.astype(bf16)
    copies = []
    for step in range(4):
        cols = slice(step * tile, (step + 1) * tile)
        total = jnp.dot(block_ref[...], w_ref[:, cols], preferred_element_type=f32)
        held_ref[:, cols] = (x_ref[:, cols].astype(f32) + gate_ref[:, cols] * total).astype(bf16)
        copies.append(
            pltpu.make_async_copy(held_ref.at[:, cols], out_ref.at[:, cols], sems.at[step])
        )
        copies[-1].start()
    for copy in copies:
        copy.wait()


def gathered_output(x, weight, blocks, pieces):
    share, width = x.shape
    return call(
        gather_kernel,
        array((share, width)),
        in_specs=[whole()] * 12,
        out_specs=whole(HBM),
        scratch_shapes=[
            VMEM((1, width), f32),
            VMEM((share, width), bf16),
            VMEM((share, weight.shape[0]), bf16),
            pltpu.SemaphoreType.DMA((4,)),
        ],
        flops=2_000_000_000,
    )(x, weight, *pieces, *blocks)


def output_kernel(count, late, *refs):
    x_ref, w_ref, *arrays, out_ref, gate_ref, held_ref, block_ref, sems = refs[late:]
    pieces, blocks = arrays[:count], arrays[count:]
    height, size = blocks[0].shape
    share = out_ref.shape[0]
    tile = w_ref.shape[1] // count
    tp = lax.axis_index("tp")
    for index in range(count):
        gate_ref[:, part(origin("tp", index) * tile, LANES, tile)] = pieces[index][4:5, :]
        rows = part(origin("tp", index) * height, LANES, height)
        block_ref[:, rows] = blocks[index][...].astype(f32).T.astype(bf16)
    inside = jnp.where(tp == 0, 0, share - size)
    inside = inside if late else share - size - inside
    mine = part(inside, GRID_W, size)
    copies = []
    for step in range(count):
        cols = slice(step * tile, (step + 1) * tile)
        total = jnp.dot(block_ref[...], w_ref[:, cols], preferred_element_type=f32)
        held_ref[:, cols] = (
            x_ref[mine, cols].astype(f32) + gate_ref[:, cols] * total
        ).astype(bf16)
        copies.append(
            pltpu.make_async_copy(held_ref.at[:, cols], out_ref.at[mine, cols], sems.at[step])
        )
        copies[-1].start()
    for copy in copies:
        copy.wait()


def output(x, weight, blocks, pieces, done=None):
    count = len(blocks)
    share, width = x.shape
    size = blocks[0].shape[1]
    late = done is not None
    return call(
        functools.partial(output_kernel, count, late),
        array((share, width)),
        in_specs=[whole(HBM)] * late + [whole()] * (2 + len(pieces) + len(blocks)),
        out_specs=whole(HBM),
        input_output_aliases={0: 0} if late else {},
        scratch_shapes=[
            VMEM((1, width), f32),
            VMEM((size, width), bf16),
            VMEM((size, weight.shape[0]), bf16),
            pltpu.SemaphoreType.DMA((count,)),
        ],
        flops=2_000_000_000,
    )(*([done] if late else []), x, weight, *pieces, *blocks)


def gathered(block, axis):
    blocks = [block]
    for step in range(1, lax.axis_size(axis)):
        blocks.append(exchange(block, axis, step))
    return blocks


def sent(blocks):
    return blocks[:1] + [exchange(blocks[step], "tp", step) for step in range(1, len(blocks))]


def local(
    latent,
    condition,
    context_tokens,
    context_condition,
    shift_weight,
    scale_weight,
    gate_weight,
    norm_gain,
    query_weight,
    key_weight,
    value_weight,
    out_weight,
    offset_bias,
):
    terms, gain = modulation_terms(
        condition, context_condition, shift_weight, scale_weight, gate_weight, norm_gain
    )
    partials = gathered(terms, "sp")
    wk, rows = bias_rows(terms, offset_bias, key_weight)
    summed = summed_terms(rows, partials)
    pieces = gathered(summed, "tp")
    wv, wq, table = bias_table(summed, rows, value_weight, query_weight)
    weights = (wq, wk, wv)
    *edges, far, a, b = edge_projections(
        latent, context_tokens, gain, weights, pieces
    )
    count = lax.axis_size("sp")
    contexts = gathered(far, "sp")
    pairs = [(i, i ^ 1) for i in range(count) if i ^ 1 < count]
    first = lax.ppermute(edges[4], "sp", pairs)
    pairs = [(i, j) for i in range(count) for j in [((i + 1) ^ 1) - 1] if 0 <= j < count]
    second = lax.ppermute(edges[5], "sp", pairs)
    special = by_destination(latent.shape[0])
    fields = main_projections(latent, a, b, weights, edges[:4], TILE if special else 0)
    if special:
        own, blocks = destination_attention(latent, *fields, table, contexts, first, second)
        return gathered_output(own, out_weight, blocks, pieces)
    inner, *fars = inner_attention(*fields, table, contexts)
    own, strips, early = middle_attention(inner, latent, *fields, *fars, table, first, second)
    early = sent(early)
    late = late_attention(*fields, *fars, table, strips)
    late = sent(late)
    done = output(own, out_weight, early, pieces)
    if not late:
        return done
    return output(own, out_weight, late, pieces, done)


def solution(mesh):
    placed = (
        P(("grp", "sp"), None),
        P("grp"),
        P(("grp", "sp"), None),
        P(),
        P("sp", "tp"),
        P("sp", "tp"),
        P("sp", "tp"),
        P(),
        P(None, "tp"),
        P(None, "tp"),
        P(None, "tp"),
        P(),
        P("tp", None, None),
    )
    return jax.shard_map(
        local, mesh=mesh, in_specs=placed, out_specs=P(("grp", "sp", "tp"), None), check_vma=False
    )
```

```python
import functools
import math

import jax
import jax.numpy as jnp
from jax import lax
from jax.experimental import pallas as pl
from jax.experimental.pallas import tpu as pltpu
from jax.sharding import PartitionSpec as P


HEAD_DIM = 64
GRID_W = 64
WIN_ROWS = 8
WIN_COLS = 16
ROW_OFFSETS = 2 * WIN_ROWS - 1
COL_OFFSETS = 2 * WIN_COLS - 1
LANES = 128
HALO_ROWS = WIN_ROWS // 2
TILE = HALO_ROWS * GRID_W
NEAR = WIN_ROWS * GRID_W
ONES = 16

epsilon = 1e-06
masked_score = -1e30
log2e = math.log2(math.e)
VMEM = pltpu.VMEM
f32 = jnp.float32
bf16 = jnp.bfloat16


def shift_along(block, axis, step):
    count = lax.axis_size(axis)
    return lax.ppermute(block, axis, [(i, (i + step) % count) for i in range(count)])


HBM = pltpu.HBM


def exchange(block, axis, step):
    count = lax.axis_size(axis)
    if count & (count - 1):
        return shift_along(block, axis, step)
    return lax.ppermute(block, axis, [(i, i ^ step) for i in range(count)])


def origin(axis, step):
    count = lax.axis_size(axis)
    index = lax.axis_index(axis)
    if count & (count - 1):
        return lax.rem(index - step + count, count)
    return jnp.bitwise_xor(index, step)


def target(axis, step):
    count = lax.axis_size(axis)
    index = lax.axis_index(axis)
    if count & (count - 1):
        return lax.rem(index + step, count)
    return jnp.bitwise_xor(index, step)


def whole(memory_space=VMEM):
    return pl.BlockSpec(memory_space=memory_space)


def call(kernel, out_shape, *, vmem=16 << 20, flops=0, **kwargs):
    cost = pl.CostEstimate(flops=flops, transcendentals=0, bytes_accessed=0)
    return pl.pallas_call(
        kernel,
        out_shape=out_shape,
        compiler_params=pltpu.CompilerParams(vmem_limit_bytes=vmem),
        cost_estimate=cost if flops else None,
        **kwargs,
    )


def in_hbm(values):
    return [pltpu.with_memory_space_constraint(value, HBM) for value in values]


def array(shape, dtype=bf16):
    return jax.ShapeDtypeStruct(tuple(shape), dtype)


def modulation_kernel(*refs):
    inputs, (out_ref, gain_ref, line_ref, cond_ref, ctx_ref, act_ref, weights_ref, sems) = refs[:6], refs[6:]
    rows = weights_ref.shape[1]
    mine = pl.ds(pl.multiple_of(lax.axis_index("sp") * rows, LANES), rows)
    targets = (cond_ref, ctx_ref, *(weights_ref.at[i] for i in range(3)), line_ref)
    copies = [
        pltpu.make_async_copy(source, target, sems.at[index])
        for index, (source, target) in enumerate(zip(inputs, targets))
    ]
    for copy in copies:
        copy.start()

    act_ref[...] = jnp.zeros_like(act_ref)
    for row, ref in enumerate((cond_ref, ctx_ref)):
        copies[row].wait()
        v = ref[...].reshape(1, -1).astype(f32)
        act_ref[row : row + 1, :] = v / (1.0 + jnp.exp(-v))
    both = act_ref[:, mine].astype(bf16)
    for index in range(3):
        copies[2 + index].wait()
        terms = jnp.dot(both, weights_ref[index], preferred_element_type=f32)
        out_ref[2 * index : 2 * index + 2, :] = terms[0:2]
    out_ref[6:8, :] = jnp.zeros_like(out_ref[6:8, :])
    copies[5].wait()
    gain_ref[...] = line_ref[...].reshape(gain_ref.shape).astype(f32)


def modulation_terms(condition, context_condition, *rest):
    rows, width = rest[0].shape
    whole_line = VMEM(condition.shape, bf16)
    return call(
        modulation_kernel,
        [array((8, width), f32), array((1, *rest[-1].shape), f32)],
        in_specs=[whole(HBM)] * 6,
        out_specs=[whole()] * 2,
        scratch_shapes=[
            whole_line,
            whole_line,
            whole_line,
            VMEM((16, *condition.shape), f32),
            VMEM((3, rows, width), bf16),
            pltpu.SemaphoreType.DMA((6,)),
        ],
        flops=3_000_000_000,
    )(*in_hbm((condition, context_condition, *rest)))


def sum_kernel(token_ref, *refs):
    total = refs[0][...]
    for ref in refs[1:-1]:
        total += ref[...]
    refs[-1][...] = total


def summed_terms(token, partials):
    return call(
        sum_kernel,
        array(partials[0].shape, f32),
        in_specs=[whole()] * (1 + len(partials)),
        out_specs=whole(),
    )(token, *partials)


def rows_kernel(token_ref, source_ref, *refs):
    table_ref, bias_ref, lines_ref, sems = refs[-4:]
    count = (len(refs) - 4) // 2
    pairs = [(source_ref, bias_ref), *zip(refs[:count], refs[count:-4])]
    copies = [
        pltpu.make_async_copy(source, target, sems.at[index])
        for index, (source, target) in enumerate(pairs)
    ]
    for copy in copies:
        copy.start()
    copies[0].wait()
    heads = bias_ref.shape[1]
    for head in range(heads):
        lines_ref[:, :] = jnp.zeros_like(lines_ref)
        lines_ref[0:ROW_OFFSETS, 0:COL_OFFSETS] = bias_ref[:, head, :] * log2e
        lines = lines_ref[...]
        first = pltpu.roll(lines, LANES - (WIN_COLS - 1), 1)
        second = pltpu.roll(lines, GRID_W - (WIN_COLS - 1), 1)
        for pair in range((ROW_OFFSETS + 1) // 2):
            line = first[2 * pair : 2 * pair + 1] + second[2 * pair + 1 : 2 * pair + 2]
            line = jnp.broadcast_to(line, (GRID_W, LANES))
            table_ref[head * GRID_W : (head + 1) * GRID_W, pair * LANES : (pair + 1) * LANES] = (
                pltpu.roll(line, 0, 1, stride=1, stride_axis=0)
            )
    for copy in copies[1:]:
        copy.wait()


def bias_rows(token, offset_bias, *weights):
    heads = offset_bias.shape[0]
    rows = (ROW_OFFSETS + 1) * GRID_W
    return call(
        rows_kernel,
        [array(weight.shape) for weight in weights] + [array((heads * HEAD_DIM, rows), f32)],
        in_specs=[whole()] + [whole(HBM)] * (1 + len(weights)),
        out_specs=[whole()] * (1 + len(weights)),
        scratch_shapes=[
            VMEM((ROW_OFFSETS, heads, COL_OFFSETS), f32),
            VMEM((ROW_OFFSETS + 1, LANES), f32),
            pltpu.SemaphoreType.DMA((1 + len(weights),)),
        ],
        flops=500_000_000,
    )(token, *in_hbm((jnp.transpose(offset_bias, (1, 0, 2)), *weights)))


def flip_kernel(token_ref, table_ref, *refs):
    *refs, out_ref, sems = refs
    count = len(refs) // 2
    copies = [
        pltpu.make_async_copy(refs[index], refs[count + index], sems.at[index])
        for index in range(count)
    ]
    for copy in copies:
        copy.start()
    width = table_ref.shape[0]
    key = lax.broadcasted_iota(jnp.int32, (LANES, LANES), 0) % GRID_W
    query = lax.broadcasted_iota(jnp.int32, (LANES, LANES), 1) % GRID_W
    first = jnp.clip(query - WIN_COLS // 2, 0, GRID_W - WIN_COLS)
    inside = (key >= first) & (key < first + WIN_COLS)
    for row in range((ROW_OFFSETS + 1) // 2):
        for col in range(width // LANES):
            rows, cols = slice(row * LANES, (row + 1) * LANES), slice(col * LANES, (col + 1) * LANES)
            out_ref[rows, cols] = jnp.where(inside, table_ref[cols, rows].T, masked_score)
    for copy in copies:
        copy.wait()


def bias_table(token, rows, *weights):
    return call(
        flip_kernel,
        [*(array(weight.shape) for weight in weights), array(rows.shape[::-1], f32)],
        in_specs=[whole()] * 2 + [whole(HBM)] * len(weights),
        out_specs=[whole()] * (1 + len(weights)),
        scratch_shapes=[pltpu.SemaphoreType.DMA((len(weights),))],
        flops=1_000_000_000,
    )(token, rows, *in_hbm(weights))


def modulators(pieces, gain_ref, scale_row, shift_row, a_ref, b_ref):
    width = pieces[0].shape[1]
    for step, piece in enumerate(pieces):
        owner = origin("tp", step)
        part = pl.ds(pl.multiple_of(owner * width, LANES), width)
        a_ref[:, part] = gain_ref[:, part] * (1.0 + piece[scale_row : scale_row + 1, :])
        b_ref[:, part] = piece[shift_row : shift_row + 1, :]


def modulated(x, a, b):
    values = x.astype(f32)
    inverse = lax.rsqrt(jnp.mean(values * values, axis=-1, keepdims=True) + epsilon)
    return ((values * inverse) * a + b).astype(bf16)


query_factor = log2e * HEAD_DIM ** (-0.5)


def edge_kernel(count, x_ref, context_ref, gain_ref, wk_ref, wv_ref, *rest):
    pieces = rest[:count]
    first_ref, second_ref, low_ref, high_ref, even_ref, odd_ref, far_ref, *rest = rest[count:]
    a_ref, b_ref, ac_ref, bc_ref = rest
    modulators(pieces, gain_ref, 3, 1, ac_ref, bc_ref)
    hidden = modulated(context_ref[...], ac_ref[...], bc_ref[...])
    far_ref[0] = jnp.dot(hidden, wk_ref[...], preferred_element_type=f32).astype(bf16)
    far_ref[1] = jnp.dot(hidden, wv_ref[...], preferred_element_type=f32).astype(bf16)
    modulators(pieces, gain_ref, 2, 0, a_ref, b_ref)
    scratch = (first_ref, second_ref)
    outs = (low_ref, high_ref)
    tokens = x_ref.shape[0]
    for start, ref in zip((0, tokens - TILE), scratch):
        ref[...] = modulated(x_ref[start : start + TILE], a_ref[...], b_ref[...])
    for ref, out_ref in zip(scratch, outs):
        out_ref[0] = jnp.dot(ref[...], wk_ref[...], preferred_element_type=f32).astype(bf16)
        out_ref[1] = jnp.dot(ref[...], wv_ref[...], preferred_element_type=f32).astype(bf16)
    even = lax.axis_index("sp") % 2 == 0
    even_ref[...] = jnp.where(even, high_ref[...], low_ref[...])
    odd_ref[...] = jnp.where(even, low_ref[...], high_ref[...])


def edge_projections(latent, context, gain, weights, pieces):
    width = latent.shape[1]
    out = weights[0].shape[1]
    return call(
        functools.partial(edge_kernel, len(pieces)),
        [
            *[array((TILE, width))] * 2,
            *[array((2, TILE, out))] * 4,
            array((2, context.shape[0], out)),
            array((1, width), f32),
            array((1, width), f32),
        ],
        in_specs=[whole()] * (5 + len(pieces)),
        out_specs=[whole()] * 9,
        scratch_shapes=[VMEM((1, width), f32)] * 2,
        flops=2_000_000_000,
    )(latent, context, gain, *weights[1:], *pieces)


def main_kernel(pad, x_ref, a_ref, b_ref, wq_ref, wk_ref, wv_ref, one_ref, two_ref, low_ref, high_ref, *rest):
    q_ref, k_ref, v_ref, *scratch = rest
    tokens, width = q_ref.shape
    tiles = tokens // TILE

    def load(index):
        rows = slice(index * TILE, (index + 1) * TILE)
        scratch[index % 2][...] = modulated(x_ref[rows], a_ref[...], b_ref[...])

    def values_at(start, values):
        turned = values.T
        start += pad
        v_ref[0, 0:width, start : start + TILE] = turned.astype(bf16)
        rolled = pltpu.roll(turned, TILE - GRID_W, 1).astype(bf16)
        v_ref[1, 0:width, start : start + TILE - GRID_W] = rolled[:, 0 : TILE - GRID_W]
        if start:
            v_ref[1, 0:width, start - GRID_W : start] = rolled[:, TILE - GRID_W :]

    def multiply(index):
        hidden = scratch[index % 2][...]
        keys = jnp.dot(hidden, wk_ref[...], preferred_element_type=f32).astype(bf16)
        values = jnp.dot(hidden, wv_ref[...], preferred_element_type=f32)
        rows = slice(index * TILE, (index + 1) * TILE)
        queries = jnp.dot(hidden, wq_ref[...], preferred_element_type=f32)
        q_ref[rows] = (queries * query_factor).astype(bf16)
        k_ref[pad + index * TILE : pad + (index + 1) * TILE] = keys
        values_at(index * TILE, values)

    load(1)
    for start, ref in ((0, one_ref), (tokens - TILE, two_ref)):
        queries = jnp.dot(ref[...], wq_ref[...], preferred_element_type=f32)
        q_ref[start : start + TILE] = (queries * query_factor).astype(bf16)
    k_ref[pad : pad + TILE] = low_ref[0]
    k_ref[pad + tokens - TILE : pad + tokens] = high_ref[0]
    for index in range(2):
        v_ref[index, width:, :] = jnp.ones((ONES, tokens + 2 * pad), bf16)
    values_at(0, low_ref[1].astype(f32))
    for index in range(1, tiles - 1):
        if index + 2 < tiles:
            load(index + 1)
        multiply(index)
    values_at(tokens - TILE, high_ref[1].astype(f32))
    if not pad:
        v_ref[1, 0:width, tokens - GRID_W :] = jnp.zeros((width, GRID_W), bf16)


def main_projections(latent, a, b, weights, edges, pad):
    tokens, width = latent.shape
    out = weights[0].shape[1]
    return call(
        functools.partial(main_kernel, pad),
        [
            array((tokens, out)),
            array((tokens + 2 * pad, out)),
            array((2, out + ONES, tokens + 2 * pad)),
        ],
        in_specs=[whole()] * 10,
        out_specs=[whole()] * 3,
        scratch_shapes=[VMEM((TILE, width), bf16), VMEM((TILE, width), bf16)],
        flops=5_000_000_000,
    )(latent, a, b, *weights, *edges)


def attend_rows(rows, q_ref, kc_ref, vc_ref, t_ref, out_ref, scores, probs, whole_rows=True):
    width = q_ref.shape[1]
    heads = width // HEAD_DIM
    lane_head = lax.broadcasted_iota(jnp.int32, (1, width), 1) // HEAD_DIM
    head_mask = [(lane_head == h).astype(f32).astype(bf16) for h in range(heads)]
    lower = lax.broadcasted_iota(jnp.int32, (HEAD_DIM, LANES), 1) < GRID_W
    dims = (((1,), (1,)), ((), ()))

    def score(index):
        row, k_ref, _, start, offset, _ = rows[index]
        s_ref = scores[index % len(scores)]
        q = q_ref[part(row * GRID_W, GRID_W, GRID_W), :]
        big = jnp.concatenate([q * mask for mask in head_mask], axis=0)
        keys = k_ref[part(start * GRID_W, GRID_W, NEAR), :]
        near = lax.dot_general(keys, big, dims, preferred_element_type=f32)
        near += t_ref[part(offset * GRID_W, GRID_W, NEAR), :]
        far = lax.dot_general(kc_ref[...], big, dims, preferred_element_type=f32)
        s_ref[0:NEAR, :] = near
        s_ref[NEAR:, :] = far
        return jnp.maximum(
            jnp.max(near, axis=0, keepdims=True), jnp.max(far, axis=0, keepdims=True)
        )

    def weigh(index, peak):
        s_ref, p_ref = scores[index % len(scores)], probs[index % len(probs)]
        p_ref[...] = jnp.exp2(s_ref[...] - peak).astype(bf16)

    def gather(index):
        _, _, v_ref, start, _, parity = rows[index]
        p_ref = probs[index % len(probs)]
        parity = start % 2 if parity is None else parity
        values = v_ref[parity, :, part(start // 2 * LANES, LANES, NEAR)]
        out = jnp.dot(values, p_ref[0:NEAR, :], preferred_element_type=f32)
        out += jnp.dot(vc_ref[...], p_ref[NEAR:, :], preferred_element_type=f32)
        return out[0:width] * (1.0 / out[width : width + 1])

    def store(index, left, right):
        row = rows[index][0] if whole_rows else index
        lanes = slice(row * GRID_W, row * GRID_W + LANES)
        for pair in range(heads // 2):
            cols = slice(pair * LANES, (pair + 1) * LANES)
            for half in range(2):
                at = slice(pair * LANES + half * HEAD_DIM, pair * LANES + (half + 1) * HEAD_DIM)
                a, b = left[at, cols], right[at, cols]
                if half == 0:
                    b = pltpu.roll(b, GRID_W, 1)
                else:
                    a = pltpu.roll(a, GRID_W, 1)
                out_ref[at, lanes] = jnp.where(lower, a, b).astype(bf16)

    peaks, outs = {}, {}
    for index in range(len(rows) + 2):
        if index < len(rows):
            peaks[index] = score(index)
        if 0 <= index - 1 < len(rows):
            weigh(index - 1, peaks.pop(index - 1))
        if 0 <= index - 2:
            outs[index - 2] = gather(index - 2)
            if (index - 2) % 2:
                store(index - 3, outs.pop(index - 3), outs.pop(index - 2))


def part(start, unit, size):
    if isinstance(start, int):
        return slice(start, start + size)
    return pl.ds(pl.multiple_of(start, unit), size)


def is_free(row, grid_rows):
    return HALO_ROWS <= row < grid_rows - HALO_ROWS


def phases(tokens):
    count = lax.axis_size("tp")
    share = tokens // count
    rows = range(tokens // GRID_W)
    if share % LANES or share < 2 * LANES:
        return rows, range(0)
    each = share // GRID_W
    late = [r for r in rows if (r < 2 if r < each else r % each >= each - 2)]
    return [r for r in rows if r not in late], late


def far_refs(contexts, kc_ref, vc_ref):
    width = kc_ref.shape[1]
    height = contexts[0].shape[1]
    for index, context in enumerate(contexts):
        kc_ref[index * height : (index + 1) * height] = context[0]
    far_values = jnp.concatenate([context[1] for context in contexts], axis=0)
    vc_ref[0:width, :] = far_values.astype(f32).T.astype(bf16)
    vc_ref[width:, :] = jnp.ones((ONES, vc_ref.shape[1]), bf16)


def row_plan(rows, grid_rows, sp_count, k_ref, v_ref, strips):
    own = lax.axis_index("sp") * grid_rows
    total = grid_rows * sp_count
    plan = []
    for row in rows:
        if is_free(row, grid_rows):
            plan.append((row, k_ref, v_ref, row - HALO_ROWS, WIN_ROWS - 1 - HALO_ROWS, None))
            continue
        kl_ref, kh_ref, vl_ref, vh_ref = strips
        first = jnp.clip(own + row - HALO_ROWS, 0, total - WIN_ROWS)
        offset = first - (own + row) + WIN_ROWS - 1
        if row < HALO_ROWS:
            plan.append((row, kl_ref, vl_ref, first - own + HALO_ROWS, offset, None))
        else:
            plan.append((row, kh_ref, vh_ref, first - own - (grid_rows - WIN_ROWS), offset, None))
    return plan


def inner_kernel(count, rows, q_ref, k_ref, v_ref, t_ref, *rest):
    contexts, (out_ref, kc_ref, vc_ref, *scratch) = rest[:count], rest[count:]
    far_refs(contexts, kc_ref, vc_ref)
    plan = row_plan(rows, q_ref.shape[0] // GRID_W, 0, k_ref, v_ref, None)
    attend_rows(plan, q_ref, kc_ref, vc_ref, t_ref, out_ref, scratch[0:2], scratch[2:4])


def fill_strips(k_ref, v_ref, first_ref, second_ref, strips):
    tokens, width = k_ref.shape
    kl_ref, kh_ref, vl_ref, vh_ref = strips
    strip = 3 * TILE
    ones = jnp.ones((ONES, strip), bf16)
    even = lax.axis_index("sp") % 2 == 0
    low_halo = jnp.where(even, second_ref[...], first_ref[...])
    high_halo = jnp.where(even, first_ref[...], second_ref[...])
    kl_ref[0:TILE] = low_halo[0]
    kl_ref[TILE:] = k_ref[0 : 2 * TILE]
    kh_ref[0 : 2 * TILE] = k_ref[tokens - 2 * TILE :]
    kh_ref[2 * TILE :] = high_halo[0]
    low = low_halo[1].astype(f32).T
    high = high_halo[1].astype(f32).T
    for ref in (vl_ref, vh_ref):
        ref[0, width:, :] = ones
        ref[1, width:, :] = ones
    rolled = pltpu.roll(low, TILE - GRID_W, 1).astype(bf16)
    vl_ref[0, 0:width, 0:TILE] = low.astype(bf16)
    vl_ref[0, 0:width, TILE:] = v_ref[0, 0:width, 0 : 2 * TILE]
    vl_ref[1, 0:width, 0 : TILE - GRID_W] = rolled[:, 0 : TILE - GRID_W]
    first = pltpu.roll(v_ref[0, 0:width, 0:LANES].astype(f32), GRID_W, 1).astype(bf16)
    vl_ref[1, 0:width, TILE - GRID_W : TILE] = first[:, GRID_W:]
    vl_ref[1, 0:width, TILE:] = v_ref[1, 0:width, 0 : 2 * TILE]
    rolled = pltpu.roll(high, TILE - GRID_W, 1).astype(bf16)
    vh_ref[0, 0:width, 0 : 2 * TILE] = v_ref[0, 0:width, tokens - 2 * TILE :]
    vh_ref[0, 0:width, 2 * TILE :] = high.astype(bf16)
    vh_ref[1, 0:width, 0 : 2 * TILE] = v_ref[1, 0:width, tokens - 2 * TILE :]
    vh_ref[1, 0:width, 2 * TILE - GRID_W : 2 * TILE] = rolled[:, TILE - GRID_W :]
    vh_ref[1, 0:width, 2 * TILE : strip - GRID_W] = rolled[:, 0 : TILE - GRID_W]
    vh_ref[1, 0:width, strip - GRID_W :] = jnp.zeros((width, GRID_W), bf16)


def split_blocks(out_ref, block_refs, late):
    for step, block_ref in enumerate(block_refs):
        size = block_ref.shape[1]
        owner = target("tp", step)
        share = out_ref.shape[1] // len(block_refs)
        inside = jnp.where(owner == 0, 0, share - size)
        inside = inside if late else share - size - inside
        start = owner * share + inside
        block_ref[...] = out_ref[:, part(start, LANES, size)]


def middle_kernel(rows, sp_count, done_ref, latent_ref, q_ref, k_ref, v_ref, kc_ref, vc_ref, t_ref, first_ref, second_ref, out_ref, own_ref, *rest):
    strips, block_refs, (sem, *scratch) = rest[:4], rest[4:-5], rest[-5:]
    share = own_ref.shape[0]
    mine = part(lax.axis_index("tp") * share, GRID_W, share)
    copy = pltpu.make_async_copy(latent_ref.at[mine], own_ref, sem)
    copy.start()
    fill_strips(k_ref, v_ref, first_ref, second_ref, strips)
    plan = row_plan(rows, q_ref.shape[0] // GRID_W, sp_count, k_ref, v_ref, strips)
    attend_rows(plan, q_ref, kc_ref, vc_ref, t_ref, out_ref, scratch[0:2], scratch[2:4])
    split_blocks(out_ref, block_refs, False)
    copy.wait()


def late_kernel(rows, sp_count, q_ref, k_ref, v_ref, kc_ref, vc_ref, t_ref, *rest):
    strips, block_refs, (out_ref, *scratch) = rest[:4], rest[4:-5], rest[-5:]
    plan = row_plan(rows, q_ref.shape[0] // GRID_W, sp_count, k_ref, v_ref, strips)
    attend_rows(plan, q_ref, kc_ref, vc_ref, t_ref, out_ref, scratch[0:2], scratch[2:4])
    split_blocks(out_ref, block_refs, True)


def attention_scratch(total, width):
    return [VMEM((total, width), f32)] * 2 + [VMEM((total, width), bf16)] * 2


def inner_attention(queries, keys, values, table, contexts):
    tokens, width = queries.shape
    far = len(contexts) * contexts[0].shape[1]
    rows = [r for r in phases(tokens)[0] if is_free(r, tokens // GRID_W)]
    rows = [r for r in rows if r ^ 1 in rows]
    return call(
        functools.partial(inner_kernel, len(contexts), rows),
        [array((width, tokens)), array((far, width)), array((width + ONES, far))],
        in_specs=[whole()] * (4 + len(contexts)),
        out_specs=[whole()] * 3,
        scratch_shapes=attention_scratch(NEAR + far, width),
        flops=4_000_000_000,
    )(queries, keys, values, table, *contexts)


def middle_attention(done, latent, queries, keys, values, far_keys, far_values, table, first, second):
    tokens, width = queries.shape
    strip = 3 * TILE
    count = lax.axis_size("tp")
    early, late = phases(tokens)
    rows = [
        r for r in early if not (is_free(r, tokens // GRID_W) and is_free(r ^ 1, tokens // GRID_W))
    ]
    block = array((width, len(early) * GRID_W // count))
    attended, own, *rest = call(
        functools.partial(middle_kernel, rows, lax.axis_size("sp")),
        [
            array((width, tokens)),
            array((tokens // count, latent.shape[1])),
            *[array((strip, width))] * 2,
            *[array((2, width + ONES, strip))] * 2,
            *[block] * (count if late else 0),
        ],
        in_specs=[whole(), whole(HBM)] + [whole()] * 8,
        out_specs=[whole()] * (6 + (count if late else 0)),
        input_output_aliases={0: 0},
        scratch_shapes=[pltpu.SemaphoreType.DMA]
        + attention_scratch(NEAR + far_keys.shape[0], width),
        flops=2_000_000_000,
    )(done, *in_hbm([latent]), queries, keys, values, far_keys, far_values, table, first, second)
    strips, blocks = rest[:4], rest[4:]
    if not late:
        share = tokens // count
        blocks = [
            lax.dynamic_slice_in_dim(attended, target("tp", step) * share, share, 1)
            for step in range(count)
        ]
    return own, strips, list(blocks)


def late_attention(queries, keys, values, far_keys, far_values, table, strips):
    tokens, width = queries.shape
    count = lax.axis_size("tp")
    late = phases(tokens)[1]
    if not late:
        return []
    return list(
        call(
            functools.partial(late_kernel, late, lax.axis_size("sp")),
            [array((width, len(late) * GRID_W // count))] * count,
            in_specs=[whole()] * 10,
            out_specs=[whole()] * count,
            scratch_shapes=[VMEM((width, tokens), bf16)]
            + attention_scratch(NEAR + far_keys.shape[0], width),
            flops=3_000_000_000,
        )(queries, keys, values, far_keys, far_values, table, *strips)
    )


def by_destination(tokens):
    each = tokens // GRID_W // 4
    return lax.axis_size("tp") == 4 and each % 2 == 0 and HALO_ROWS <= each


def free_target():
    return jnp.where(lax.axis_index("tp") < 2, 2, 1)


def halo_target():
    return jnp.where(lax.axis_index("tp") < 2, 3, 0)


def destination_plan(owner, tokens, sp_count, k_ref, v_ref, free):
    grid_rows = tokens // GRID_W
    each = grid_rows // 4
    own = lax.axis_index("sp") * grid_rows
    plan = []
    for index in range(each):
        row = owner * each + index
        if free:
            plan.append((row, k_ref, v_ref, row, WIN_ROWS - 1 - HALO_ROWS, index % 2))
            continue
        first = jnp.clip(own + row - HALO_ROWS, 0, grid_rows * sp_count - WIN_ROWS)
        offset = first - (own + row) + WIN_ROWS - 1
        plan.append((row, k_ref, v_ref, first - own + HALO_ROWS, offset, None))
    return plan


def first_kernel(count, k_in, v_in, q_ref, t_ref, *rest):
    contexts, (k_ref, v_ref, kc_ref, vc_ref, out_ref, *scratch) = rest[:count], rest[count:]
    far_refs(contexts, kc_ref, vc_ref)
    plan = destination_plan(free_target(), q_ref.shape[0], 0, k_ref, v_ref, True)
    attend_rows(
        plan, q_ref, kc_ref, vc_ref, t_ref, out_ref, scratch[0:2], scratch[2:4], whole_rows=False
    )


def second_kernel(sp_count, k_in, v_in, q_ref, kc_ref, vc_ref, t_ref, one_ref, two_ref, k_ref, v_ref, out_ref, *scratch):
    tokens, width = q_ref.shape
    even = lax.axis_index("sp") % 2 == 0
    low = jnp.where(even, two_ref[...], one_ref[...])
    high = jnp.where(even, one_ref[...], two_ref[...])
    end = TILE + tokens
    k_ref[0:TILE] = low[0]
    k_ref[end:] = high[0]
    turned = low[1].astype(f32).T
    rolled = pltpu.roll(turned, TILE - GRID_W, 1).astype(bf16)
    v_ref[0, 0:width, 0:TILE] = turned.astype(bf16)
    v_ref[1, 0:width, 0 : TILE - GRID_W] = rolled[:, 0 : TILE - GRID_W]
    turned = high[1].astype(f32).T
    rolled = pltpu.roll(turned, TILE - GRID_W, 1).astype(bf16)
    v_ref[0, 0:width, end:] = turned.astype(bf16)
    v_ref[1, 0:width, end - GRID_W : end] = rolled[:, TILE - GRID_W :]
    v_ref[1, 0:width, end : end + TILE - GRID_W] = rolled[:, 0 : TILE - GRID_W]
    v_ref[1, 0:width, end + TILE - GRID_W :] = jnp.zeros((width, GRID_W), bf16)
    plan = destination_plan(halo_target(), tokens, sp_count, k_ref, v_ref, False)
    attend_rows(
        plan, q_ref, kc_ref, vc_ref, t_ref, out_ref, scratch[0:2], scratch[2:4], whole_rows=False
    )


def near_kernel(step, sp_count, k_ref, v_ref, q_ref, kc_ref, vc_ref, t_ref, out_ref, *scratch):
    owner = target("tp", step)
    plan = destination_plan(owner, q_ref.shape[0], sp_count, k_ref, v_ref, False)
    attend_rows(
        plan, q_ref, kc_ref, vc_ref, t_ref, out_ref, scratch[0:2], scratch[2:4], whole_rows=False
    )


def destination_attention(queries, keys, values, table, contexts, one, two):
    tokens, width = queries.shape
    far = len(contexts) * contexts[0].shape[1]
    sp_count = lax.axis_size("sp")
    share = tokens // 4
    scratch = attention_scratch(NEAR + far, width)
    padded = [array(keys.shape), array(values.shape)]
    keys, values, far_keys, far_values, block = call(
        functools.partial(first_kernel, len(contexts)),
        [*padded, array((far, width)), array((width + ONES, far)), array((width, share))],
        in_specs=[whole()] * (4 + len(contexts)),
        out_specs=[whole()] * 5,
        input_output_aliases={0: 0, 1: 1},
        scratch_shapes=scratch,
        flops=3_000_000_000,
    )(keys, values, queries, table, *contexts)
    x1 = exchange(block, "tp", 2)
    keys, values, block = call(
        functools.partial(second_kernel, sp_count),
        [*padded, array((width, share))],
        in_specs=[whole()] * 8,
        out_specs=[whole()] * 3,
        input_output_aliases={0: 0, 1: 1},
        scratch_shapes=scratch,
        flops=3_000_000_000,
    )(keys, values, queries, far_keys, far_values, table, one, two)
    x2 = exchange(block, "tp", 2)
    blocks = []
    for step in (1, 0):
        blocks.append(
            call(
                functools.partial(near_kernel, step, sp_count),
                array((width, share)),
                in_specs=[whole()] * 6,
                out_specs=whole(),
                scratch_shapes=scratch,
                flops=3_000_000_000,
            )(keys, values, queries, far_keys, far_values, table)
        )
    neighbour = exchange(blocks[0], "tp", 1)
    passed1 = exchange(x1, "tp", 1)
    passed2 = exchange(x2, "tp", 1)
    return blocks[1], neighbour, x1, x2, passed1, passed2


def gather_kernel(x_ref, w_ref, *rest):
    pieces, blocks, (out_ref, gate_ref, held_ref, block_ref, sems) = rest[:4], rest[4:10], rest[10:]
    mine_ref, neighbour_ref, x1_ref, x2_ref, passed1_ref, passed2_ref = blocks
    height = mine_ref.shape[0]
    tile = w_ref.shape[1] // 4
    tp = lax.axis_index("tp")
    free = (tp == 1) | (tp == 2)
    mine = part(tp * held_ref.shape[0], GRID_W, held_ref.shape[0])
    for index in range(4):
        gate_ref[:, part(origin("tp", index) * tile, LANES, tile)] = pieces[index][4:5, :]
    values = (
        mine_ref[...],
        neighbour_ref[...],
        jnp.where(free, x1_ref[...], x2_ref[...]),
        jnp.where(free, passed1_ref[...], passed2_ref[...]),
    )
    for index, value in enumerate(values):
        rows = part(origin("tp", index) * height, LANES, height)
        block_ref[:, rows] = value.astype(f32).T.astype(bf16)
    copies = []
    for step in range(4):
        cols = slice(step * tile, (step + 1) * tile)
        total = jnp.dot(block_ref[...], w_ref[:, cols], preferred_element_type=f32)
        held_ref[:, cols] = (x_ref[mine, cols].astype(f32) + gate_ref[:, cols] * total).astype(bf16)
        copies.append(
            pltpu.make_async_copy(held_ref.at[:, cols], out_ref.at[:, cols], sems.at[step])
        )
        copies[-1].start()
    for copy in copies:
        copy.wait()


def gathered_output(x, weight, blocks, pieces):
    share, width = x.shape[0] // 4, x.shape[1]
    return call(
        gather_kernel,
        array((share, width)),
        in_specs=[whole()] * 12,
        out_specs=whole(HBM),
        scratch_shapes=[
            VMEM((1, width), f32),
            VMEM((share, width), bf16),
            VMEM((share, weight.shape[0]), bf16),
            pltpu.SemaphoreType.DMA((4,)),
        ],
        flops=2_000_000_000,
    )(x, weight, *pieces, *blocks)


def output_kernel(count, late, *refs):
    x_ref, w_ref, *arrays, out_ref, gate_ref, held_ref, block_ref, sems = refs[late:]
    pieces, blocks = arrays[:count], arrays[count:]
    height, size = blocks[0].shape
    share = out_ref.shape[0]
    tile = w_ref.shape[1] // count
    tp = lax.axis_index("tp")
    for index in range(count):
        gate_ref[:, part(origin("tp", index) * tile, LANES, tile)] = pieces[index][4:5, :]
        rows = part(origin("tp", index) * height, LANES, height)
        block_ref[:, rows] = blocks[index][...].astype(f32).T.astype(bf16)
    inside = jnp.where(tp == 0, 0, share - size)
    inside = inside if late else share - size - inside
    mine = part(inside, GRID_W, size)
    copies = []
    for step in range(count):
        cols = slice(step * tile, (step + 1) * tile)
        total = jnp.dot(block_ref[...], w_ref[:, cols], preferred_element_type=f32)
        held_ref[:, cols] = (
            x_ref[mine, cols].astype(f32) + gate_ref[:, cols] * total
        ).astype(bf16)
        copies.append(
            pltpu.make_async_copy(held_ref.at[:, cols], out_ref.at[mine, cols], sems.at[step])
        )
        copies[-1].start()
    for copy in copies:
        copy.wait()


def output(x, weight, blocks, pieces, done=None):
    count = len(blocks)
    share, width = x.shape
    size = blocks[0].shape[1]
    late = done is not None
    return call(
        functools.partial(output_kernel, count, late),
        array((share, width)),
        in_specs=[whole(HBM)] * late + [whole()] * (2 + len(pieces) + len(blocks)),
        out_specs=whole(HBM),
        input_output_aliases={0: 0} if late else {},
        scratch_shapes=[
            VMEM((1, width), f32),
            VMEM((size, width), bf16),
            VMEM((size, weight.shape[0]), bf16),
            pltpu.SemaphoreType.DMA((count,)),
        ],
        flops=2_000_000_000,
    )(*([done] if late else []), x, weight, *pieces, *blocks)


def gathered(block, axis):
    blocks = [block]
    for step in range(1, lax.axis_size(axis)):
        blocks.append(exchange(block, axis, step))
    return blocks


def sent(blocks):
    return blocks[:1] + [exchange(blocks[step], "tp", step) for step in range(1, len(blocks))]


def local(
    latent,
    condition,
    context_tokens,
    context_condition,
    shift_weight,
    scale_weight,
    gate_weight,
    norm_gain,
    query_weight,
    key_weight,
    value_weight,
    out_weight,
    offset_bias,
):
    terms, gain = modulation_terms(
        condition, context_condition, shift_weight, scale_weight, gate_weight, norm_gain
    )
    partials = gathered(terms, "sp")
    wk, rows = bias_rows(terms, offset_bias, key_weight)
    summed = summed_terms(rows, partials)
    pieces = gathered(summed, "tp")
    wv, wq, table = bias_table(summed, rows, value_weight, query_weight)
    weights = (wq, wk, wv)
    *edges, far, a, b = edge_projections(
        latent, context_tokens, gain, weights, pieces
    )
    count = lax.axis_size("sp")
    contexts = gathered(far, "sp")
    pairs = [(i, i ^ 1) for i in range(count) if i ^ 1 < count]
    first = lax.ppermute(edges[4], "sp", pairs)
    pairs = [(i, j) for i in range(count) for j in [((i + 1) ^ 1) - 1] if 0 <= j < count]
    second = lax.ppermute(edges[5], "sp", pairs)
    special = by_destination(latent.shape[0])
    fields = main_projections(latent, a, b, weights, edges[:4], TILE if special else 0)
    if special:
        blocks = destination_attention(*fields, table, contexts, first, second)
        return gathered_output(latent, out_weight, blocks, pieces)
    inner, *fars = inner_attention(*fields, table, contexts)
    own, strips, early = middle_attention(inner, latent, *fields, *fars, table, first, second)
    early = sent(early)
    late = late_attention(*fields, *fars, table, strips)
    late = sent(late)
    done = output(own, out_weight, early, pieces)
    if not late:
        return done
    return output(own, out_weight, late, pieces, done)


def solution(mesh):
    placed = (
        P(("grp", "sp"), None),
        P("grp"),
        P(("grp", "sp"), None),
        P(),
        P("sp", "tp"),
        P("sp", "tp"),
        P("sp", "tp"),
        P(),
        P(None, "tp"),
        P(None, "tp"),
        P(None, "tp"),
        P(),
        P("tp", None, None),
    )
    return jax.shard_map(
        local, mesh=mesh, in_specs=placed, out_specs=P(("grp", "sp", "tp"), None), check_vma=False
    )
```

```python
import functools
import math

import jax
import jax.numpy as jnp
from jax import lax
from jax.experimental import pallas as pl
from jax.experimental.pallas import tpu as pltpu
from jax.sharding import PartitionSpec as P


HEAD_DIM = 64
GRID_W = 64
WIN_ROWS = 8
WIN_COLS = 16
ROW_OFFSETS = 2 * WIN_ROWS - 1
COL_OFFSETS = 2 * WIN_COLS - 1
LANES = 128
HALO_ROWS = WIN_ROWS // 2
TILE = HALO_ROWS * GRID_W
NEAR = WIN_ROWS * GRID_W
ONES = 16

epsilon = 1e-06
masked_score = -1e30
log2e = math.log2(math.e)
VMEM = pltpu.VMEM
f32 = jnp.float32
bf16 = jnp.bfloat16


def shift_along(block, axis, step):
    count = lax.axis_size(axis)
    return lax.ppermute(block, axis, [(i, (i + step) % count) for i in range(count)])


HBM = pltpu.HBM


def exchange(block, axis, step):
    count = lax.axis_size(axis)
    if count & (count - 1):
        return shift_along(block, axis, step)
    return lax.ppermute(block, axis, [(i, i ^ step) for i in range(count)])


def origin(axis, step):
    count = lax.axis_size(axis)
    index = lax.axis_index(axis)
    if count & (count - 1):
        return lax.rem(index - step + count, count)
    return jnp.bitwise_xor(index, step)


def target(axis, step):
    count = lax.axis_size(axis)
    index = lax.axis_index(axis)
    if count & (count - 1):
        return lax.rem(index + step, count)
    return jnp.bitwise_xor(index, step)


def whole(memory_space=VMEM):
    return pl.BlockSpec(memory_space=memory_space)


def call(kernel, out_shape, *, vmem=16 << 20, flops=0, **kwargs):
    cost = pl.CostEstimate(flops=flops, transcendentals=0, bytes_accessed=0)
    return pl.pallas_call(
        kernel,
        out_shape=out_shape,
        compiler_params=pltpu.CompilerParams(vmem_limit_bytes=vmem),
        cost_estimate=cost if flops else None,
        **kwargs,
    )


def in_hbm(values):
    return [pltpu.with_memory_space_constraint(value, HBM) for value in values]


def array(shape, dtype=bf16):
    return jax.ShapeDtypeStruct(tuple(shape), dtype)


def modulation_kernel(*refs):
    inputs, (out_ref, gain_ref, line_ref, cond_ref, ctx_ref, act_ref, weights_ref, sems) = refs[:6], refs[6:]
    rows = weights_ref.shape[1]
    mine = pl.ds(pl.multiple_of(lax.axis_index("sp") * rows, LANES), rows)
    targets = (cond_ref, ctx_ref, *(weights_ref.at[i] for i in range(3)), line_ref)
    copies = [
        pltpu.make_async_copy(source, target, sems.at[index])
        for index, (source, target) in enumerate(zip(inputs, targets))
    ]
    for copy in copies:
        copy.start()

    act_ref[...] = jnp.zeros_like(act_ref)
    for row, ref in enumerate((cond_ref, ctx_ref)):
        copies[row].wait()
        v = ref[...].reshape(1, -1).astype(f32)
        act_ref[row : row + 1, :] = v / (1.0 + jnp.exp(-v))
    both = act_ref[:, mine].astype(bf16)
    for index in range(3):
        copies[2 + index].wait()
        terms = jnp.dot(both, weights_ref[index], preferred_element_type=f32)
        out_ref[2 * index : 2 * index + 2, :] = terms[0:2]
    out_ref[6:8, :] = jnp.zeros_like(out_ref[6:8, :])
    copies[5].wait()
    gain_ref[...] = line_ref[...].reshape(gain_ref.shape).astype(f32)


def modulation_terms(condition, context_condition, *rest):
    rows, width = rest[0].shape
    whole_line = VMEM(condition.shape, bf16)
    return call(
        modulation_kernel,
        [array((8, width), f32), array((1, *rest[-1].shape), f32)],
        in_specs=[whole(HBM)] * 6,
        out_specs=[whole()] * 2,
        scratch_shapes=[
            whole_line,
            whole_line,
            whole_line,
            VMEM((16, *condition.shape), f32),
            VMEM((3, rows, width), bf16),
            pltpu.SemaphoreType.DMA((6,)),
        ],
        flops=3_000_000_000,
    )(*in_hbm((condition, context_condition, *rest)))


def sum_kernel(token_ref, *refs):
    total = refs[0][...]
    for ref in refs[1:-1]:
        total += ref[...]
    refs[-1][...] = total


def summed_terms(token, partials):
    return call(
        sum_kernel,
        array(partials[0].shape, f32),
        in_specs=[whole()] * (1 + len(partials)),
        out_specs=whole(),
    )(token, *partials)


def rows_kernel(token_ref, source_ref, *refs):
    table_ref, bias_ref, lines_ref, sems = refs[-4:]
    count = (len(refs) - 4) // 2
    pairs = [(source_ref, bias_ref), *zip(refs[:count], refs[count:-4])]
    copies = [
        pltpu.make_async_copy(source, target, sems.at[index])
        for index, (source, target) in enumerate(pairs)
    ]
    for copy in copies:
        copy.start()
    copies[0].wait()
    heads = bias_ref.shape[1]
    for head in range(heads):
        lines_ref[:, :] = jnp.zeros_like(lines_ref)
        lines_ref[0:ROW_OFFSETS, 0:COL_OFFSETS] = bias_ref[:, head, :] * log2e
        lines = lines_ref[...]
        first = pltpu.roll(lines, LANES - (WIN_COLS - 1), 1)
        second = pltpu.roll(lines, GRID_W - (WIN_COLS - 1), 1)
        for pair in range((ROW_OFFSETS + 1) // 2):
            line = first[2 * pair : 2 * pair + 1] + second[2 * pair + 1 : 2 * pair + 2]
            line = jnp.broadcast_to(line, (GRID_W, LANES))
            table_ref[head * GRID_W : (head + 1) * GRID_W, pair * LANES : (pair + 1) * LANES] = (
                pltpu.roll(line, 0, 1, stride=1, stride_axis=0)
            )
    for copy in copies[1:]:
        copy.wait()


def bias_rows(token, offset_bias, *weights):
    heads = offset_bias.shape[0]
    rows = (ROW_OFFSETS + 1) * GRID_W
    return call(
        rows_kernel,
        [array(weight.shape) for weight in weights] + [array((heads * HEAD_DIM, rows), f32)],
        in_specs=[whole()] + [whole(HBM)] * (1 + len(weights)),
        out_specs=[whole()] * (1 + len(weights)),
        scratch_shapes=[
            VMEM((ROW_OFFSETS, heads, COL_OFFSETS), f32),
            VMEM((ROW_OFFSETS + 1, LANES), f32),
            pltpu.SemaphoreType.DMA((1 + len(weights),)),
        ],
        flops=500_000_000,
    )(token, *in_hbm((jnp.transpose(offset_bias, (1, 0, 2)), *weights)))


def flip_kernel(token_ref, table_ref, *refs):
    *refs, out_ref, sems = refs
    count = len(refs) // 2
    copies = [
        pltpu.make_async_copy(refs[index], refs[count + index], sems.at[index])
        for index in range(count)
    ]
    for copy in copies:
        copy.start()
    width = table_ref.shape[0]
    key = lax.broadcasted_iota(jnp.int32, (LANES, LANES), 0) % GRID_W
    query = lax.broadcasted_iota(jnp.int32, (LANES, LANES), 1) % GRID_W
    first = jnp.clip(query - WIN_COLS // 2, 0, GRID_W - WIN_COLS)
    inside = (key >= first) & (key < first + WIN_COLS)
    for row in range((ROW_OFFSETS + 1) // 2):
        for col in range(width // LANES):
            rows, cols = slice(row * LANES, (row + 1) * LANES), slice(col * LANES, (col + 1) * LANES)
            out_ref[rows, cols] = jnp.where(inside, table_ref[cols, rows].T, masked_score)
    for copy in copies:
        copy.wait()


def bias_table(token, rows, *weights):
    return call(
        flip_kernel,
        [*(array(weight.shape) for weight in weights), array(rows.shape[::-1], f32)],
        in_specs=[whole()] * 2 + [whole(HBM)] * len(weights),
        out_specs=[whole()] * (1 + len(weights)),
        scratch_shapes=[pltpu.SemaphoreType.DMA((len(weights),))],
        flops=1_000_000_000,
    )(token, rows, *in_hbm(weights))


def modulators(pieces, gain_ref, scale_row, shift_row, a_ref, b_ref):
    width = pieces[0].shape[1]
    for step, piece in enumerate(pieces):
        owner = origin("tp", step)
        part = pl.ds(pl.multiple_of(owner * width, LANES), width)
        a_ref[:, part] = gain_ref[:, part] * (1.0 + piece[scale_row : scale_row + 1, :])
        b_ref[:, part] = piece[shift_row : shift_row + 1, :]


def modulated(x, a, b):
    values = x.astype(f32)
    inverse = lax.rsqrt(jnp.mean(values * values, axis=-1, keepdims=True) + epsilon)
    return ((values * inverse) * a + b).astype(bf16)


query_factor = log2e * HEAD_DIM ** (-0.5)


def edge_kernel(count, x_ref, context_ref, gain_ref, wk_ref, wv_ref, *rest):
    pieces = rest[:count]
    first_ref, second_ref, low_ref, high_ref, even_ref, odd_ref, far_ref, *rest = rest[count:]
    a_ref, b_ref, ac_ref, bc_ref = rest
    modulators(pieces, gain_ref, 3, 1, ac_ref, bc_ref)
    hidden = modulated(context_ref[...], ac_ref[...], bc_ref[...])
    far_ref[0] = jnp.dot(hidden, wk_ref[...], preferred_element_type=f32).astype(bf16)
    far_ref[1] = jnp.dot(hidden, wv_ref[...], preferred_element_type=f32).astype(bf16)
    modulators(pieces, gain_ref, 2, 0, a_ref, b_ref)
    scratch = (first_ref, second_ref)
    outs = (low_ref, high_ref)
    tokens = x_ref.shape[0]
    for start, ref in zip((0, tokens - TILE), scratch):
        ref[...] = modulated(x_ref[start : start + TILE], a_ref[...], b_ref[...])
    for ref, out_ref in zip(scratch, outs):
        out_ref[0] = jnp.dot(ref[...], wk_ref[...], preferred_element_type=f32).astype(bf16)
        out_ref[1] = jnp.dot(ref[...], wv_ref[...], preferred_element_type=f32).astype(bf16)
    even = lax.axis_index("sp") % 2 == 0
    even_ref[...] = jnp.where(even, high_ref[...], low_ref[...])
    odd_ref[...] = jnp.where(even, low_ref[...], high_ref[...])


def edge_projections(latent, context, gain, weights, pieces):
    width = latent.shape[1]
    out = weights[0].shape[1]
    return call(
        functools.partial(edge_kernel, len(pieces)),
        [
            *[array((TILE, width))] * 2,
            *[array((2, TILE, out))] * 4,
            array((2, context.shape[0], out)),
            array((1, width), f32),
            array((1, width), f32),
        ],
        in_specs=[whole()] * (5 + len(pieces)),
        out_specs=[whole()] * 9,
        scratch_shapes=[VMEM((1, width), f32)] * 2,
        flops=2_000_000_000,
    )(latent, context, gain, *weights[1:], *pieces)


def main_kernel(pad, x_ref, a_ref, b_ref, wq_ref, wk_ref, wv_ref, one_ref, two_ref, low_ref, high_ref, *rest):
    q_ref, k_ref, v_ref, *scratch = rest
    tokens, width = q_ref.shape
    tiles = tokens // TILE

    def load(index):
        rows = slice(index * TILE, (index + 1) * TILE)
        scratch[index % 2][...] = modulated(x_ref[rows], a_ref[...], b_ref[...])

    def values_at(start, values):
        turned = values.T
        start += pad
        v_ref[0, 0:width, start : start + TILE] = turned.astype(bf16)
        rolled = pltpu.roll(turned, TILE - GRID_W, 1).astype(bf16)
        v_ref[1, 0:width, start : start + TILE - GRID_W] = rolled[:, 0 : TILE - GRID_W]
        if start:
            v_ref[1, 0:width, start - GRID_W : start] = rolled[:, TILE - GRID_W :]

    def multiply(index):
        hidden = scratch[index % 2][...]
        keys = jnp.dot(hidden, wk_ref[...], preferred_element_type=f32).astype(bf16)
        values = jnp.dot(hidden, wv_ref[...], preferred_element_type=f32)
        rows = slice(index * TILE, (index + 1) * TILE)
        queries = jnp.dot(hidden, wq_ref[...], preferred_element_type=f32)
        q_ref[rows] = (queries * query_factor).astype(bf16)
        k_ref[pad + index * TILE : pad + (index + 1) * TILE] = keys
        values_at(index * TILE, values)

    load(1)
    for start, ref in ((0, one_ref), (tokens - TILE, two_ref)):
        queries = jnp.dot(ref[...], wq_ref[...], preferred_element_type=f32)
        q_ref[start : start + TILE] = (queries * query_factor).astype(bf16)
    k_ref[pad : pad + TILE] = low_ref[0]
    k_ref[pad + tokens - TILE : pad + tokens] = high_ref[0]
    for index in range(2):
        v_ref[index, width:, :] = jnp.ones((ONES, tokens + 2 * pad), bf16)
    values_at(0, low_ref[1].astype(f32))
    for index in range(1, tiles - 1):
        if index + 2 < tiles:
            load(index + 1)
        multiply(index)
    values_at(tokens - TILE, high_ref[1].astype(f32))
    if not pad:
        v_ref[1, 0:width, tokens - GRID_W :] = jnp.zeros((width, GRID_W), bf16)


def main_projections(latent, a, b, weights, edges, pad):
    tokens, width = latent.shape
    out = weights[0].shape[1]
    return call(
        functools.partial(main_kernel, pad),
        [
            array((tokens, out)),
            array((tokens + 2 * pad, out)),
            array((2, out + ONES, tokens + 2 * pad)),
        ],
        in_specs=[whole()] * 10,
        out_specs=[whole()] * 3,
        scratch_shapes=[VMEM((TILE, width), bf16), VMEM((TILE, width), bf16)],
        flops=5_000_000_000,
    )(latent, a, b, *weights, *edges)


def attend_rows(rows, q_ref, kc_ref, vc_ref, t_ref, out_ref, scores, probs, whole_rows=True):
    width = q_ref.shape[1]
    heads = width // HEAD_DIM
    lane_head = lax.broadcasted_iota(jnp.int32, (1, width), 1) // HEAD_DIM
    head_mask = [(lane_head == h).astype(f32).astype(bf16) for h in range(heads)]
    lower = lax.broadcasted_iota(jnp.int32, (HEAD_DIM, LANES), 1) < GRID_W
    dims = (((1,), (1,)), ((), ()))

    def score(index):
        row, k_ref, _, start, offset, _ = rows[index]
        s_ref = scores[index % len(scores)]
        q = q_ref[part(row * GRID_W, GRID_W, GRID_W), :]
        big = jnp.concatenate([q * mask for mask in head_mask], axis=0)
        keys = k_ref[part(start * GRID_W, GRID_W, NEAR), :]
        near = lax.dot_general(keys, big, dims, preferred_element_type=f32)
        near += t_ref[part(offset * GRID_W, GRID_W, NEAR), :]
        far = lax.dot_general(kc_ref[...], big, dims, preferred_element_type=f32)
        s_ref[0:NEAR, :] = near
        s_ref[NEAR:, :] = far
        return jnp.maximum(
            jnp.max(near, axis=0, keepdims=True), jnp.max(far, axis=0, keepdims=True)
        )

    def weigh(index, peak):
        s_ref, p_ref = scores[index % len(scores)], probs[index % len(probs)]
        p_ref[...] = jnp.exp2(s_ref[...] - peak).astype(bf16)

    def gather(index):
        _, _, v_ref, start, _, parity = rows[index]
        p_ref = probs[index % len(probs)]
        parity = start % 2 if parity is None else parity
        values = v_ref[parity, :, part(start // 2 * LANES, LANES, NEAR)]
        out = jnp.dot(values, p_ref[0:NEAR, :], preferred_element_type=f32)
        out += jnp.dot(vc_ref[...], p_ref[NEAR:, :], preferred_element_type=f32)
        return out[0:width] * (1.0 / out[width : width + 1])

    def store(index, left, right):
        row = rows[index][0] if whole_rows else index
        lanes = slice(row * GRID_W, row * GRID_W + LANES)
        for pair in range(heads // 2):
            cols = slice(pair * LANES, (pair + 1) * LANES)
            for half in range(2):
                at = slice(pair * LANES + half * HEAD_DIM, pair * LANES + (half + 1) * HEAD_DIM)
                a, b = left[at, cols], right[at, cols]
                if half == 0:
                    b = pltpu.roll(b, GRID_W, 1)
                else:
                    a = pltpu.roll(a, GRID_W, 1)
                out_ref[at, lanes] = jnp.where(lower, a, b).astype(bf16)

    peaks, outs = {}, {}
    for index in range(len(rows) + 2):
        if 0 <= index - 2:
            outs[index - 2] = gather(index - 2)
            if (index - 2) % 2:
                store(index - 3, outs.pop(index - 3), outs.pop(index - 2))
        if 0 <= index - 1 < len(rows):
            weigh(index - 1, peaks.pop(index - 1))
        if index < len(rows):
            peaks[index] = score(index)


def part(start, unit, size):
    if isinstance(start, int):
        return slice(start, start + size)
    return pl.ds(pl.multiple_of(start, unit), size)


def is_free(row, grid_rows):
    return HALO_ROWS <= row < grid_rows - HALO_ROWS


def phases(tokens):
    count = lax.axis_size("tp")
    share = tokens // count
    rows = range(tokens // GRID_W)
    if share % LANES or share < 2 * LANES:
        return rows, range(0)
    each = share // GRID_W
    late = [r for r in rows if (r < 2 if r < each else r % each >= each - 2)]
    return [r for r in rows if r not in late], late


def far_refs(contexts, kc_ref, vc_ref):
    width = kc_ref.shape[1]
    height = contexts[0].shape[1]
    for index, context in enumerate(contexts):
        kc_ref[index * height : (index + 1) * height] = context[0]
    far_values = jnp.concatenate([context[1] for context in contexts], axis=0)
    vc_ref[0:width, :] = far_values.astype(f32).T.astype(bf16)
    vc_ref[width:, :] = jnp.ones((ONES, vc_ref.shape[1]), bf16)


def row_plan(rows, grid_rows, sp_count, k_ref, v_ref, strips):
    own = lax.axis_index("sp") * grid_rows
    total = grid_rows * sp_count
    plan = []
    for row in rows:
        if is_free(row, grid_rows):
            plan.append((row, k_ref, v_ref, row - HALO_ROWS, WIN_ROWS - 1 - HALO_ROWS, None))
            continue
        kl_ref, kh_ref, vl_ref, vh_ref = strips
        first = jnp.clip(own + row - HALO_ROWS, 0, total - WIN_ROWS)
        offset = first - (own + row) + WIN_ROWS - 1
        if row < HALO_ROWS:
            plan.append((row, kl_ref, vl_ref, first - own + HALO_ROWS, offset, None))
        else:
            plan.append((row, kh_ref, vh_ref, first - own - (grid_rows - WIN_ROWS), offset, None))
    return plan


def inner_kernel(count, rows, q_ref, k_ref, v_ref, t_ref, *rest):
    contexts, (out_ref, kc_ref, vc_ref, *scratch) = rest[:count], rest[count:]
    far_refs(contexts, kc_ref, vc_ref)
    plan = row_plan(rows, q_ref.shape[0] // GRID_W, 0, k_ref, v_ref, None)
    attend_rows(plan, q_ref, kc_ref, vc_ref, t_ref, out_ref, scratch[0:2], scratch[2:4])


def fill_strips(k_ref, v_ref, first_ref, second_ref, strips):
    tokens, width = k_ref.shape
    kl_ref, kh_ref, vl_ref, vh_ref = strips
    strip = 3 * TILE
    ones = jnp.ones((ONES, strip), bf16)
    even = lax.axis_index("sp") % 2 == 0
    low_halo = jnp.where(even, second_ref[...], first_ref[...])
    high_halo = jnp.where(even, first_ref[...], second_ref[...])
    kl_ref[0:TILE] = low_halo[0]
    kl_ref[TILE:] = k_ref[0 : 2 * TILE]
    kh_ref[0 : 2 * TILE] = k_ref[tokens - 2 * TILE :]
    kh_ref[2 * TILE :] = high_halo[0]
    low = low_halo[1].astype(f32).T
    high = high_halo[1].astype(f32).T
    for ref in (vl_ref, vh_ref):
        ref[0, width:, :] = ones
        ref[1, width:, :] = ones
    rolled = pltpu.roll(low, TILE - GRID_W, 1).astype(bf16)
    vl_ref[0, 0:width, 0:TILE] = low.astype(bf16)
    vl_ref[0, 0:width, TILE:] = v_ref[0, 0:width, 0 : 2 * TILE]
    vl_ref[1, 0:width, 0 : TILE - GRID_W] = rolled[:, 0 : TILE - GRID_W]
    first = pltpu.roll(v_ref[0, 0:width, 0:LANES].astype(f32), GRID_W, 1).astype(bf16)
    vl_ref[1, 0:width, TILE - GRID_W : TILE] = first[:, GRID_W:]
    vl_ref[1, 0:width, TILE:] = v_ref[1, 0:width, 0 : 2 * TILE]
    rolled = pltpu.roll(high, TILE - GRID_W, 1).astype(bf16)
    vh_ref[0, 0:width, 0 : 2 * TILE] = v_ref[0, 0:width, tokens - 2 * TILE :]
    vh_ref[0, 0:width, 2 * TILE :] = high.astype(bf16)
    vh_ref[1, 0:width, 0 : 2 * TILE] = v_ref[1, 0:width, tokens - 2 * TILE :]
    vh_ref[1, 0:width, 2 * TILE - GRID_W : 2 * TILE] = rolled[:, TILE - GRID_W :]
    vh_ref[1, 0:width, 2 * TILE : strip - GRID_W] = rolled[:, 0 : TILE - GRID_W]
    vh_ref[1, 0:width, strip - GRID_W :] = jnp.zeros((width, GRID_W), bf16)


def split_blocks(out_ref, block_refs, late):
    for step, block_ref in enumerate(block_refs):
        size = block_ref.shape[1]
        owner = target("tp", step)
        share = out_ref.shape[1] // len(block_refs)
        inside = jnp.where(owner == 0, 0, share - size)
        inside = inside if late else share - size - inside
        start = owner * share + inside
        block_ref[...] = out_ref[:, part(start, LANES, size)]


def middle_kernel(rows, sp_count, done_ref, latent_ref, q_ref, k_ref, v_ref, kc_ref, vc_ref, t_ref, first_ref, second_ref, out_ref, own_ref, *rest):
    strips, block_refs, (sem, *scratch) = rest[:4], rest[4:-5], rest[-5:]
    share = own_ref.shape[0]
    mine = part(lax.axis_index("tp") * share, GRID_W, share)
    copy = pltpu.make_async_copy(latent_ref.at[mine], own_ref, sem)
    copy.start()
    fill_strips(k_ref, v_ref, first_ref, second_ref, strips)
    plan = row_plan(rows, q_ref.shape[0] // GRID_W, sp_count, k_ref, v_ref, strips)
    attend_rows(plan, q_ref, kc_ref, vc_ref, t_ref, out_ref, scratch[0:2], scratch[2:4])
    split_blocks(out_ref, block_refs, False)
    copy.wait()


def late_kernel(rows, sp_count, q_ref, k_ref, v_ref, kc_ref, vc_ref, t_ref, *rest):
    strips, block_refs, (out_ref, *scratch) = rest[:4], rest[4:-5], rest[-5:]
    plan = row_plan(rows, q_ref.shape[0] // GRID_W, sp_count, k_ref, v_ref, strips)
    attend_rows(plan, q_ref, kc_ref, vc_ref, t_ref, out_ref, scratch[0:2], scratch[2:4])
    split_blocks(out_ref, block_refs, True)


def attention_scratch(total, width):
    return [VMEM((total, width), f32)] * 2 + [VMEM((total, width), bf16)] * 2


def inner_attention(queries, keys, values, table, contexts):
    tokens, width = queries.shape
    far = len(contexts) * contexts[0].shape[1]
    rows = [r for r in phases(tokens)[0] if is_free(r, tokens // GRID_W)]
    rows = [r for r in rows if r ^ 1 in rows]
    return call(
        functools.partial(inner_kernel, len(contexts), rows),
        [array((width, tokens)), array((far, width)), array((width + ONES, far))],
        in_specs=[whole()] * (4 + len(contexts)),
        out_specs=[whole()] * 3,
        scratch_shapes=attention_scratch(NEAR + far, width),
        flops=4_000_000_000,
    )(queries, keys, values, table, *contexts)


def middle_attention(done, latent, queries, keys, values, far_keys, far_values, table, first, second):
    tokens, width = queries.shape
    strip = 3 * TILE
    count = lax.axis_size("tp")
    early, late = phases(tokens)
    rows = [
        r for r in early if not (is_free(r, tokens // GRID_W) and is_free(r ^ 1, tokens // GRID_W))
    ]
    block = array((width, len(early) * GRID_W // count))
    attended, own, *rest = call(
        functools.partial(middle_kernel, rows, lax.axis_size("sp")),
        [
            array((width, tokens)),
            array((tokens // count, latent.shape[1])),
            *[array((strip, width))] * 2,
            *[array((2, width + ONES, strip))] * 2,
            *[block] * (count if late else 0),
        ],
        in_specs=[whole(), whole(HBM)] + [whole()] * 8,
        out_specs=[whole()] * (6 + (count if late else 0)),
        input_output_aliases={0: 0},
        scratch_shapes=[pltpu.SemaphoreType.DMA]
        + attention_scratch(NEAR + far_keys.shape[0], width),
        flops=2_000_000_000,
    )(done, *in_hbm([latent]), queries, keys, values, far_keys, far_values, table, first, second)
    strips, blocks = rest[:4], rest[4:]
    if not late:
        share = tokens // count
        blocks = [
            lax.dynamic_slice_in_dim(attended, target("tp", step) * share, share, 1)
            for step in range(count)
        ]
    return own, strips, list(blocks)


def late_attention(queries, keys, values, far_keys, far_values, table, strips):
    tokens, width = queries.shape
    count = lax.axis_size("tp")
    late = phases(tokens)[1]
    if not late:
        return []
    return list(
        call(
            functools.partial(late_kernel, late, lax.axis_size("sp")),
            [array((width, len(late) * GRID_W // count))] * count,
            in_specs=[whole()] * 10,
            out_specs=[whole()] * count,
            scratch_shapes=[VMEM((width, tokens), bf16)]
            + attention_scratch(NEAR + far_keys.shape[0], width),
            flops=3_000_000_000,
        )(queries, keys, values, far_keys, far_values, table, *strips)
    )


def by_destination(tokens):
    each = tokens // GRID_W // 4
    return lax.axis_size("tp") == 4 and each % 2 == 0 and HALO_ROWS <= each


def free_target():
    return jnp.where(lax.axis_index("tp") < 2, 2, 1)


def halo_target():
    return jnp.where(lax.axis_index("tp") < 2, 3, 0)


def destination_plan(owner, tokens, sp_count, k_ref, v_ref, free):
    grid_rows = tokens // GRID_W
    each = grid_rows // 4
    own = lax.axis_index("sp") * grid_rows
    plan = []
    for index in range(each):
        row = owner * each + index
        if free:
            plan.append((row, k_ref, v_ref, row, WIN_ROWS - 1 - HALO_ROWS, index % 2))
            continue
        first = jnp.clip(own + row - HALO_ROWS, 0, grid_rows * sp_count - WIN_ROWS)
        offset = first - (own + row) + WIN_ROWS - 1
        plan.append((row, k_ref, v_ref, first - own + HALO_ROWS, offset, None))
    return plan


def first_kernel(count, k_in, v_in, q_ref, t_ref, *rest):
    contexts, (k_ref, v_ref, kc_ref, vc_ref, out_ref, *scratch) = rest[:count], rest[count:]
    far_refs(contexts, kc_ref, vc_ref)
    plan = destination_plan(free_target(), q_ref.shape[0], 0, k_ref, v_ref, True)
    attend_rows(
        plan, q_ref, kc_ref, vc_ref, t_ref, out_ref, scratch[0:2], scratch[2:4], whole_rows=False
    )


def second_kernel(sp_count, k_in, v_in, q_ref, kc_ref, vc_ref, t_ref, one_ref, two_ref, k_ref, v_ref, out_ref, *scratch):
    tokens, width = q_ref.shape
    even = lax.axis_index("sp") % 2 == 0
    low = jnp.where(even, two_ref[...], one_ref[...])
    high = jnp.where(even, one_ref[...], two_ref[...])
    end = TILE + tokens
    k_ref[0:TILE] = low[0]
    k_ref[end:] = high[0]
    turned = low[1].astype(f32).T
    rolled = pltpu.roll(turned, TILE - GRID_W, 1).astype(bf16)
    v_ref[0, 0:width, 0:TILE] = turned.astype(bf16)
    v_ref[1, 0:width, 0 : TILE - GRID_W] = rolled[:, 0 : TILE - GRID_W]
    turned = high[1].astype(f32).T
    rolled = pltpu.roll(turned, TILE - GRID_W, 1).astype(bf16)
    v_ref[0, 0:width, end:] = turned.astype(bf16)
    v_ref[1, 0:width, end - GRID_W : end] = rolled[:, TILE - GRID_W :]
    v_ref[1, 0:width, end : end + TILE - GRID_W] = rolled[:, 0 : TILE - GRID_W]
    v_ref[1, 0:width, end + TILE - GRID_W :] = jnp.zeros((width, GRID_W), bf16)
    plan = destination_plan(halo_target(), tokens, sp_count, k_ref, v_ref, False)
    attend_rows(
        plan, q_ref, kc_ref, vc_ref, t_ref, out_ref, scratch[0:2], scratch[2:4], whole_rows=False
    )


def near_kernel(step, sp_count, k_ref, v_ref, q_ref, kc_ref, vc_ref, t_ref, out_ref, *scratch):
    owner = target("tp", step)
    plan = destination_plan(owner, q_ref.shape[0], sp_count, k_ref, v_ref, False)
    attend_rows(
        plan, q_ref, kc_ref, vc_ref, t_ref, out_ref, scratch[0:2], scratch[2:4], whole_rows=False
    )


def destination_attention(queries, keys, values, table, contexts, one, two):
    tokens, width = queries.shape
    far = len(contexts) * contexts[0].shape[1]
    sp_count = lax.axis_size("sp")
    share = tokens // 4
    scratch = attention_scratch(NEAR + far, width)
    padded = [array(keys.shape), array(values.shape)]
    keys, values, far_keys, far_values, block = call(
        functools.partial(first_kernel, len(contexts)),
        [*padded, array((far, width)), array((width + ONES, far)), array((width, share))],
        in_specs=[whole()] * (4 + len(contexts)),
        out_specs=[whole()] * 5,
        input_output_aliases={0: 0, 1: 1},
        scratch_shapes=scratch,
        flops=3_000_000_000,
    )(keys, values, queries, table, *contexts)
    x1 = exchange(block, "tp", 2)
    keys, values, block = call(
        functools.partial(second_kernel, sp_count),
        [*padded, array((width, share))],
        in_specs=[whole()] * 8,
        out_specs=[whole()] * 3,
        input_output_aliases={0: 0, 1: 1},
        scratch_shapes=scratch,
        flops=3_000_000_000,
    )(keys, values, queries, far_keys, far_values, table, one, two)
    x2 = exchange(block, "tp", 2)
    blocks = []
    for step in (1, 0):
        blocks.append(
            call(
                functools.partial(near_kernel, step, sp_count),
                array((width, share)),
                in_specs=[whole()] * 6,
                out_specs=whole(),
                scratch_shapes=scratch,
                flops=3_000_000_000,
            )(keys, values, queries, far_keys, far_values, table)
        )
    neighbour = exchange(blocks[0], "tp", 1)
    passed1 = exchange(x1, "tp", 1)
    passed2 = exchange(x2, "tp", 1)
    return blocks[1], neighbour, x1, x2, passed1, passed2


def weight_rows(step, height):
    return part(origin("tp", step) * height, LANES, height)


def is_free_target():
    tp = lax.axis_index("tp")
    return (tp == 1) | (tp == 2)


def partial_kernel(w_ref, mine_ref, neighbour_ref, x1_ref, x2_ref, sum_ref, *turned):
    height = mine_ref.shape[0]
    tile = w_ref.shape[1] // 4
    values = (
        mine_ref[...],
        neighbour_ref[...],
        jnp.where(is_free_target(), x1_ref[...], x2_ref[...]),
    )
    for ref, value in zip(turned, values):
        ref[...] = value.astype(f32).T.astype(bf16)
    for step in range(4):
        cols = slice(step * tile, (step + 1) * tile)
        total = None
        for index, ref in enumerate(turned):
            weight = w_ref[weight_rows(index, height), cols]
            term = jnp.dot(ref[...], weight, preferred_element_type=f32)
            total = term if total is None else total + term
        sum_ref[:, cols] = total


def gather_kernel(x_ref, w_ref, sum_ref, one_ref, two_ref, *rest):
    pieces, (out_ref, gate_ref, held_ref, turned_ref, sems) = rest[:4], rest[4:]
    height, share = one_ref.shape
    tile = w_ref.shape[1] // 4
    mine = part(lax.axis_index("tp") * share, GRID_W, share)
    for index in range(4):
        gate_ref[:, part(origin("tp", index) * tile, LANES, tile)] = pieces[index][4:5, :]
    value = jnp.where(is_free_target(), one_ref[...], two_ref[...])
    turned_ref[...] = value.astype(f32).T.astype(bf16)
    copies = []
    for step in range(4):
        cols = slice(step * tile, (step + 1) * tile)
        weight = w_ref[weight_rows(3, height), cols]
        total = sum_ref[:, cols] + jnp.dot(turned_ref[...], weight, preferred_element_type=f32)
        held_ref[:, cols] = (x_ref[mine, cols].astype(f32) + gate_ref[:, cols] * total).astype(bf16)
        copies.append(
            pltpu.make_async_copy(held_ref.at[:, cols], out_ref.at[:, cols], sems.at[step])
        )
        copies[-1].start()
    for copy in copies:
        copy.wait()


def gathered_output(x, weight, blocks, pieces):
    mine, neighbour, x1, x2, passed1, passed2 = blocks
    share, width = x.shape[0] // 4, x.shape[1]
    height = mine.shape[0]
    total = call(
        partial_kernel,
        array((share, width), f32),
        in_specs=[whole()] * 5,
        out_specs=whole(),
        scratch_shapes=[VMEM((share, height), bf16)] * 3,
        flops=2_000_000_000,
    )(weight, mine, neighbour, x1, x2)
    return call(
        gather_kernel,
        array((share, width)),
        in_specs=[whole()] * 9,
        out_specs=whole(HBM),
        scratch_shapes=[
            VMEM((1, width), f32),
            VMEM((share, width), bf16),
            VMEM((share, height), bf16),
            pltpu.SemaphoreType.DMA((4,)),
        ],
        flops=2_000_000_000,
    )(x, weight, total, passed1, passed2, *pieces)


def output_kernel(count, late, *refs):
    x_ref, w_ref, *arrays, out_ref, gate_ref, held_ref, block_ref, sems = refs[late:]
    pieces, blocks = arrays[:count], arrays[count:]
    height, size = blocks[0].shape
    share = out_ref.shape[0]
    tile = w_ref.shape[1] // count
    tp = lax.axis_index("tp")
    for index in range(count):
        gate_ref[:, part(origin("tp", index) * tile, LANES, tile)] = pieces[index][4:5, :]
        rows = part(origin("tp", index) * height, LANES, height)
        block_ref[:, rows] = blocks[index][...].astype(f32).T.astype(bf16)
    inside = jnp.where(tp == 0, 0, share - size)
    inside = inside if late else share - size - inside
    mine = part(inside, GRID_W, size)
    copies = []
    for step in range(count):
        cols = slice(step * tile, (step + 1) * tile)
        total = jnp.dot(block_ref[...], w_ref[:, cols], preferred_element_type=f32)
        held_ref[:, cols] = (
            x_ref[mine, cols].astype(f32) + gate_ref[:, cols] * total
        ).astype(bf16)
        copies.append(
            pltpu.make_async_copy(held_ref.at[:, cols], out_ref.at[mine, cols], sems.at[step])
        )
        copies[-1].start()
    for copy in copies:
        copy.wait()


def output(x, weight, blocks, pieces, done=None):
    count = len(blocks)
    share, width = x.shape
    size = blocks[0].shape[1]
    late = done is not None
    return call(
        functools.partial(output_kernel, count, late),
        array((share, width)),
        in_specs=[whole(HBM)] * late + [whole()] * (2 + len(pieces) + len(blocks)),
        out_specs=whole(HBM),
        input_output_aliases={0: 0} if late else {},
        scratch_shapes=[
            VMEM((1, width), f32),
            VMEM((size, width), bf16),
            VMEM((size, weight.shape[0]), bf16),
            pltpu.SemaphoreType.DMA((count,)),
        ],
        flops=2_000_000_000,
    )(*([done] if late else []), x, weight, *pieces, *blocks)


def gathered(block, axis):
    blocks = [block]
    for step in range(1, lax.axis_size(axis)):
        blocks.append(exchange(block, axis, step))
    return blocks


def sent(blocks):
    return blocks[:1] + [exchange(blocks[step], "tp", step) for step in range(1, len(blocks))]


def local(
    latent,
    condition,
    context_tokens,
    context_condition,
    shift_weight,
    scale_weight,
    gate_weight,
    norm_gain,
    query_weight,
    key_weight,
    value_weight,
    out_weight,
    offset_bias,
):
    terms, gain = modulation_terms(
        condition, context_condition, shift_weight, scale_weight, gate_weight, norm_gain
    )
    partials = gathered(terms, "sp")
    wk, rows = bias_rows(terms, offset_bias, key_weight)
    summed = summed_terms(rows, partials)
    pieces = gathered(summed, "tp")
    wv, wq, table = bias_table(summed, rows, value_weight, query_weight)
    weights = (wq, wk, wv)
    *edges, far, a, b = edge_projections(
        latent, context_tokens, gain, weights, pieces
    )
    count = lax.axis_size("sp")
    contexts = gathered(far, "sp")
    pairs = [(i, i ^ 1) for i in range(count) if i ^ 1 < count]
    first = lax.ppermute(edges[4], "sp", pairs)
    pairs = [(i, j) for i in range(count) for j in [((i + 1) ^ 1) - 1] if 0 <= j < count]
    second = lax.ppermute(edges[5], "sp", pairs)
    special = by_destination(latent.shape[0])
    fields = main_projections(latent, a, b, weights, edges[:4], TILE if special else 0)
    if special:
        blocks = destination_attention(*fields, table, contexts, first, second)
        return gathered_output(latent, out_weight, blocks, pieces)
    inner, *fars = inner_attention(*fields, table, contexts)
    own, strips, early = middle_attention(inner, latent, *fields, *fars, table, first, second)
    early = sent(early)
    late = late_attention(*fields, *fars, table, strips)
    late = sent(late)
    done = output(own, out_weight, early, pieces)
    if not late:
        return done
    return output(own, out_weight, late, pieces, done)


def solution(mesh):
    placed = (
        P(("grp", "sp"), None),
        P("grp"),
        P(("grp", "sp"), None),
        P(),
        P("sp", "tp"),
        P("sp", "tp"),
        P("sp", "tp"),
        P(),
        P(None, "tp"),
        P(None, "tp"),
        P(None, "tp"),
        P(),
        P("tp", None, None),
    )
    return jax.shard_map(
        local, mesh=mesh, in_specs=placed, out_specs=P(("grp", "sp", "tp"), None), check_vma=False
    )
```
